128 devices in a mesh: fs: 16 (over z, x), tp: 8 (over y, core).
Axes of the slice: x: 4, y: 4, z: 4, core: 2. Of those that a mesh axis runs over, the one named last changes fastest.
Arguments:
- inputs: bfloat16 [16384, 4096], P('fs'), may hold values from -8 to 8
- value_cot: bfloat16 [16384, 2048], P('fs', 'tp'), may hold values from -0.01171875 to 0.01171875
- gate_cot: bfloat16 [16384, 2048], P('fs', 'tp'), may hold values from -0.01171875 to 0.01171875
- out_cot: bfloat16 [16384, 4096], P('fs'), may hold values from -0.015625 to 0.015625
- conv_output: bfloat16 [16384, 2048], P('fs', 'tp'), may hold values from -6 to 6
- factors: bfloat16 [3, 4096, 256], P(None, 'fs'), may hold values from -0.375 to 0.375
- value_weight: float32 [4096, 2048], P('fs', 'tp'), may hold values from -0.09375 to 0.09375
- gate_weight: float32 [4096, 2048], P('fs', 'tp'), may hold values from -0.09375 to 0.09375
- out_weight: float32 [2048, 4096], P('tp', 'fs'), may hold values from -0.125 to 0.125
- first_moment: float32 [3, 256, 2048], P(None, 'fs', 'tp'), may hold values from -7.2 to 7.2
- second_moment: float32 [3, 256, 2048], P(None, 'fs', 'tp'), may hold values from 0.005 to 0.05
Outputs:
- new_first: float32 [3, 256, 2048], P(None, 'fs', 'tp')
- new_second: float32 [3, 256, 2048], P(None, 'fs', 'tp')
- value_update: float32 [4096, 2048], P('fs', 'tp')
- gate_update: float32 [4096, 2048], P('fs', 'tp')
- out_update: float32 [2048, 4096], P('tp', 'fs')
- value_copy: bfloat16 [4096, 2048], P(None, 'tp')
- gate_copy: bfloat16 [4096, 2048], P(None, 'tp')
- out_copy: bfloat16 [2048, 4096], P('tp')
The draws below stay inside these ranges and needn't reach their ends.
All inputs are finite; a program needn't handle non-finite values.
Results may differ from the reference program's by a relative error of at most 0.001.
Values may be sent and summed in bfloat16 or wider, within the bound.
A program may use at most 128 MiB of HBM per device.

```python
import math
import jax
import jax.numpy as jnp
from jax import lax

D = 4096
C = 2048
RANK = 256
TOKENS = 16384


def draw_first_moment(key, part):
    key_one, key_two = jax.random.split(jax.random.fold_in(key, 11), 2)
    row_rise = jnp.arange(RANK, dtype=jnp.float32) / max(RANK - 1, 1)
    col_rise = jnp.arange(C, dtype=jnp.float32) / max(C - 1, 1)
    rise_table = jnp.exp(jnp.log(3.0) * row_rise)[:, None] * jnp.exp(jnp.log(3.0) * col_rise)[None, :]
    roughness = jnp.exp(jax.random.uniform(key_two, (3, RANK, C), jnp.float32, 0.0, jnp.log(2.0)))
    base_draw = jnp.clip(jax.random.normal(key_one, (3, RANK, C), jnp.float32), -4.0, 4.0)
    return (0.1 * base_draw * rise_table[None, :, :] * roughness).astype(jnp.float32)


def spiked(result, rng, source, target, blocks, factor):
    owner, partner = [(jnp.arange(result.shape[axis_at]) // (result.shape[axis_at] // blocks)).reshape([-1 if axis == axis_at else 1 for axis in range(result.ndim)]) for axis_at in (source, target)]
    chosen = jax.random.permutation(rng, blocks)[partner]
    strong = (owner == chosen) | (owner == (partner + blocks // 2) % blocks)
    return jnp.where(strong, factor * result, result)


def block_levels(stream_key, extent, cuts, least, largest):
    factor_of = 1.0
    for dim, parts in cuts:
        draws = jax.random.uniform(jax.random.fold_in(jax.random.fold_in(stream_key, 6), dim), (parts,), jnp.float32, least / len(cuts), largest / len(cuts))
        factor_of = factor_of * jnp.repeat(jnp.exp(draws), extent[dim] // parts).reshape((-1,) + (1,) * (len(extent) - 1 - dim))
    return factor_of


def centred(own_key, dims, deviation, bound, cuts=(), held_as=jnp.bfloat16):
    result = deviation * jax.random.normal(own_key, dims, jnp.float32)
    if cuts:
        result = result * block_levels(own_key, dims, cuts, -0.22, 0.18)
    return jnp.clip(result, -bound, bound).astype(held_as)


def gaussian_with(key, extent, width, limit, pieces, heavy, kind=jnp.bfloat16):
    array = width * jax.random.normal(key, extent, jnp.float32)
    if pieces:
        array = array * block_levels(key, extent, pieces, -0.22, 0.18)
    return jnp.clip(spiked(array, jax.random.fold_in(key, 3), *heavy), -limit, limit).astype(kind)


def setup_inputs(seed: int = 0) -> dict:
    keys = jax.random.split(jax.random.key(seed), 12)
    inputs = gaussian_with(keys[0], (TOKENS, D), 1.0, 8.0, ((0, 16),), (0, 1, 16, 2.0))
    value_cot = centred(keys[1], (TOKENS, C), (RANK ** 0.5 * (D * TOKENS) ** -0.5), 0.01171875, ((0, 16), (1, 8)))
    gate_cot = centred(keys[2], (TOKENS, C), (RANK ** 0.5 * (D * TOKENS) ** -0.5), 0.01171875, ((0, 16), (1, 8)))
    out_cot = gaussian_with(keys[3], (TOKENS, D), (RANK ** 0.5 * (D * TOKENS) ** -0.5), 0.015625, ((0, 16),), (0, 1, 16, 2.0))
    conv_output = centred(keys[4], (TOKENS, C), 1.0, 6.0, ((0, 16), (1, 8)))
    factors = centred(keys[5], (3, D, RANK), RANK ** -0.5, 0.375, ((1, 16),))
    value_weight = centred(keys[6], (D, C), D ** -0.5, 0.09375, ((0, 16), (1, 8)), jnp.float32)
    gate_weight = centred(keys[7], (D, C), D ** -0.5, 0.09375, ((0, 16), (1, 8)), jnp.float32)
    out_weight = centred(keys[8], (C, D), C ** -0.5, 0.125, ((0, 8), (1, 16)), jnp.float32)
    first_moment = draw_first_moment(jax.random.fold_in(keys[11], 71), 0)
    second_moment = jnp.clip(jnp.exp(math.log(0.05) - 2.3025851 * jax.random.uniform(keys[10], (3, RANK, C), jnp.float32) ** block_levels(keys[10], (3, RANK, C), ((1, 16), (2, 8)), -0.2, 0.2)), 0.005, 0.05)
    return dict(inputs=inputs, value_cot=value_cot, gate_cot=gate_cot, out_cot=out_cot, conv_output=conv_output, factors=factors, value_weight=value_weight, gate_weight=gate_weight, out_weight=out_weight, first_moment=first_moment, second_moment=second_moment)


FIRST_DECAY = 0.9
SECOND_DECAY = 0.95
DIVISOR_EPS = 1e-08
SQUARE_EPS = 1e-06
LEARN_RATE = 0.01

def project_side(source, factor, target):
    left_proj = jnp.dot(source.astype(jnp.float32), factor.astype(jnp.float32), precision=lax.Precision.HIGHEST)
    return jnp.dot(left_proj.T, target.astype(jnp.float32), precision=lax.Precision.HIGHEST)

def reference(inputs, value_cot, gate_cot, out_cot, conv_output, factors, value_weight, gate_weight, out_weight, first_moment, second_moment):
    projected = jnp.stack([project_side(inputs, factors[0], value_cot), project_side(inputs, factors[1], gate_cot), project_side(out_cot, factors[2], conv_output)])
    new_first = FIRST_DECAY * first_moment + (1.0 - FIRST_DECAY) * projected
    new_second = SECOND_DECAY * second_moment + (1.0 - SECOND_DECAY) * projected * projected
    direction = new_first / (jnp.sqrt(new_second) + DIVISOR_EPS)
    total = jnp.sum(direction * direction)
    norm_scale = lax.rsqrt(total / (3 * RANK * C) + SQUARE_EPS)
    float_factors = factors.astype(jnp.float32)
    value_update = norm_scale * jnp.dot(float_factors[0], direction[0], precision=lax.Precision.HIGHEST)
    gate_update = norm_scale * jnp.dot(float_factors[1], direction[1], precision=lax.Precision.HIGHEST)
    out_update = (norm_scale * jnp.dot(float_factors[2], direction[2], precision=lax.Precision.HIGHEST)).T
    value_copy = (value_weight - LEARN_RATE * value_update).astype(jnp.bfloat16)
    gate_copy = (gate_weight - LEARN_RATE * gate_update).astype(jnp.bfloat16)
    out_copy = (out_weight - LEARN_RATE * out_update).astype(jnp.bfloat16)
    return (new_first, new_second, value_update, gate_update, out_update, value_copy, gate_copy, out_copy)
```

```python
import functools

import jax
import jax.numpy as jnp
from jax import lax
from jax.experimental import pallas as pl
from jax.experimental.pallas import tpu as pltpu
from jax.sharding import PartitionSpec as P

C = 2048
RANK = 256
FIRST_DECAY = 0.9
SECOND_DECAY = 0.95
DIVISOR_EPS = 1e-08
SQUARE_EPS = 1e-06
LEARN_RATE = 0.01

SIDE = 4
FS = SIDE * SIDE
TP = 8
W = 256
RS = RANK // FS
TOK = 1024
D = 4096
MESH = pl.DeviceIdType.MESH
F32 = jnp.float32
BF16 = jnp.bfloat16

MESSAGES = []
for _k in (0, 1):
    for _d in (1, -1):
        MESSAGES.append((_k, 1, 0, _d))
        MESSAGES.append((_k, 2, 0, _d))
        for _po in (0, -1, 1, 2):
            MESSAGES.append((_k, 3, _po, _d))
            MESSAGES.append((_k, 4, _po, _d))
INDEX = {message: at for at, message in enumerate(MESSAGES)}
COUNT = len(MESSAGES)


class RingGather:
    def __init__(self, me, part, send, recv):
        self.z, self.x = me // SIDE, lax.rem(me, SIDE)
        self.part, self.send, self.recv = part, send, recv

    def slot(self, k, po, qo):
        dx, dz = (po, qo) if k == 0 else (qo, po)
        z = lax.rem(self.z + dz + SIDE, SIDE)
        x = lax.rem(self.x + dx + SIDE, SIDE)
        return z * SIDE + x

    def copy(self, message, received):
        k, stage, po, d = message
        if stage == 1:
            at, half, first = (0, 0), None, True
        elif stage == 2:
            at, half, first = (-d, 0), 0 if d > 0 else 1, True
        elif stage == 3:
            at, half, first = (po, 0), None, False
        else:
            at, half, first = (po, -d), 0 if d > 0 else 1, False
        to = self.slot(k, d, 0) if first else self.slot(k, 0, d)
        if received:
            at = (at[0] - d, at[1]) if first else (at[0], at[1] - d)
        at = tuple((o + 1) % SIDE - 1 for o in at)
        ref = self.part(self.slot(k, *at), k, half)
        index = INDEX[message]
        return pltpu.make_async_remote_copy(
            src_ref=ref,
            dst_ref=ref,
            send_sem=self.send.at[index],
            recv_sem=self.recv.at[index],
            device_id={"fs": to},
            device_id_type=MESH,
        )

    def start(self, *message):
        self.copy(message, False).start()

    def wait(self, *message):
        self.copy(message, True).wait_recv()

    def run(self, arrived):
        for stage in (1, 3):
            for d in (1, -1):
                for k in (0, 1):
                    self.start(k, stage, 0, d)
        for d in (1, -1):
            for k in (0, 1):
                self.wait(k, 1, 0, d)
                self.start(k, 2, 0, d)
                self.start(k, 3, -d, 1)
                self.start(k, 3, -d, -1)
                arrived(k, -d, 0)
        for d in (1, -1):
            for k in (0, 1):
                self.wait(k, 3, 0, d)
                self.start(k, 4, 0, d)
                arrived(k, 0, -d)
        for k in (0, 1):
            self.wait(k, 2, 0, 1)
            self.wait(k, 2, 0, -1)
            self.start(k, 3, 2, 1)
            self.start(k, 3, 2, -1)
            arrived(k, 2, 0)
        for po in (-1, 1):
            for d in (1, -1):
                for k in (0, 1):
                    self.wait(k, 3, po, d)
                    self.start(k, 4, po, d)
                    arrived(k, po, -d)
        for k in (0, 1):
            self.wait(k, 4, 0, 1)
            self.wait(k, 4, 0, -1)
            arrived(k, 0, 2)
        for d in (1, -1):
            for k in (0, 1):
                self.wait(k, 3, 2, d)
                self.start(k, 4, 2, d)
                arrived(k, 2, -d)
        for po in (-1, 1, 2):
            for k in (0, 1):
                self.wait(k, 4, po, 1)
                self.wait(k, 4, po, -1)
                arrived(k, po, 2)

    def finish(self):
        for message in MESSAGES:
            self.copy(message, False).wait_send()


def high_low(values):
    upper = values.astype(BF16)
    return upper, (values - upper.astype(F32)).astype(BF16)


def kernel(
    inputs,
    value_cot,
    gate_cot,
    out_cot,
    conv_output,
    factors,
    value_weight,
    gate_weight,
    out_weight,
    first_moment,
    second_moment,
    first_out,
    second_out,
    value_update,
    gate_update,
    out_update,
    value_copy,
    gate_copy,
    out_copy,
    inp,
    oct_,
    cots,
    cots_t,
    fbuf,
    wbuf,
    mom,
    summed,
    pieces,
    arrived_pieces,
    dirs,
    sums,
    upd,
    copies,
    local_sem,
    out_sem,
    f_send,
    f_recv,
    core_send,
    core_recv,
    a_send,
    a_recv,
    d_send,
    d_recv,
    s_send,
    s_recv,
    c_send,
    c_recv,
):
    me = lax.axis_index("fs")
    t = lax.axis_index("tp")
    core = lax.rem(t, 2)
    partner = t + 1 - 2 * core

    loads = []

    def load(src, dst):
        copy = pltpu.make_async_copy(src, dst, local_sem.at[len(loads)])
        copy.start()
        loads.append(copy)

    load(factors, fbuf.at[me])
    load(inputs, inp)
    load(out_cot, oct_)
    load(value_cot, cots.at[0])
    load(gate_cot, cots.at[1])
    load(conv_output, cots.at[2])
    load(first_moment, mom.at[0])
    load(second_moment, mom.at[1])
    load(value_weight, wbuf.at[0])
    load(gate_weight, wbuf.at[1])
    load(out_weight, wbuf.at[2])

    barrier = pltpu.get_barrier_semaphore()

    def greet_fs(j, _):
        pl.semaphore_signal(
            barrier, inc=1, device_id={"fs": lax.rem(me + j, FS)}, device_id_type=MESH
        )
        return _

    def greet_tp(j, _):
        pl.semaphore_signal(
            barrier, inc=1, device_id={"tp": lax.rem(t + j, TP)}, device_id_type=MESH
        )
        return _

    lax.fori_loop(1, FS, greet_fs, 0)
    lax.fori_loop(1, TP, greet_tp, 0)
    pl.semaphore_wait(barrier, FS - 1 + TP - 1)

    def factor_part(of_core):
        def part(s, k, half):
            at = of_core * 128 + 64 * k
            size = 64
            if half is not None:
                at, size = at + 32 * half, 32
            return fbuf.at[s, :, pl.ds(pl.multiple_of(at, 32), size), :]

        return part

    ring = RingGather(me, factor_part(core), f_send, f_recv)

    def share(k, po, qo, mine):
        at = (po + 1) * SIDE + (qo + 1) + FS * k
        ref = factor_part(core if mine else 1 - core)(ring.slot(k, po, qo), k, None)
        return pltpu.make_async_remote_copy(
            src_ref=ref,
            dst_ref=ref,
            send_sem=core_send.at[at],
            recv_sem=core_recv.at[at],
            device_id={"tp": partner},
            device_id_type=MESH,
        )

    def multiply(s, first):
        cols = pl.ds(pl.multiple_of(s * W, W), W)

        def tile(i, _):
            rows = pl.ds(pl.multiple_of(i * 256, 256), 256)
            left = inp[rows, cols]
            other = oct_[rows, cols]
            for m in range(3):
                product = jnp.dot(
                    other if m == 2 else left, fbuf[s, m], preferred_element_type=F32
                )
                if first:
                    summed[m, rows, :] = product
                else:
                    summed[m, rows, :] += product
            return _

        lax.fori_loop(0, TOK // 256, tile, 0)

    parts_here = {}

    def turn_cots():
        for copy in loads[3:6]:
            copy.wait()
        for m in range(3):

            def turn(i, _):
                rows = pl.ds(pl.multiple_of(i * 256, 256), 256)
                cots_t[m, :, rows] = cots[m, rows, :].T
                return _

            lax.fori_loop(0, TOK // 256, turn, 0)

    def factor_arrived(k, po, qo):
        share(k, po, qo, True).start()
        dx, dz = (po, qo) if k == 0 else (qo, po)
        if (dx, dz) not in parts_here:
            parts_here[dx, dz] = 1
            return
        for kk in (0, 1):
            pq = (dx, dz) if kk == 0 else (dz, dx)
            share(kk, *pq, False).wait_recv()
        multiply(ring.slot(0, dx, dz), False)

    loads[0].wait()

    class First:
        done = False

    def on_factor(k, po, qo):
        if not First.done:
            First.done = True
            turn_cots()
            loads[1].wait()
            loads[2].wait()
            multiply(me, True)
        factor_arrived(k, po, qo)

    ring.run(on_factor)

    for m in range(3):
        upper, lower = high_low(summed[m])
        product = jnp.dot(cots_t[m], upper, preferred_element_type=F32)
        product += jnp.dot(cots_t[m], lower, preferred_element_type=F32)
        pieces[:, m, :, :] = product.T.reshape(FS, RS, W)

    def to_owner(j):
        peer = lax.rem(me + j, FS)
        return pltpu.make_async_remote_copy(
            src_ref=pieces.at[peer],
            dst_ref=arrived_pieces.at[me],
            send_sem=a_send.at[j],
            recv_sem=a_recv.at[j],
            device_id={"fs": peer},
            device_id_type=MESH,
        )

    def from_peer(j):
        source = lax.rem(me - j + FS, FS)
        return pltpu.make_async_remote_copy(
            src_ref=pieces.at[source],
            dst_ref=arrived_pieces.at[source],
            send_sem=a_send.at[j],
            recv_sem=a_recv.at[j],
            device_id={"fs": source},
            device_id_type=MESH,
        )

    def loop(start, stop, step):
        def body(j, carry):
            step(j)
            return carry

        lax.fori_loop(start, stop, body, 0)

    loop(1, FS, lambda j: to_owner(j).start())

    def add_piece(j, total):
        from_peer(j).wait_recv()
        return total + arrived_pieces[lax.rem(me - j + FS, FS)]

    projected = lax.fori_loop(1, FS, add_piece, pieces[me])

    loads[6].wait()
    loads[7].wait()
    new_first = FIRST_DECAY * mom[0] + (1.0 - FIRST_DECAY) * projected
    new_second = SECOND_DECAY * mom[1] + (1.0 - SECOND_DECAY) * projected * projected
    dirs[me] = new_first / (jnp.sqrt(new_second) + DIVISOR_EPS)
    mom[0] = new_first
    mom[1] = new_second

    def direction(j, received):
        source = lax.rem(me - j + FS, FS) if received else me
        return pltpu.make_async_remote_copy(
            src_ref=dirs.at[source],
            dst_ref=dirs.at[source],
            send_sem=d_send.at[j],
            recv_sem=d_recv.at[j],
            device_id={"fs": lax.rem(me + j, FS)},
            device_id_type=MESH,
        )

    loop(1, FS, lambda j: direction(j, False).start())

    stores = []

    def store(src, dst):
        copy = pltpu.make_async_copy(src, dst, out_sem.at[len(stores)])
        copy.start()
        stores.append(copy)

    store(mom.at[0], first_out)
    store(mom.at[1], second_out)

    loop(1, FS, lambda j: direction(j, True).wait_recv())

    def square(s, total):
        block = dirs[s].reshape(3 * RS // 8, 8, W)
        return total + jnp.sum(block * block, axis=0)

    squares = lax.fori_loop(0, FS, square, jnp.zeros((8, W), F32))
    sums[t] = squares[:, :128] + squares[:, 128:]

    def scalar(j, received):
        source = lax.rem(t - j + TP, TP) if received else t
        return pltpu.make_async_remote_copy(
            src_ref=sums.at[source],
            dst_ref=sums.at[source],
            send_sem=s_send.at[j],
            recv_sem=s_recv.at[j],
            device_id={"tp": lax.rem(t + j, TP)},
            device_id_type=MESH,
        )

    loop(1, TP, lambda j: scalar(j, False).start())

    unscaled = []
    for m in range(3):
        whole = dirs[:, m, :, :].reshape(RANK, W)
        if m == 2:
            upper, lower = high_low(whole.T)
            contract = (((1,), (1,)), ((), ()))
            own = fbuf[me, m]
            update = lax.dot_general(upper, own, contract, preferred_element_type=F32)
            update += lax.dot_general(lower, own, contract, preferred_element_type=F32)
        else:
            upper, lower = high_low(whole)
            update = jnp.dot(fbuf[me, m], upper, preferred_element_type=F32)
            update += jnp.dot(fbuf[me, m], lower, preferred_element_type=F32)
        upd[m] = update
    for copy in loads[8:]:
        copy.wait()
    loop(1, TP, lambda j: scalar(j, True).wait_recv())
    total = jnp.sum(jnp.sum(sums[...], axis=0), keepdims=True)
    norm_scale = lax.rsqrt(total / (3 * RANK * C) + SQUARE_EPS)
    for m in range(3):
        update = norm_scale * upd[m]
        upd[m] = update
        copies[me, m] = (wbuf[m] - LEARN_RATE * update).astype(BF16)

    def copy_part(s, k, half):
        at, size = 128 * k, 128
        if half is not None:
            at, size = at + 64 * half, 64
        return copies.at[s, :, pl.ds(at, size), :]

    gather = RingGather(me, copy_part, c_send, c_recv)

    def store_block(s):
        at = pl.ds(pl.multiple_of(s * W, W), W)
        store(copies.at[s, 0], value_copy.at[at, :])
        store(copies.at[s, 1], gate_copy.at[at, :])
        store(copies.at[s, 2], out_copy.at[:, at])

    blocks = {}

    def copy_arrived(k, po, qo):
        dx, dz = (po, qo) if k == 0 else (qo, po)
        if not blocks:
            for m, ref in enumerate((value_update, gate_update, out_update)):
                store(upd.at[m], ref)
            store_block(me)
        if (dx, dz) in blocks:
            store_block(gather.slot(0, dx, dz))
        blocks[dx, dz] = 1

    gather.run(copy_arrived)

    gather.finish()
    ring.finish()
    for k in (0, 1):
        for po in (-1, 0, 1, 2):
            for qo in (-1, 0, 1, 2):
                if (po, qo) != (0, 0):
                    share(k, po, qo, True).wait_send()
    loop(1, FS, lambda j: to_owner(j).wait_send())
    loop(1, FS, lambda j: direction(j, False).wait_send())
    loop(1, TP, lambda j: scalar(j, False).wait_send())
    for copy in stores:
        copy.wait()


def shards(*args):
    anywhere = pl.BlockSpec(memory_space=pl.ANY)
    dma = pltpu.SemaphoreType.DMA
    return pl.pallas_call(
        kernel,
        out_shape=(
            jax.ShapeDtypeStruct((3, RS, W), F32),
            jax.ShapeDtypeStruct((3, RS, W), F32),
            jax.ShapeDtypeStruct((W, W), F32),
            jax.ShapeDtypeStruct((W, W), F32),
            jax.ShapeDtypeStruct((W, W), F32),
            jax.ShapeDtypeStruct((D, W), BF16),
            jax.ShapeDtypeStruct((D, W), BF16),
            jax.ShapeDtypeStruct((W, D), BF16),
        ),
        in_specs=[anywhere] * 11,
        out_specs=(anywhere,) * 8,
        scratch_shapes=[
            pltpu.VMEM((TOK, D), BF16),
            pltpu.VMEM((TOK, D), BF16),
            pltpu.VMEM((3, TOK, W), BF16),
            pltpu.VMEM((3, W, TOK), BF16),
            pltpu.VMEM((FS, 3, W, RANK), BF16),
            pltpu.VMEM((3, W, W), F32),
            pltpu.VMEM((2, 3, RS, W), F32),
            pltpu.VMEM((3, TOK, RANK), F32),
            pltpu.VMEM((FS, 3, RS, W), F32),
            pltpu.VMEM((FS, 3, RS, W), F32),
            pltpu.VMEM((FS, 3, RS, W), F32),
            pltpu.VMEM((TP, 8, 128), F32),
            pltpu.VMEM((3, W, W), F32),
            pltpu.VMEM((FS, 3, W, W), BF16),
            dma((11,)),
            dma((5 + 3 * FS,)),
            dma((COUNT,)),
            dma((COUNT,)),
            dma((2 * FS,)),
            dma((2 * FS,)),
            dma((FS,)),
            dma((FS,)),
            dma((FS,)),
            dma((FS,)),
            dma((TP,)),
            dma((TP,)),
            dma((COUNT,)),
            dma((COUNT,)),
        ],
        compiler_params=pltpu.CompilerParams(
            collective_id=0, has_side_effects=True, vmem_limit_bytes=60 * 1024 * 1024
        ),
    )(*args)


def solution(mesh):
    placed = (
        P("fs", None),
        P("fs", "tp"),
        P("fs", "tp"),
        P("fs", None),
        P("fs", "tp"),
        P(None, "fs", None),
        P("fs", "tp"),
        P("fs", "tp"),
        P("tp", "fs"),
        P(None, "fs", "tp"),
        P(None, "fs", "tp"),
    )
    return jax.shard_map(
        shards,
        mesh=mesh,
        in_specs=placed,
        out_specs=(
            P(None, "fs", "tp"),
            P(None, "fs", "tp"),
            P("fs", "tp"),
            P("fs", "tp"),
            P("tp", "fs"),
            P(None, "tp"),
            P(None, "tp"),
            P("tp", None),
        ),
        check_vma=False,
    )
```

```python
import functools

import jax
import jax.numpy as jnp
from jax import lax
from jax.experimental import pallas as pl
from jax.experimental.pallas import tpu as pltpu
from jax.sharding import PartitionSpec as P

C = 2048
RANK = 256
FIRST_DECAY = 0.9
SECOND_DECAY = 0.95
DIVISOR_EPS = 1e-08
SQUARE_EPS = 1e-06
LEARN_RATE = 0.01

SIDE = 4
FS = SIDE * SIDE
TP = 8
W = 256
RS = RANK // FS
TOK = 1024
D = 4096
MESH = pl.DeviceIdType.MESH
F32 = jnp.float32
BF16 = jnp.bfloat16

MESSAGES = []
for _k in (0, 1):
    for _d in (1, -1):
        MESSAGES.append((_k, 1, 0, _d))
        MESSAGES.append((_k, 2, 0, _d))
        for _po in (0, -1, 1, 2):
            MESSAGES.append((_k, 3, _po, _d))
            MESSAGES.append((_k, 4, _po, _d))
INDEX = {message: at for at, message in enumerate(MESSAGES)}
COUNT = len(MESSAGES)


class RingGather:
    def __init__(self, me, part, send, recv):
        self.z, self.x = me // SIDE, lax.rem(me, SIDE)
        self.part, self.send, self.recv = part, send, recv

    def slot(self, k, po, qo):
        dx, dz = (po, qo) if k == 0 else (qo, po)
        z = lax.rem(self.z + dz + SIDE, SIDE)
        x = lax.rem(self.x + dx + SIDE, SIDE)
        return z * SIDE + x

    def copy(self, message, received):
        k, stage, po, d = message
        if stage == 1:
            at, half, first = (0, 0), None, True
        elif stage == 2:
            at, half, first = (-d, 0), 0 if d > 0 else 1, True
        elif stage == 3:
            at, half, first = (po, 0), None, False
        else:
            at, half, first = (po, -d), 0 if d > 0 else 1, False
        to = self.slot(k, d, 0) if first else self.slot(k, 0, d)
        if received:
            at = (at[0] - d, at[1]) if first else (at[0], at[1] - d)
        at = tuple((o + 1) % SIDE - 1 for o in at)
        ref = self.part(self.slot(k, *at), k, half)
        index = INDEX[message]
        return pltpu.make_async_remote_copy(
            src_ref=ref,
            dst_ref=ref,
            send_sem=self.send.at[index],
            recv_sem=self.recv.at[index],
            device_id={"fs": to},
            device_id_type=MESH,
        )

    def start(self, *message):
        self.copy(message, False).start()

    def wait(self, *message):
        with jax.named_scope("wait_{}_{}_{}_{}".format(*message)):
            self.copy(message, True).wait_recv()

    def run(self, arrived):
        for stage in (1, 3):
            for d in (1, -1):
                for k in (0, 1):
                    self.start(k, stage, 0, d)
        for d in (1, -1):
            for k in (0, 1):
                self.wait(k, 1, 0, d)
                self.start(k, 2, 0, d)
                self.start(k, 3, -d, 1)
                self.start(k, 3, -d, -1)
                arrived(k, -d, 0)
        for d in (1, -1):
            for k in (0, 1):
                self.wait(k, 3, 0, d)
                self.start(k, 4, 0, d)
                arrived(k, 0, -d)
        for k in (0, 1):
            self.wait(k, 2, 0, 1)
            self.wait(k, 2, 0, -1)
            self.start(k, 3, 2, 1)
            self.start(k, 3, 2, -1)
            arrived(k, 2, 0)
        for po in (-1, 1):
            for d in (1, -1):
                for k in (0, 1):
                    self.wait(k, 3, po, d)
                    self.start(k, 4, po, d)
                    arrived(k, po, -d)
        for k in (0, 1):
            self.wait(k, 4, 0, 1)
            self.wait(k, 4, 0, -1)
            arrived(k, 0, 2)
        for d in (1, -1):
            for k in (0, 1):
                self.wait(k, 3, 2, d)
                self.start(k, 4, 2, d)
                arrived(k, 2, -d)
        for po in (-1, 1, 2):
            for k in (0, 1):
                self.wait(k, 4, po, 1)
                self.wait(k, 4, po, -1)
                arrived(k, po, 2)

    def finish(self):
        for message in MESSAGES:
            self.copy(message, False).wait_send()


def high_low(values):
    upper = values.astype(BF16)
    return upper, (values - upper.astype(F32)).astype(BF16)


def kernel(
    inputs,
    value_cot,
    gate_cot,
    out_cot,
    conv_output,
    factors,
    value_weight,
    gate_weight,
    out_weight,
    first_moment,
    second_moment,
    mom,
    upd,
    copies,
    inp,
    oct_,
    cots,
    cots_t,
    fbuf,
    wbuf,
    summed,
    pieces,
    arrived_pieces,
    dirs,
    sums,
    fs_sums,
    local_sem,
    f_send,
    f_recv,
    core_send,
    core_recv,
    a_send,
    a_recv,
    d_send,
    d_recv,
    s_send,
    s_recv,
    q_send,
    q_recv,
    c_send,
    c_recv,
):
    me = lax.axis_index("fs")
    t = lax.axis_index("tp")
    core = lax.rem(t, 2)
    partner = t + 1 - 2 * core

    loads = []

    def load(src, dst):
        copy = pltpu.make_async_copy(src, dst, local_sem.at[len(loads)])
        copy.start()
        loads.append(copy)

    load(factors, fbuf.at[me])
    load(value_cot, cots.at[0])
    load(gate_cot, cots.at[1])
    load(conv_output, cots.at[2])
    load(inputs, inp)
    load(out_cot, oct_)
    load(first_moment, mom.at[0])
    load(second_moment, mom.at[1])
    load(value_weight, wbuf.at[0])
    load(gate_weight, wbuf.at[1])
    load(out_weight, wbuf.at[2])

    barrier = pltpu.get_barrier_semaphore()

    def greet_fs(j, _):
        pl.semaphore_signal(
            barrier, inc=1, device_id={"fs": lax.rem(me + j, FS)}, device_id_type=MESH
        )
        return _

    def greet_tp(j, _):
        pl.semaphore_signal(
            barrier, inc=1, device_id={"tp": lax.rem(t + j, TP)}, device_id_type=MESH
        )
        return _

    lax.fori_loop(1, FS, greet_fs, 0)
    lax.fori_loop(1, TP, greet_tp, 0)

    with jax.named_scope("turn"):
        for copy in loads[1:4]:
            copy.wait()
        for m in range(3):

            def turn(i, _):
                rows = pl.ds(pl.multiple_of(i * 256, 256), 256)
                cots_t[m, :, rows] = cots[m, rows, :].T
                return _

            lax.fori_loop(0, TOK // 256, turn, 0)

    with jax.named_scope("barrier"):
        pl.semaphore_wait(barrier, FS - 1 + TP - 1)

    def factor_part(of_core):
        def part(s, k, half):
            at = of_core * 128 + 64 * k
            size = 64
            if half is not None:
                at, size = at + 32 * half, 32
            return fbuf.at[s, :, pl.ds(pl.multiple_of(at, 32), size), :]

        return part

    ring = RingGather(me, factor_part(core), f_send, f_recv)

    def share(k, po, qo, mine):
        at = (po + 1) * SIDE + (qo + 1) + FS * k
        ref = factor_part(core if mine else 1 - core)(ring.slot(k, po, qo), k, None)
        return pltpu.make_async_remote_copy(
            src_ref=ref,
            dst_ref=ref,
            send_sem=core_send.at[at],
            recv_sem=core_recv.at[at],
            device_id={"tp": partner},
            device_id_type=MESH,
        )

    def multiply(s, first):
        cols = pl.ds(pl.multiple_of(s * W, W), W)

        def tile(i, _):
            rows = pl.ds(pl.multiple_of(i * 512, 512), 512)
            left = inp[rows, cols]
            other = oct_[rows, cols]
            for m in range(3):
                product = jnp.dot(
                    other if m == 2 else left, fbuf[s, m], preferred_element_type=F32
                )
                if first:
                    summed[m, rows, :] = product
                else:
                    summed[m, rows, :] += product
            return _

        with jax.named_scope("multiply"):
            lax.fori_loop(0, TOK // 512, tile, 0)

    loads[0].wait()
    halves = set()
    waiting = []

    def multiply_next():
        if not waiting:
            return
        offsets = waiting.pop(0)
        if offsets is None:
            with jax.named_scope("wait_loads"):
                loads[4].wait()
                loads[5].wait()
            multiply(me, True)
            return
        dx, dz = offsets
        with jax.named_scope("wait_share"):
            share(0, dx, dz, False).wait_recv()
            share(1, dz, dx, False).wait_recv()
        multiply(ring.slot(0, dx, dz), False)

    waiting.append(None)

    def on_factor(k, po, qo):
        share(k, po, qo, True).start()
        offsets = (po, qo) if k == 0 else (qo, po)
        if offsets not in halves:
            halves.add(offsets)
            return
        multiply_next()
        waiting.append(offsets)

    ring.run(on_factor)
    while waiting:
        multiply_next()

    for m in range(3):
        with jax.named_scope("project"):
            upper, lower = high_low(summed[m])
            product = jnp.dot(cots_t[m], upper, preferred_element_type=F32)
            product += jnp.dot(cots_t[m], lower, preferred_element_type=F32)
            pieces[:, m, :, :] = product.T.reshape(FS, RS, W)

    def to_owner(j):
        peer = lax.rem(me + j, FS)
        return pltpu.make_async_remote_copy(
            src_ref=pieces.at[peer],
            dst_ref=arrived_pieces.at[me],
            send_sem=a_send.at[j],
            recv_sem=a_recv.at[j],
            device_id={"fs": peer},
            device_id_type=MESH,
        )

    def from_peer(j):
        source = lax.rem(me - j + FS, FS)
        return pltpu.make_async_remote_copy(
            src_ref=pieces.at[source],
            dst_ref=arrived_pieces.at[source],
            send_sem=a_send.at[j],
            recv_sem=a_recv.at[j],
            device_id={"fs": source},
            device_id_type=MESH,
        )

    def loop(start, stop, step):
        def body(j, carry):
            step(j)
            return carry

        lax.fori_loop(start, stop, body, 0)

    loop(1, FS, lambda j: to_owner(j).start())

    def add_piece(j, total):
        from_peer(j).wait_recv()
        return total + arrived_pieces[lax.rem(me - j + FS, FS)]

    with jax.named_scope("sum_pieces"):
        projected = lax.fori_loop(1, FS, add_piece, pieces[me])

    loads[6].wait()
    loads[7].wait()
    new_first = FIRST_DECAY * mom[0] + (1.0 - FIRST_DECAY) * projected
    new_second = SECOND_DECAY * mom[1] + (1.0 - SECOND_DECAY) * projected * projected
    dirs[me] = new_first / (jnp.sqrt(new_second) + DIVISOR_EPS)
    mom[0] = new_first
    mom[1] = new_second

    def direction(j, received):
        source = lax.rem(me - j + FS, FS) if received else me
        return pltpu.make_async_remote_copy(
            src_ref=dirs.at[source],
            dst_ref=dirs.at[source],
            send_sem=d_send.at[j],
            recv_sem=d_recv.at[j],
            device_id={"fs": lax.rem(me + j, FS)},
            device_id_type=MESH,
        )

    loop(1, FS, lambda j: direction(j, False).start())

    own = dirs[me].reshape(3 * RS // 8, 8, W)
    squares = jnp.sum(own * own, axis=0)
    sums[t] = squares[:, :128] + squares[:, 128:]

    def scalar(j, received):
        source = lax.rem(t - j + TP, TP) if received else t
        return pltpu.make_async_remote_copy(
            src_ref=sums.at[source],
            dst_ref=sums.at[source],
            send_sem=s_send.at[j],
            recv_sem=s_recv.at[j],
            device_id={"tp": lax.rem(t + j, TP)},
            device_id_type=MESH,
        )

    def fs_scalar(j, received):
        source = lax.rem(me - j + FS, FS) if received else me
        return pltpu.make_async_remote_copy(
            src_ref=fs_sums.at[source],
            dst_ref=fs_sums.at[source],
            send_sem=q_send.at[j],
            recv_sem=q_recv.at[j],
            device_id={"fs": lax.rem(me + j, FS)},
            device_id_type=MESH,
        )

    loop(1, TP, lambda j: scalar(j, False).start())
    with jax.named_scope("wait_scalar"):
        loop(1, TP, lambda j: scalar(j, True).wait_recv())
    fs_sums[me] = jnp.sum(sums[...], axis=0)
    loop(1, FS, lambda j: fs_scalar(j, False).start())
    with jax.named_scope("wait_directions"):
        loop(1, FS, lambda j: direction(j, True).wait_recv())

    for m in range(3):
        whole = dirs[:, m, :, :].reshape(RANK, W)
        if m == 2:
            upper, lower = high_low(whole.T)
            contract = (((1,), (1,)), ((), ()))
            own = fbuf[me, m]
            update = lax.dot_general(upper, own, contract, preferred_element_type=F32)
            update += lax.dot_general(lower, own, contract, preferred_element_type=F32)
        else:
            upper, lower = high_low(whole)
            update = jnp.dot(fbuf[me, m], upper, preferred_element_type=F32)
            update += jnp.dot(fbuf[me, m], lower, preferred_element_type=F32)
        upd[m] = update
    for copy in loads[8:]:
        copy.wait()
    with jax.named_scope("wait_fs_scalar"):
        loop(1, FS, lambda j: fs_scalar(j, True).wait_recv())
    total = jnp.sum(jnp.sum(fs_sums[...], axis=0), keepdims=True)
    norm_scale = lax.rsqrt(total / (3 * RANK * C) + SQUARE_EPS)
    for m in range(3):
        update = norm_scale * upd[m]
        upd[m] = update
        copies[me, m] = (wbuf[m] - LEARN_RATE * update).astype(BF16)

    def copy_part(s, k, half):
        at, size = 128 * k, 128
        if half is not None:
            at, size = at + 64 * half, 64
        return copies.at[s, :, pl.ds(at, size), :]

    gather = RingGather(me, copy_part, c_send, c_recv)

    gather.run(lambda k, po, qo: None)

    with jax.named_scope("finish"):
        gather.finish()
    with jax.named_scope("finish_rest"):
        ring.finish()
        for k in (0, 1):
            for po in (-1, 0, 1, 2):
                for qo in (-1, 0, 1, 2):
                    if (po, qo) != (0, 0):
                        share(k, po, qo, True).wait_send()
        loop(1, FS, lambda j: to_owner(j).wait_send())
        loop(1, FS, lambda j: direction(j, False).wait_send())
        loop(1, TP, lambda j: scalar(j, False).wait_send())
        loop(1, FS, lambda j: fs_scalar(j, False).wait_send())


def store_kernel(
    mom,
    upd,
    copies,
    first_out,
    second_out,
    value_update,
    gate_update,
    out_update,
    value_copy,
    gate_copy,
    out_copy,
    sem,
    block_sem,
):
    small = [
        pltpu.make_async_copy(src, dst, sem.at[i])
        for i, (src, dst) in enumerate(
            (
                (mom.at[0], first_out),
                (mom.at[1], second_out),
                (upd.at[0], value_update),
                (upd.at[1], gate_update),
                (upd.at[2], out_update),
            )
        )
    ]

    def block(s):
        at = pl.ds(pl.multiple_of(s * W, W), W)
        return [
            pltpu.make_async_copy(copies.at[s, 0], value_copy.at[at, :], block_sem.at[s, 0]),
            pltpu.make_async_copy(copies.at[s, 1], gate_copy.at[at, :], block_sem.at[s, 1]),
            pltpu.make_async_copy(copies.at[s, 2], out_copy.at[:, at], block_sem.at[s, 2]),
        ]

    def start(s, carry):
        for copy in block(s):
            copy.start()
        return carry

    def wait(s, carry):
        for copy in block(s):
            copy.wait()
        return carry

    for copy in small:
        copy.start()
    lax.fori_loop(0, FS, start, 0)
    lax.fori_loop(0, FS, wait, 0)
    for copy in small:
        copy.wait()


def shards(*args):
    anywhere = pl.BlockSpec(memory_space=pl.ANY)
    vmem = pl.BlockSpec(memory_space=pltpu.VMEM)
    dma = pltpu.SemaphoreType.DMA
    results = pl.pallas_call(
        kernel,
        out_shape=(
            pltpu.VMEM((2, 3, RS, W), F32),
            pltpu.VMEM((3, W, W), F32),
            pltpu.VMEM((FS, 3, W, W), BF16),
        ),
        in_specs=[anywhere] * 11,
        out_specs=(vmem,) * 3,
        scratch_shapes=[
            pltpu.VMEM((TOK, D), BF16),
            pltpu.VMEM((TOK, D), BF16),
            pltpu.VMEM((3, TOK, W), BF16),
            pltpu.VMEM((3, W, TOK), BF16),
            pltpu.VMEM((FS, 3, W, RANK), BF16),
            pltpu.VMEM((3, W, W), F32),
            pltpu.VMEM((3, TOK, RANK), F32),
            pltpu.VMEM((FS, 3, RS, W), F32),
            pltpu.VMEM((FS, 3, RS, W), F32),
            pltpu.VMEM((FS, 3, RS, W), F32),
            pltpu.VMEM((TP, 8, 128), F32),
            pltpu.VMEM((FS, 8, 128), F32),
            dma((11,)),
            dma((COUNT,)),
            dma((COUNT,)),
            dma((2 * FS,)),
            dma((2 * FS,)),
            dma((FS,)),
            dma((FS,)),
            dma((FS,)),
            dma((FS,)),
            dma((TP,)),
            dma((TP,)),
            dma((FS,)),
            dma((FS,)),
            dma((COUNT,)),
            dma((COUNT,)),
        ],
        compiler_params=pltpu.CompilerParams(
            collective_id=0, has_side_effects=True, vmem_limit_bytes=48 * 1024 * 1024
        ),
    )(*[pltpu.with_memory_space_constraint(a, pltpu.HBM) for a in args])
    return pl.pallas_call(
        store_kernel,
        out_shape=(
            jax.ShapeDtypeStruct((3, RS, W), F32),
            jax.ShapeDtypeStruct((3, RS, W), F32),
            jax.ShapeDtypeStruct((W, W), F32),
            jax.ShapeDtypeStruct((W, W), F32),
            jax.ShapeDtypeStruct((W, W), F32),
            jax.ShapeDtypeStruct((D, W), BF16),
            jax.ShapeDtypeStruct((D, W), BF16),
            jax.ShapeDtypeStruct((W, D), BF16),
        ),
        in_specs=[vmem] * 3,
        out_specs=(anywhere,) * 8,
        scratch_shapes=[dma((5,)), dma((FS, 3))],
        compiler_params=pltpu.CompilerParams(vmem_limit_bytes=4 * 1024 * 1024),
    )(*[pltpu.with_memory_space_constraint(r, pltpu.VMEM) for r in results])


def solution(mesh):
    placed = (
        P("fs", None),
        P("fs", "tp"),
        P("fs", "tp"),
        P("fs", None),
        P("fs", "tp"),
        P(None, "fs", None),
        P("fs", "tp"),
        P("fs", "tp"),
        P("tp", "fs"),
        P(None, "fs", "tp"),
        P(None, "fs", "tp"),
    )
    return jax.shard_map(
        shards,
        mesh=mesh,
        in_specs=placed,
        out_specs=(
            P(None, "fs", "tp"),
            P(None, "fs", "tp"),
            P("fs", "tp"),
            P("fs", "tp"),
            P("tp", "fs"),
            P(None, "tp"),
            P(None, "tp"),
            P("tp", None),
        ),
        check_vma=False,
    )
```

```python
import functools

import jax
import jax.numpy as jnp
from jax import lax
from jax.experimental import pallas as pl
from jax.experimental.pallas import tpu as pltpu
from jax.sharding import PartitionSpec as P

C = 2048
RANK = 256
FIRST_DECAY = 0.9
SECOND_DECAY = 0.95
DIVISOR_EPS = 1e-08
SQUARE_EPS = 1e-06
LEARN_RATE = 0.01

SIDE = 4
FS = SIDE * SIDE
TP = 8
W = 256
RS = RANK // FS
TOK = 1024
D = 4096
MESH = pl.DeviceIdType.MESH
F32 = jnp.float32
BF16 = jnp.bfloat16

RECEIVED = []
for _k in (0, 1):
    RECEIVED += [(_k, 1, 0, 1), (_k, 1, 0, -1), (_k, 2, 0, 0)]
    for _po in (0, -1, 1, 2):
        RECEIVED += [(_k, 3, _po, 1), (_k, 3, _po, -1), (_k, 4, _po, 0)]
INDEX = {message: at for at, message in enumerate(RECEIVED)}


PRODUCTS = {"3_0": 3, "2": 1, "3_1": 2, "4_0": 2, "3_2": 2, "4_-1": 1, "4_1": 1}


class RingGather:
    def __init__(self, me, part, send, recv):
        self.z, self.x = me // SIDE, lax.rem(me, SIDE)
        self.part, self.send, self.recv = part, send, recv

    def slot(self, k, po, qo):
        dx, dz = (po, qo) if k == 0 else (qo, po)
        z = lax.rem(self.z + dz + SIDE, SIDE)
        x = lax.rem(self.x + dx + SIDE, SIDE)
        return z * SIDE + x

    def copy(self, ref, k, stage, po, d, to):
        sem = self.recv.at[INDEX[k, stage, po, 0 if stage in (2, 4) else d]]
        return pltpu.make_async_remote_copy(
            src_ref=ref,
            dst_ref=ref,
            send_sem=self.send,
            recv_sem=sem,
            device_id={"fs": to},
            device_id_type=MESH,
        )

    def start(self, k, stage, po, d):
        first = stage in (1, 2)
        at = {1: (0, 0), 2: (-d, 0), 3: (po, 0), 4: (po, -d)}[stage]
        half = None if stage in (1, 3) else (0 if d > 0 else 1)
        to = self.slot(k, d, 0) if first else self.slot(k, 0, d)
        ref = self.part(self.slot(k, *at), k, half)
        self.copy(ref, k, stage, po, d, to).start()

    def wait(self, k, stage, po, d=0):
        at = {1: (-d, 0), 2: (2, 0), 3: (po, -d), 4: (po, 2)}[stage]
        ref = self.part(self.slot(k, *at), k, None)
        with jax.named_scope(f"wait_{k}_{stage}_{po}_{d}"):
            self.copy(ref, k, stage, po, d, self.slot(k, 1, 0)).wait_recv()

    def run(self, arrived, after):
        for stage in (1, 3):
            for d in (1, -1):
                for k in (0, 1):
                    self.start(k, stage, 0, d)
        after("start")
        for d in (1, -1):
            for k in (0, 1):
                self.wait(k, 1, 0, d)
                self.start(k, 2, 0, d)
                self.start(k, 3, -d, 1)
                self.start(k, 3, -d, -1)
                arrived(k, -d, 0)
        self.second(arrived, 0)
        after("3_0")
        for k in (0, 1):
            self.wait(k, 2, 0)
            self.start(k, 3, 2, 1)
            self.start(k, 3, 2, -1)
            arrived(k, 2, 0)
        after("2")
        for po in (-1, 1):
            self.second(arrived, po)
            after(f"3_{po}")
        self.last(arrived, 0)
        after("4_0")
        self.second(arrived, 2)
        after("3_2")
        for po in (-1, 1, 2):
            self.last(arrived, po)
            after(f"4_{po}")

    def second(self, arrived, po):
        for d in (1, -1):
            for k in (0, 1):
                self.wait(k, 3, po, d)
                self.start(k, 4, po, d)
                arrived(k, po, -d)

    def last(self, arrived, po):
        for k in (0, 1):
            self.wait(k, 4, po)
            arrived(k, po, 2)

    def finish(self, everything):
        self.copy(everything, 0, 1, 0, 1, self.slot(0, 1, 0)).wait_send()


def high_low(values):
    upper = values.astype(BF16)
    return upper, (values - upper.astype(F32)).astype(BF16)


def kernel(
    inputs,
    value_cot,
    gate_cot,
    out_cot,
    conv_output,
    factors,
    value_weight,
    gate_weight,
    out_weight,
    first_moment,
    second_moment,
    mom,
    upd,
    copies,
    inp,
    oct_,
    cots,
    cots_t,
    fbuf,
    wbuf,
    summed,
    pieces,
    arrived,
    dirs,
    sums,
    fs_sums,
    load_sem,
    ring_send,
    ring_recv,
    core_send,
    core_recv,
    a_send,
    a_recv,
    d_send,
    d_recv,
    s_send,
    s_recv,
):
    me = lax.axis_index("fs")
    t = lax.axis_index("tp")
    core = lax.rem(t, 2)
    partner = t + 1 - 2 * core

    def load(at, *pairs):
        for src, dst in pairs:
            pltpu.make_async_copy(src, dst, load_sem.at[at]).start()

    def loaded(at, ref):
        pltpu.make_async_copy(ref, ref, load_sem.at[at]).wait()

    load(0, (factors, fbuf.at[me]))
    load(1, *((r, cots.at[m]) for m, r in enumerate((value_cot, gate_cot, conv_output))))
    load(2, (inputs, inp))
    load(3, (out_cot, oct_))
    load(4, (first_moment, mom.at[0]), (second_moment, mom.at[1]))
    load(5, *((r, wbuf.at[m]) for m, r in enumerate((value_weight, gate_weight, out_weight))))

    barrier = pltpu.get_barrier_semaphore()

    def greet_fs(j, _):
        pl.semaphore_signal(
            barrier, inc=1, device_id={"fs": lax.rem(me + j, FS)}, device_id_type=MESH
        )
        return _

    def greet_tp(j, _):
        pl.semaphore_signal(
            barrier, inc=1, device_id={"tp": lax.rem(t + j, TP)}, device_id_type=MESH
        )
        return _

    lax.fori_loop(1, FS, greet_fs, 0)
    lax.fori_loop(1, TP, greet_tp, 0)

    with jax.named_scope("turn"):
        loaded(1, cots)
        for m in range(3):

            def turn(i, _):
                rows = pl.ds(pl.multiple_of(i * 256, 256), 256)
                cots_t[m, :, rows] = cots[m, rows, :].T
                return _

            lax.fori_loop(0, TOK // 256, turn, 0)

    with jax.named_scope("barrier"):
        pl.semaphore_wait(barrier, FS - 1 + TP - 1)

    def factor_part(of_core):
        def part(s, k, half):
            at = of_core * 128 + 64 * k
            size = 64
            if half is not None:
                at, size = at + 32 * half, 32
            return fbuf.at[s, :, pl.ds(pl.multiple_of(at, 32), size), :]

        return part

    ring = RingGather(me, factor_part(core), ring_send.at[0], ring_recv)

    def core_copy(ref, dx, dz):
        return pltpu.make_async_remote_copy(
            src_ref=ref,
            dst_ref=ref,
            send_sem=core_send.at[0],
            recv_sem=core_recv.at[(dx + 1) * SIDE + dz + 1],
            device_id={"tp": partner},
            device_id_type=MESH,
        )

    def half_of(of_core, *slots):
        at = pl.multiple_of(of_core * 128, 128)
        return fbuf.at[(*slots, slice(None), pl.ds(at, 128), slice(None))]

    def multiply(s, first):
        cols = pl.ds(pl.multiple_of(s * W, W), W)

        def tile(i, _):
            rows = pl.ds(pl.multiple_of(i * 512, 512), 512)
            left = inp[rows, cols]
            other = oct_[rows, cols]
            for m in range(3):
                product = jnp.dot(
                    other if m == 2 else left, fbuf[s, m], preferred_element_type=F32
                )
                if first:
                    summed[m, rows, :] = product
                else:
                    summed[m, rows, :] += product
            return _

        with jax.named_scope("multiply"):
            lax.fori_loop(0, TOK // 512, tile, 0)

    loaded(0, fbuf.at[me])
    halves = set()
    waiting = []

    def multiply_next():
        dx, dz = waiting.pop(0)
        with jax.named_scope("wait_share"):
            s = ring.slot(0, dx, dz)
            core_copy(half_of(1 - core, s), dx, dz).wait_recv()
        multiply(s, False)

    def on_factor(k, po, qo):
        dx, dz = (po, qo) if k == 0 else (qo, po)
        core_copy(factor_part(core)(ring.slot(k, po, qo), k, None), dx, dz).start()
        if (dx, dz) in halves:
            waiting.append((dx, dz))
        halves.add((dx, dz))

    def between(group):
        if group == "start":
            with jax.named_scope("wait_loads"):
                loaded(2, inp)
                loaded(3, oct_)
            multiply(me, True)
        for _ in range(PRODUCTS.get(group, 0)):
            multiply_next()

    ring.run(on_factor, between)
    while waiting:
        multiply_next()

    def loop(start, stop, step):
        def body(j, carry):
            step(j)
            return carry

        lax.fori_loop(start, stop, body, 0)

    def to_fs(src, dst, send, recv, j):
        return pltpu.make_async_remote_copy(
            src_ref=src,
            dst_ref=dst,
            send_sem=send,
            recv_sem=recv,
            device_id={"fs": lax.rem(me + j, FS)},
            device_id_type=MESH,
        )

    others = pl.ds(0, FS - 1)

    for m in range(3):
        with jax.named_scope("project"):
            upper, lower = high_low(summed[m])
            product = jnp.dot(cots_t[m], upper, preferred_element_type=F32)
            product += jnp.dot(cots_t[m], lower, preferred_element_type=F32)
            pieces[m] = product.T.reshape(FS, RS, W)

        def send_piece(j):
            to_fs(
                pieces.at[m, lax.rem(me + j, FS)],
                arrived.at[m, me],
                a_send.at[0],
                a_recv.at[m],
                j,
            ).start()

        loop(1, FS, send_piece)
        arrived[m, me] = pieces[m, me]

    loaded(4, mom)
    squares = jnp.zeros((8, W), F32)
    for m in range(3):
        with jax.named_scope("wait_pieces"):
            ref = arrived.at[m, others]
            to_fs(ref, ref, a_send.at[0], a_recv.at[m], 1).wait_recv()
        projected = jnp.sum(arrived[m], axis=0)
        new_first = FIRST_DECAY * mom[0, m] + (1.0 - FIRST_DECAY) * projected
        new_second = (
            SECOND_DECAY * mom[1, m] + (1.0 - SECOND_DECAY) * projected * projected
        )
        direction = new_first / (jnp.sqrt(new_second) + DIVISOR_EPS)
        mom[0, m] = new_first
        mom[1, m] = new_second
        dirs[m, me] = direction

        def send_direction(j):
            ref = dirs.at[m, me]
            to_fs(ref, ref, d_send.at[0], d_recv.at[m], j).start()

        loop(1, FS, send_direction)
        squares += direction[:8] * direction[:8] + direction[8:] * direction[8:]

    sums[t] = squares[:, :128] + squares[:, 128:]

    def to_tp(ref, j):
        return pltpu.make_async_remote_copy(
            src_ref=ref,
            dst_ref=ref,
            send_sem=s_send.at[0],
            recv_sem=s_recv.at[0],
            device_id={"tp": lax.rem(t + j, TP)},
            device_id_type=MESH,
        )

    loop(1, TP, lambda j: to_tp(sums.at[t], j).start())

    def update(m):
        with jax.named_scope("wait_directions"):
            ref = dirs.at[m, others]
            to_fs(ref, ref, d_send.at[0], d_recv.at[m], 1).wait_recv()
        whole = dirs[m].reshape(RANK, W)
        if m == 2:
            upper, lower = high_low(whole.T)
            contract = (((1,), (1,)), ((), ()))
            own = fbuf[me, m]
            product = lax.dot_general(upper, own, contract, preferred_element_type=F32)
            product += lax.dot_general(lower, own, contract, preferred_element_type=F32)
        else:
            upper, lower = high_low(whole)
            product = jnp.dot(fbuf[me, m], upper, preferred_element_type=F32)
            product += jnp.dot(fbuf[me, m], lower, preferred_element_type=F32)
        upd[m] = product

    update(0)
    with jax.named_scope("wait_scalar"):
        to_tp(sums.at[pl.ds(0, TP - 1)], 1).wait_recv()
    fs_sums[me] = jnp.sum(sums[...], axis=0)

    def send_sum(j):
        ref = fs_sums.at[me]
        to_fs(ref, ref, s_send.at[1], s_recv.at[1], j).start()

    loop(1, FS, send_sum)
    update(1)
    loaded(5, wbuf)
    ring.finish(half_of(0, others))
    update(2)
    with jax.named_scope("wait_fs_scalar"):
        ref = fs_sums.at[others]
        to_fs(ref, ref, s_send.at[1], s_recv.at[1], 1).wait_recv()
    total = jnp.sum(jnp.sum(fs_sums[...], axis=0), keepdims=True)
    norm_scale = lax.rsqrt(total / (3 * RANK * C) + SQUARE_EPS)
    for m in range(3):
        scaled = norm_scale * upd[m]
        upd[m] = scaled
        copies[me, m] = (wbuf[m] - LEARN_RATE * scaled).astype(BF16)

    def copy_part(s, k, half):
        at, size = 128 * k, 128
        if half is not None:
            at, size = at + 64 * half, 64
        return copies.at[s, :, pl.ds(at, size), :]

    gather = RingGather(me, copy_part, ring_send.at[0], ring_recv)
    gather.run(lambda k, po, qo: None, lambda group: None)

    with jax.named_scope("finish"):
        gather.finish(copies.at[others])
        core_copy(half_of(0, others), 0, 0).wait_send()
        for m in range(3):
            ref = pieces.at[m, others]
            to_fs(ref, ref, a_send.at[0], a_recv.at[m], 1).wait_send()
            ref = dirs.at[m, others]
            to_fs(ref, ref, d_send.at[0], d_recv.at[m], 1).wait_send()
        to_tp(sums.at[pl.ds(0, TP - 1)], 1).wait_send()
        ref = fs_sums.at[others]
        to_fs(ref, ref, s_send.at[1], s_recv.at[1], 1).wait_send()


def store_kernel(
    mom,
    upd,
    copies,
    first_out,
    second_out,
    value_update,
    gate_update,
    out_update,
    value_copy,
    gate_copy,
    out_copy,
    sem,
):
    def store(src, dst):
        pltpu.make_async_copy(src, dst, sem.at[0]).start()

    def store_block(s, carry):
        at = pl.ds(pl.multiple_of(s * W, W), W)
        store(copies.at[s, 0], value_copy.at[at, :])
        store(copies.at[s, 1], gate_copy.at[at, :])
        store(copies.at[s, 2], out_copy.at[:, at])
        return carry

    lax.fori_loop(0, FS, store_block, 0)
    store(upd.at[0], value_update)
    store(upd.at[1], gate_update)
    store(upd.at[2], out_update)
    store(mom.at[0], first_out)
    store(mom.at[1], second_out)
    for ref in (copies, upd, mom):
        pltpu.make_async_copy(ref, ref, sem.at[0]).wait()


def shards(*args):
    anywhere = pl.BlockSpec(memory_space=pl.ANY)
    vmem = pl.BlockSpec(memory_space=pltpu.VMEM)
    dma = pltpu.SemaphoreType.DMA
    results = pl.pallas_call(
        kernel,
        out_shape=(
            pltpu.VMEM((2, 3, RS, W), F32),
            pltpu.VMEM((3, W, W), F32),
            pltpu.VMEM((FS, 3, W, W), BF16),
        ),
        in_specs=[anywhere] * 11,
        out_specs=(vmem,) * 3,
        scratch_shapes=[
            pltpu.VMEM((TOK, D), BF16),
            pltpu.VMEM((TOK, D), BF16),
            pltpu.VMEM((3, TOK, W), BF16),
            pltpu.VMEM((3, W, TOK), BF16),
            pltpu.VMEM((FS, 3, W, RANK), BF16),
            pltpu.VMEM((3, W, W), F32),
            pltpu.VMEM((3, TOK, RANK), F32),
            pltpu.VMEM((3, FS, RS, W), F32),
            pltpu.VMEM((3, FS, RS, W), F32),
            pltpu.VMEM((3, FS, RS, W), F32),
            pltpu.VMEM((TP, 8, 128), F32),
            pltpu.VMEM((FS, 8, 128), F32),
            dma((6,)),
            dma((1,)),
            dma((len(RECEIVED),)),
            dma((1,)),
            dma((FS,)),
            dma((1,)),
            dma((3,)),
            dma((1,)),
            dma((3,)),
            dma((2,)),
            dma((2,)),
        ],
        compiler_params=pltpu.CompilerParams(
            collective_id=0, has_side_effects=True, vmem_limit_bytes=48 * 1024 * 1024
        ),
    )(*[pltpu.with_memory_space_constraint(a, pltpu.HBM) for a in args])
    return pl.pallas_call(
        store_kernel,
        out_shape=(
            jax.ShapeDtypeStruct((3, RS, W), F32),
            jax.ShapeDtypeStruct((3, RS, W), F32),
            jax.ShapeDtypeStruct((W, W), F32),
            jax.ShapeDtypeStruct((W, W), F32),
            jax.ShapeDtypeStruct((W, W), F32),
            jax.ShapeDtypeStruct((D, W), BF16),
            jax.ShapeDtypeStruct((D, W), BF16),
            jax.ShapeDtypeStruct((W, D), BF16),
        ),
        in_specs=[vmem] * 3,
        out_specs=(anywhere,) * 8,
        scratch_shapes=[dma((1,))],
        compiler_params=pltpu.CompilerParams(vmem_limit_bytes=4 * 1024 * 1024),
    )(*[pltpu.with_memory_space_constraint(r, pltpu.VMEM) for r in results])


def solution(mesh):
    placed = (
        P("fs", None),
        P("fs", "tp"),
        P("fs", "tp"),
        P("fs", None),
        P("fs", "tp"),
        P(None, "fs", None),
        P("fs", "tp"),
        P("fs", "tp"),
        P("tp", "fs"),
        P(None, "fs", "tp"),
        P(None, "fs", "tp"),
    )
    return jax.shard_map(
        shards,
        mesh=mesh,
        in_specs=placed,
        out_specs=(
            P(None, "fs", "tp"),
            P(None, "fs", "tp"),
            P("fs", "tp"),
            P("fs", "tp"),
            P("tp", "fs"),
            P(None, "tp"),
            P(None, "tp"),
            P("tp", None),
        ),
        check_vma=False,
    )
```

```python
import functools

import jax
import jax.numpy as jnp
from jax import lax
from jax.experimental import pallas as pl
from jax.experimental.pallas import tpu as pltpu
from jax.sharding import PartitionSpec as P

C = 2048
RANK = 256
FIRST_DECAY = 0.9
SECOND_DECAY = 0.95
DIVISOR_EPS = 1e-08
SQUARE_EPS = 1e-06
LEARN_RATE = 0.01

SIDE = 4
FS = SIDE * SIDE
TP = 8
HALF = 128
W = 256
RS = RANK // FS
TOK = 1024
D = 4096
MESH = pl.DeviceIdType.MESH
F32 = jnp.float32
BF16 = jnp.bfloat16

RECEIVED = []
for _k in (0, 1):
    RECEIVED += [(_k, 1, 0, 1), (_k, 1, 0, -1), (_k, 2, 0, 0)]
    for _po in (0, -1, 1, 2):
        RECEIVED += [(_k, 3, _po, 1), (_k, 3, _po, -1), (_k, 4, _po, 0)]
INDEX = {message: at for at, message in enumerate(RECEIVED)}


class RingGather:
    def __init__(self, name, me, part, send, recv):
        self.name = name
        self.z, self.x = me // SIDE, lax.rem(me, SIDE)
        self.part, self.send, self.recv = part, send, recv

    def slot(self, k, po, qo):
        dx, dz = (po, qo) if k == 0 else (qo, po)
        z = lax.rem(self.z + dz + SIDE, SIDE)
        x = lax.rem(self.x + dx + SIDE, SIDE)
        return z * SIDE + x

    def copy(self, ref, k, stage, po, d, to):
        sem = self.recv.at[INDEX[k, stage, po, 0 if stage in (2, 4) else d]]
        return pltpu.make_async_remote_copy(
            src_ref=ref,
            dst_ref=ref,
            send_sem=self.send,
            recv_sem=sem,
            device_id={"fs": to},
            device_id_type=MESH,
        )

    def start(self, k, stage, po, d):
        first = stage in (1, 2)
        at = {1: (0, 0), 2: (-d, 0), 3: (po, 0), 4: (po, -d)}[stage]
        half = None if stage in (1, 3) else (0 if d > 0 else 1)
        to = self.slot(k, d, 0) if first else self.slot(k, 0, d)
        ref = self.part(self.slot(k, *at), k, half)
        self.copy(ref, k, stage, po, d, to).start()

    def wait(self, k, stage, po, d=0):
        at = {1: (-d, 0), 2: (2, 0), 3: (po, -d), 4: (po, 2)}[stage]
        ref = self.part(self.slot(k, *at), k, None)
        with jax.named_scope(f"w{self.name}_{k}_{stage}_{po}_{d}"):
            self.copy(ref, k, stage, po, d, self.slot(k, 1, 0)).wait_recv()

    def steps(self, arrived):
        for stage in (1, 3):
            for d in (1, -1):
                for k in (0, 1):
                    self.start(k, stage, 0, d)
        yield "start"
        for d in (1, -1):
            for k in (0, 1):
                self.wait(k, 1, 0, d)
                self.start(k, 2, 0, d)
                arrived(k, -d, 0)
        for po in (-1, 1):
            for d in (1, -1):
                for k in (0, 1):
                    self.start(k, 3, po, d)
        yield "1"
        self.second(arrived, 0)
        yield "3_0"
        for k in (0, 1):
            self.wait(k, 2, 0)
            self.start(k, 3, 2, 1)
            self.start(k, 3, 2, -1)
            arrived(k, 2, 0)
        yield "2"
        for po in (-1, 1):
            self.second(arrived, po)
            yield f"3_{po}"
        self.last(arrived, 0)
        yield "4_0"
        self.second(arrived, 2)
        yield "3_2"
        for po in (-1, 1, 2):
            self.last(arrived, po)
            yield f"4_{po}"

    def second(self, arrived, po):
        for d in (1, -1):
            for k in (0, 1):
                self.wait(k, 3, po, d)
                self.start(k, 4, po, d)
                arrived(k, po, -d)

    def last(self, arrived, po):
        for k in (0, 1):
            self.wait(k, 4, po)
            arrived(k, po, 2)

    def finish(self, everything):
        self.copy(everything, 0, 1, 0, 1, self.slot(0, 1, 0)).wait_send()


def high_low(values):
    upper = values.astype(BF16)
    return upper, (values - upper.astype(F32)).astype(BF16)


def kernel(
    inputs,
    value_cot,
    gate_cot,
    out_cot,
    conv_output,
    factors,
    value_weight,
    gate_weight,
    out_weight,
    first_moment,
    second_moment,
    mom,
    upd,
    copies,
    left,
    cots,
    cots_t,
    fbuf,
    fown,
    wbuf,
    summed,
    pieces,
    from_core,
    arrived,
    dirs,
    sums,
    fs_sums,
    load_sem,
    ring_send,
    ring_recv,
    core_send,
    core_recv,
    a_send,
    a_recv,
    d_send,
    d_recv,
    s_send,
    s_recv,
):
    me = lax.axis_index("fs")
    t = lax.axis_index("tp")
    core = lax.rem(t, 2)
    partner = t + 1 - 2 * core

    def load(at, *pairs):
        for src, dst in pairs:
            pltpu.make_async_copy(src, dst, load_sem.at[at]).start()

    def loaded(at, ref):
        pltpu.make_async_copy(ref, ref, load_sem.at[at]).wait()

    half = pl.ds(pl.multiple_of(core * HALF, HALF), HALF)
    load(0, (factors.at[:, half, :], fbuf.at[me]))
    load(1, *((r, cots.at[m]) for m, r in enumerate((value_cot, gate_cot, conv_output))))

    def load_half(s, carry):
        src = pl.ds(pl.multiple_of(s * W + core * HALF, HALF), HALF)
        dst = pl.ds(pl.multiple_of(s * HALF, HALF), HALF)
        load(2, (inputs.at[:, src], left.at[0, :, dst]))
        load(3, (out_cot.at[:, src], left.at[1, :, dst]))
        return carry

    lax.fori_loop(0, FS, load_half, 0)
    load(4, (first_moment, mom.at[0]), (second_moment, mom.at[1]))
    load(5, *((r, wbuf.at[m]) for m, r in enumerate((value_weight, gate_weight, out_weight))))
    load(6, (factors, fown))

    barrier = pltpu.get_barrier_semaphore()

    def greet_fs(j, _):
        pl.semaphore_signal(
            barrier, inc=1, device_id={"fs": lax.rem(me + j, FS)}, device_id_type=MESH
        )
        return _

    def greet_tp(j, _):
        pl.semaphore_signal(
            barrier, inc=1, device_id={"tp": lax.rem(t + j, TP)}, device_id_type=MESH
        )
        return _

    lax.fori_loop(1, FS, greet_fs, 0)
    lax.fori_loop(1, TP, greet_tp, 0)

    with jax.named_scope("turn"):
        loaded(1, cots)
        for m in range(3):

            def turn(i, _):
                rows = pl.ds(pl.multiple_of(i * 256, 256), 256)
                cots_t[0, m, :, rows] = cots[m, rows, :].T
                return _

            lax.fori_loop(0, TOK // 256, turn, 0)

    with jax.named_scope("barrier"):
        pl.semaphore_wait(barrier, FS - 1 + TP - 1)

    def to_partner(src, dst, at):
        return pltpu.make_async_remote_copy(
            src_ref=src,
            dst_ref=dst,
            send_sem=core_send.at[0],
            recv_sem=core_recv.at[at],
            device_id={"tp": partner},
            device_id_type=MESH,
        )

    def factor_part(s, k, half):
        at, size = 64 * k, 64
        if half is not None:
            at, size = at + 32 * half, 32
        return fbuf.at[s, pl.ds(odd_base, 2), pl.ds(at, size), :]

    y = t // 2
    odd = lax.rem(y, 2)
    odd_base = 1 - odd
    lacking, handed = 2 * odd, 2 - 2 * odd

    def along_y(ref, k):
        return pltpu.make_async_remote_copy(
            src_ref=ref,
            dst_ref=ref,
            send_sem=core_send.at[1],
            recv_sem=core_recv.at[4],
            device_id={"tp": lax.rem(t + (2 if k == 0 else TP - 2), TP)},
            device_id_type=MESH,
        )

    ring = RingGather("a", me, factor_part, ring_send.at[0], ring_recv)
    parts_here, waiting = set(), []

    def factor_arrived(k, po, qo):
        dx, dz = (po, qo) if k == 0 else (qo, po)
        s = ring.slot(0, dx, dz)
        along_y(fbuf.at[s, handed, pl.ds(64 * k, 64), :], k).start()
        if (dx, dz) in parts_here:
            waiting.append(s)
        parts_here.add((dx, dz))

    def multiply(*slots, first=False):
        with jax.named_scope("multiply"):
            for m in (odd_base, odd_base + 1):
                ours = [
                    left[m // 2, :, pl.ds(pl.multiple_of(s * HALF, HALF), HALF)]
                    for s in slots
                ]
                product = jnp.dot(
                    jnp.concatenate(ours, axis=1),
                    jnp.concatenate([fbuf[s, m] for s in slots], axis=0),
                    preferred_element_type=F32,
                )
                if first:
                    summed[m] = product
                else:
                    summed[m] += product

    def multiply_lacking():
        with jax.named_scope("multiply_lacking"):
            right = fbuf[:, lacking].reshape(D // 2, RANK)

            def tile(i, carry):
                rows = pl.ds(pl.multiple_of(i * 256, 256), 256)
                ours = left[lacking // 2, rows, :]
                summed[lacking, rows, :] = jnp.dot(ours, right, preferred_element_type=F32)
                return carry

            lax.fori_loop(0, TOK // 256, tile, 0)

    def loop(start, stop, step):
        def body(j, carry):
            step(j)
            return carry

        lax.fori_loop(start, stop, body, 0)

    def to_fs(src, dst, send, recv, j):
        return pltpu.make_async_remote_copy(
            src_ref=src,
            dst_ref=dst,
            send_sem=send,
            recv_sem=recv,
            device_id={"fs": lax.rem(me + j, FS)},
            device_id_type=MESH,
        )

    others = pl.ds(0, FS - 1)

    def project(m):
        with jax.named_scope("project"):
            split = jnp.concatenate(high_low(summed[m]), axis=1)
            turned = cots_t[:, m].reshape(2 * W, TOK)
            product = jnp.dot(turned, split, preferred_element_type=F32)
            product = product[:, :RANK] + product[:, RANK:]
            pieces[1, m] = product[W:].T.reshape(FS, RS, W)
            to_partner(pieces.at[1, m], from_core.at[m], m).start()
            pieces[0, m] = product[:W].T.reshape(FS, RS, W)

    def send_pieces(m):
        with jax.named_scope("wait_core"):
            to_partner(pieces.at[1, m], from_core.at[m], m).wait_recv()
        pieces[0, m] += from_core[m]

        def send_piece(j):
            to_fs(
                pieces.at[0, m, lax.rem(me + j, FS)],
                arrived.at[m, me],
                a_send.at[0],
                a_recv.at[m],
                j,
            ).start()

        loop(1, FS, send_piece)
        arrived[m, me] = pieces[0, m, me]

    squares = []

    def moments(m):
        with jax.named_scope("wait_pieces"):
            ref = arrived.at[m, others]
            to_fs(ref, ref, a_send.at[0], a_recv.at[m], 1).wait_recv()
        projected = jnp.sum(arrived[m], axis=0)
        new_first = FIRST_DECAY * mom[0, m] + (1.0 - FIRST_DECAY) * projected
        new_second = (
            SECOND_DECAY * mom[1, m] + (1.0 - SECOND_DECAY) * projected * projected
        )
        direction = new_first / (jnp.sqrt(new_second) + DIVISOR_EPS)
        mom[0, m] = new_first
        mom[1, m] = new_second
        dirs[m, me] = direction

        def send_direction(j):
            ref = dirs.at[m, me]
            to_fs(ref, ref, d_send.at[0], d_recv.at[m], j).start()

        loop(1, FS, send_direction)
        squares.append(direction[:8] * direction[:8] + direction[8:] * direction[8:])

    loaded(0, fbuf.at[me])
    groups = ring.steps(factor_arrived)

    def to(group):
        while next(groups) != group:
            pass

    to("start")
    to_partner(cots_t.at[0], cots_t.at[1], 3).start()
    with jax.named_scope("wait_loads"):
        loaded(2, left.at[0])
        loaded(3, left.at[1])
    multiply(me, first=True)
    for group in ("2", "4_0", "4_-1", "4_2"):
        to(group)
        multiply(*waiting)
        waiting.clear()
    to_partner(cots_t.at[0], cots_t.at[1], 3).wait_recv()
    order = (odd_base, odd_base + 1, lacking)
    project(order[0])
    project(order[1])
    send_pieces(order[0])
    with jax.named_scope("wait_y"):
        along_y(fbuf.at[others, 0], 0).wait_recv()
    multiply_lacking()
    send_pieces(order[1])
    project(order[2])
    send_pieces(order[2])
    loaded(4, mom)
    for m in order:
        moments(m)

    square = squares[0] + squares[1] + squares[2]
    sums[t] = square[:, :128] + square[:, 128:]

    def to_tp(ref, j):
        return pltpu.make_async_remote_copy(
            src_ref=ref,
            dst_ref=ref,
            send_sem=s_send.at[0],
            recv_sem=s_recv.at[0],
            device_id={"tp": lax.rem(t + j, TP)},
            device_id_type=MESH,
        )

    loop(1, TP, lambda j: to_tp(sums.at[t], j).start())

    def wait_directions(m):
        with jax.named_scope("wait_directions"):
            ref = dirs.at[m, others]
            to_fs(ref, ref, d_send.at[0], d_recv.at[m], 1).wait_recv()

    def update(m):
        full = dirs[m].reshape(RANK, W)
        if m == 2:
            upper, lower = high_low(full.T)
            contract = (((1,), (1,)), ((), ()))
            own = fown[m]
            product = lax.dot_general(upper, own, contract, preferred_element_type=F32)
            product += lax.dot_general(lower, own, contract, preferred_element_type=F32)
        else:
            upper, lower = high_low(full)
            product = jnp.dot(fown[m], upper, preferred_element_type=F32)
            product += jnp.dot(fown[m], lower, preferred_element_type=F32)
        upd[m] = product

    loaded(6, fown)
    loaded(5, wbuf)
    wait_directions(order[0])
    with jax.named_scope("wait_scalar"):
        to_tp(sums.at[pl.ds(0, TP - 1)], 1).wait_recv()
    fs_sums[me] = jnp.sum(sums[...], axis=0)

    def send_sum(j):
        ref = fs_sums.at[me]
        to_fs(ref, ref, s_send.at[1], s_recv.at[1], j).start()

    loop(1, FS, send_sum)
    wait_directions(order[1])
    update(1)
    ring.finish(fbuf.at[others, pl.ds(0, 2)])
    along_y(fbuf.at[others, 0], 0).wait_send()
    wait_directions(order[2])
    update(0)
    update(2)
    with jax.named_scope("wait_fs_scalar"):
        ref = fs_sums.at[others]
        to_fs(ref, ref, s_send.at[1], s_recv.at[1], 1).wait_recv()
    total = jnp.sum(jnp.sum(fs_sums[...], axis=0), keepdims=True)
    norm_scale = lax.rsqrt(total / (3 * RANK * C) + SQUARE_EPS)
    for m in range(3):
        scaled = norm_scale * upd[m]
        upd[m] = scaled
        copies[me, m] = (wbuf[m] - LEARN_RATE * scaled).astype(BF16)

    def copy_part(s, k, half):
        at, size = 128 * k, 128
        if half is not None:
            at, size = at + 64 * half, 64
        return copies.at[s, :, pl.ds(at, size), :]

    gather = RingGather("c", me, copy_part, ring_send.at[0], ring_recv)
    for _ in gather.steps(lambda k, po, qo: None):
        pass

    with jax.named_scope("finish"):
        gather.finish(copies.at[others])
        to_partner(cots_t.at[0], cots_t.at[1], 3).wait_send()
        for m in range(3):
            to_partner(pieces.at[1, m], from_core.at[m], m).wait_send()
            ref = pieces.at[0, m, others]
            to_fs(ref, ref, a_send.at[0], a_recv.at[m], 1).wait_send()
            ref = dirs.at[m, others]
            to_fs(ref, ref, d_send.at[0], d_recv.at[m], 1).wait_send()
        to_tp(sums.at[pl.ds(0, TP - 1)], 1).wait_send()
        ref = fs_sums.at[others]
        to_fs(ref, ref, s_send.at[1], s_recv.at[1], 1).wait_send()


def store_kernel(
    mom,
    upd,
    copies,
    first_out,
    second_out,
    value_update,
    gate_update,
    out_update,
    value_copy,
    gate_copy,
    out_copy,
    sem,
):
    def store(src, dst):
        pltpu.make_async_copy(src, dst, sem.at[0]).start()

    def store_block(s, carry):
        at = pl.ds(pl.multiple_of(s * W, W), W)
        store(copies.at[s, 0], value_copy.at[at, :])
        store(copies.at[s, 1], gate_copy.at[at, :])
        store(copies.at[s, 2], out_copy.at[:, at])
        return carry

    lax.fori_loop(0, FS, store_block, 0)
    store(upd.at[0], value_update)
    store(upd.at[1], gate_update)
    store(upd.at[2], out_update)
    store(mom.at[0], first_out)
    store(mom.at[1], second_out)
    for ref in (copies, upd, mom):
        pltpu.make_async_copy(ref, ref, sem.at[0]).wait()


def shards(*args):
    anywhere = pl.BlockSpec(memory_space=pl.ANY)
    vmem = pl.BlockSpec(memory_space=pltpu.VMEM)
    dma = pltpu.SemaphoreType.DMA
    results = pl.pallas_call(
        kernel,
        out_shape=(
            pltpu.VMEM((2, 3, RS, W), F32),
            pltpu.VMEM((3, W, W), F32),
            pltpu.VMEM((FS, 3, W, W), BF16),
        ),
        in_specs=[anywhere] * 11,
        out_specs=(vmem,) * 3,
        scratch_shapes=[
            pltpu.VMEM((2, TOK, D // 2), BF16),
            pltpu.VMEM((3, TOK, W), BF16),
            pltpu.VMEM((2, 3, W, TOK), BF16),
            pltpu.VMEM((FS, 3, HALF, RANK), BF16),
            pltpu.VMEM((3, W, RANK), BF16),
            pltpu.VMEM((3, W, W), F32),
            pltpu.VMEM((3, TOK, RANK), F32),
            pltpu.VMEM((2, 3, FS, RS, W), F32),
            pltpu.VMEM((3, FS, RS, W), F32),
            pltpu.VMEM((3, FS, RS, W), F32),
            pltpu.VMEM((3, FS, RS, W), F32),
            pltpu.VMEM((TP, 8, 128), F32),
            pltpu.VMEM((FS, 8, 128), F32),
            dma((7,)),
            dma((1,)),
            dma((len(RECEIVED),)),
            dma((2,)),
            dma((5,)),
            dma((1,)),
            dma((3,)),
            dma((1,)),
            dma((3,)),
            dma((2,)),
            dma((2,)),
        ],
        compiler_params=pltpu.CompilerParams(
            collective_id=0, has_side_effects=True, vmem_limit_bytes=48 * 1024 * 1024
        ),
    )(*[pltpu.with_memory_space_constraint(a, pltpu.HBM) for a in args])
    return pl.pallas_call(
        store_kernel,
        out_shape=(
            jax.ShapeDtypeStruct((3, RS, W), F32),
            jax.ShapeDtypeStruct((3, RS, W), F32),
            jax.ShapeDtypeStruct((W, W), F32),
            jax.ShapeDtypeStruct((W, W), F32),
            jax.ShapeDtypeStruct((W, W), F32),
            jax.ShapeDtypeStruct((D, W), BF16),
            jax.ShapeDtypeStruct((D, W), BF16),
            jax.ShapeDtypeStruct((W, D), BF16),
        ),
        in_specs=[vmem] * 3,
        out_specs=(anywhere,) * 8,
        scratch_shapes=[dma((1,))],
        compiler_params=pltpu.CompilerParams(vmem_limit_bytes=4 * 1024 * 1024),
    )(*[pltpu.with_memory_space_constraint(r, pltpu.VMEM) for r in results])


def solution(mesh):
    placed = (
        P("fs", None),
        P("fs", "tp"),
        P("fs", "tp"),
        P("fs", None),
        P("fs", "tp"),
        P(None, "fs", None),
        P("fs", "tp"),
        P("fs", "tp"),
        P("tp", "fs"),
        P(None, "fs", "tp"),
        P(None, "fs", "tp"),
    )
    return jax.shard_map(
        shards,
        mesh=mesh,
        in_specs=placed,
        out_specs=(
            P(None, "fs", "tp"),
            P(None, "fs", "tp"),
            P("fs", "tp"),
            P("fs", "tp"),
            P("tp", "fs"),
            P(None, "tp"),
            P(None, "tp"),
            P("tp", None),
        ),
        check_vma=False,
    )
```

```python
import functools

import jax
import jax.numpy as jnp
from jax import lax
from jax.experimental import pallas as pl
from jax.experimental.pallas import tpu as pltpu
from jax.sharding import PartitionSpec as P

C = 2048
RANK = 256
FIRST_DECAY = 0.9
SECOND_DECAY = 0.95
DIVISOR_EPS = 1e-08
SQUARE_EPS = 1e-06
LEARN_RATE = 0.01

SIDE = 4
FS = SIDE * SIDE
TP = 8
HALF = 128
W = 256
RS = RANK // FS
TOK = 1024
D = 4096
MESH = pl.DeviceIdType.MESH
F32 = jnp.float32
BF16 = jnp.bfloat16

RECEIVED = []
for _k in (0, 1):
    RECEIVED += [(_k, 1, 0, 1), (_k, 1, 0, -1), (_k, 2, 0, 0)]
    for _po in (0, -1, 1, 2):
        RECEIVED += [(_k, 3, _po, 1), (_k, 3, _po, -1), (_k, 4, _po, 0)]
INDEX = {message: at for at, message in enumerate(RECEIVED)}


class RingGather:
    def __init__(self, name, me, part, send, recv):
        self.name = name
        self.z, self.x = me // SIDE, lax.rem(me, SIDE)
        self.part, self.send, self.recv = part, send, recv

    def slot(self, k, po, qo):
        dx, dz = (po, qo) if k == 0 else (qo, po)
        z = lax.rem(self.z + dz + SIDE, SIDE)
        x = lax.rem(self.x + dx + SIDE, SIDE)
        return z * SIDE + x

    def copy(self, ref, k, stage, po, d, to):
        sem = self.recv.at[INDEX[k, stage, po, 0 if stage in (2, 4) else d]]
        return pltpu.make_async_remote_copy(
            src_ref=ref,
            dst_ref=ref,
            send_sem=self.send,
            recv_sem=sem,
            device_id={"fs": to},
            device_id_type=MESH,
        )

    def start(self, k, stage, po, d):
        first = stage in (1, 2)
        at = {1: (0, 0), 2: (-d, 0), 3: (po, 0), 4: (po, -d)}[stage]
        half = None if stage in (1, 3) else (0 if d > 0 else 1)
        to = self.slot(k, d, 0) if first else self.slot(k, 0, d)
        ref = self.part(self.slot(k, *at), k, half)
        self.copy(ref, k, stage, po, d, to).start()

    def wait(self, k, stage, po, d=0):
        at = {1: (-d, 0), 2: (2, 0), 3: (po, -d), 4: (po, 2)}[stage]
        ref = self.part(self.slot(k, *at), k, None)
        with jax.named_scope(f"w{self.name}_{k}_{stage}_{po}_{d}"):
            self.copy(ref, k, stage, po, d, self.slot(k, 1, 0)).wait_recv()

    def steps(self, arrived):
        for stage in (1, 3):
            for d in (1, -1):
                for k in (0, 1):
                    self.start(k, stage, 0, d)
        yield "start"
        for d in (1, -1):
            for k in (0, 1):
                self.wait(k, 1, 0, d)
                self.start(k, 2, 0, d)
                arrived(k, -d, 0)
        for po in (-1, 1):
            for d in (1, -1):
                for k in (0, 1):
                    self.start(k, 3, po, d)
        yield "1"
        self.second(arrived, 0)
        yield "3_0"
        for k in (0, 1):
            self.wait(k, 2, 0)
            self.start(k, 3, 2, 1)
            self.start(k, 3, 2, -1)
            arrived(k, 2, 0)
        yield "2"
        for po in (-1, 1):
            self.second(arrived, po)
            yield f"3_{po}"
        self.last(arrived, 0)
        yield "4_0"
        self.second(arrived, 2)
        yield "3_2"
        for po in (-1, 1, 2):
            self.last(arrived, po)
            yield f"4_{po}"

    def second(self, arrived, po):
        for d in (1, -1):
            for k in (0, 1):
                self.wait(k, 3, po, d)
                self.start(k, 4, po, d)
                arrived(k, po, -d)

    def last(self, arrived, po):
        for k in (0, 1):
            self.wait(k, 4, po)
            arrived(k, po, 2)

    def finish(self, everything):
        self.copy(everything, 0, 1, 0, 1, self.slot(0, 1, 0)).wait_send()


def high_low(values):
    upper = values.astype(BF16)
    return upper, (values - upper.astype(F32)).astype(BF16)


def kernel(
    inputs,
    value_cot,
    gate_cot,
    out_cot,
    conv_output,
    factors,
    value_weight,
    gate_weight,
    out_weight,
    first_moment,
    second_moment,
    mom,
    upd,
    copies,
    left,
    cots,
    cots_t,
    fbuf,
    wbuf,
    summed,
    pieces,
    from_core,
    arrived,
    dirs,
    sums,
    fs_sums,
    load_sem,
    ring_send,
    ring_recv,
    core_send,
    core_recv,
    batch_recv,
    a_send,
    a_recv,
    d_send,
    d_recv,
    s_send,
    s_recv,
):
    me = lax.axis_index("fs")
    t = lax.axis_index("tp")
    core = lax.rem(t, 2)
    partner = t + 1 - 2 * core

    def load(at, *pairs):
        for src, dst in pairs:
            pltpu.make_async_copy(src, dst, load_sem.at[at]).start()

    def loaded(at, ref):
        pltpu.make_async_copy(ref, ref, load_sem.at[at]).wait()

    half = pl.ds(pl.multiple_of(core * HALF, HALF), HALF)
    load(0, (factors, fbuf.at[me]))
    load(1, *((r, cots.at[m]) for m, r in enumerate((value_cot, gate_cot, conv_output))))

    def load_half(s, carry):
        src = pl.ds(pl.multiple_of(s * W + core * HALF, HALF), HALF)
        dst = pl.ds(pl.multiple_of(s * HALF, HALF), HALF)
        load(2, (inputs.at[:, src], left.at[0, :, dst]))
        load(3, (out_cot.at[:, src], left.at[1, :, dst]))
        return carry

    lax.fori_loop(0, FS, load_half, 0)
    load(4, (first_moment, mom.at[0]), (second_moment, mom.at[1]))
    load(5, *((r, wbuf.at[m]) for m, r in enumerate((value_weight, gate_weight, out_weight))))

    barrier = pltpu.get_barrier_semaphore()

    def greet_fs(j, _):
        pl.semaphore_signal(
            barrier, inc=1, device_id={"fs": lax.rem(me + j, FS)}, device_id_type=MESH
        )
        return _

    def greet_tp(j, _):
        pl.semaphore_signal(
            barrier, inc=1, device_id={"tp": lax.rem(t + j, TP)}, device_id_type=MESH
        )
        return _

    lax.fori_loop(1, FS, greet_fs, 0)
    lax.fori_loop(1, TP, greet_tp, 0)

    with jax.named_scope("barrier"):
        pl.semaphore_wait(barrier, FS - 1 + TP - 1)

    def to_partner(src, dst, at):
        return pltpu.make_async_remote_copy(
            src_ref=src,
            dst_ref=dst,
            send_sem=core_send.at[0],
            recv_sem=core_recv.at[at],
            device_id={"tp": partner},
            device_id_type=MESH,
        )

    def factor_part(s, k, half):
        at, size = HALF * k, HALF
        if half is not None:
            at, size = at + 64 * half, 64
        return fbuf.at[s, pl.ds(odd_base, 2), pl.ds(at, size), :]

    y = t // 2
    odd = lax.rem(y, 2)
    odd_base = 1 - odd
    lacking, handed = 2 * odd, 2 - 2 * odd

    def along_y(ref, k):
        to = lax.rem(2 * y + (2 if k == 0 else TP - 2), TP) + k
        return pltpu.make_async_remote_copy(
            src_ref=ref,
            dst_ref=ref,
            send_sem=core_send.at[1],
            recv_sem=core_recv.at[4],
            device_id={"tp": to},
            device_id_type=MESH,
        )

    ring = RingGather("a", me, factor_part, ring_send.at[0], ring_recv)
    here = []

    def to_other_core(ref, batch):
        return pltpu.make_async_remote_copy(
            src_ref=ref,
            dst_ref=ref,
            send_sem=core_send.at[2],
            recv_sem=batch_recv.at[batch],
            device_id={"tp": partner},
            device_id_type=MESH,
        )

    def factor_arrived(k, po, qo):
        s = ring.slot(k, po, qo)
        if k == 0:
            here.append((po, qo))
            to_other_core(factor_part(s, 0, None), state["batch"]).start()
        along_y(fbuf.at[s, handed, pl.ds(HALF * k, HALF), :], k).start()

    state = {"batch": 0}
    groups = ring.steps(factor_arrived)

    def slots_until(group):
        @pl.when(core == 1)
        def _():
            while next(groups) != group:
                pass

        count = len(here)

        @pl.when(core == 0)
        def _():
            with jax.named_scope("wait_batch"):
                ref = fbuf.at[pl.ds(0, count), pl.ds(0, 2), pl.ds(0, HALF), :]
                to_other_core(ref, state["batch"]).wait_recv()

        slots = []
        for po, qo in here:
            zero, one = ring.slot(0, po, qo), ring.slot(1, po, qo)
            slots.append(zero + core * (one - zero))
        here.clear()
        state["batch"] += 1
        return slots

    def multiply(*slots, first=False, matrices=(odd_base, odd_base + 1)):
        with jax.named_scope("multiply"):
            for m in matrices:
                ours = [
                    left[m // 2, :, pl.ds(pl.multiple_of(s * HALF, HALF), HALF)]
                    for s in slots
                ]
                product = jnp.dot(
                    jnp.concatenate(ours, axis=1),
                    jnp.concatenate([fbuf[s, m, half, :] for s in slots], axis=0),
                    preferred_element_type=F32,
                )
                if first:
                    summed[m] = product
                else:
                    summed[m] += product

    def multiply_lacking():
        with jax.named_scope("multiply_lacking"):
            right = fbuf[:, lacking, half, :].reshape(D // 2, RANK)

            def tile(i, carry):
                rows = pl.ds(pl.multiple_of(i * 256, 256), 256)
                ours = left[lacking // 2, rows, :]
                summed[lacking, rows, :] = jnp.dot(ours, right, preferred_element_type=F32)
                return carry

            lax.fori_loop(0, TOK // 256, tile, 0)

    def loop(start, stop, step):
        def body(j, carry):
            step(j)
            return carry

        lax.fori_loop(start, stop, body, 0)

    def to_fs(src, dst, send, recv, j):
        return pltpu.make_async_remote_copy(
            src_ref=src,
            dst_ref=dst,
            send_sem=send,
            recv_sem=recv,
            device_id={"fs": lax.rem(me + j, FS)},
            device_id_type=MESH,
        )

    others = pl.ds(0, FS - 1)

    def project(m):
        with jax.named_scope("project"):
            split = jnp.concatenate(high_low(summed[m]), axis=1)
            for side in (1, 0):
                product = jnp.dot(cots_t[side, m], split, preferred_element_type=F32)
                product = product[:, :RANK] + product[:, RANK:]
                pieces[side, m] = product.T.reshape(FS, RS, W)
                if side == 1:
                    to_partner(pieces.at[1, m], from_core.at[m], m).start()

    def send_pieces(m):
        with jax.named_scope("wait_core"):
            to_partner(pieces.at[1, m], from_core.at[m], m).wait_recv()
        pieces[0, m] += from_core[m]

        def send_piece(j):
            to_fs(
                pieces.at[0, m, lax.rem(me + j, FS)],
                arrived.at[m, me],
                a_send.at[0],
                a_recv.at[m],
                j,
            ).start()

        loop(1, FS, send_piece)
        arrived[m, me] = pieces[0, m, me]

    squares = []

    def moments(m):
        with jax.named_scope("wait_pieces"):
            ref = arrived.at[m, others]
            to_fs(ref, ref, a_send.at[0], a_recv.at[m], 1).wait_recv()
        projected = jnp.sum(arrived[m], axis=0)
        new_first = FIRST_DECAY * mom[0, m] + (1.0 - FIRST_DECAY) * projected
        new_second = (
            SECOND_DECAY * mom[1, m] + (1.0 - SECOND_DECAY) * projected * projected
        )
        direction = new_first / (jnp.sqrt(new_second) + DIVISOR_EPS)
        mom[0, m] = new_first
        mom[1, m] = new_second
        dirs[m, me] = direction

        def send_direction(j):
            ref = dirs.at[m, me]
            to_fs(ref, ref, d_send.at[0], d_recv.at[m], j).start()

        loop(1, FS, send_direction)
        squares.append(direction[:8] * direction[:8] + direction[8:] * direction[8:])

    loaded(0, fbuf.at[me])

    @pl.when(core == 1)
    def _():
        next(groups)

    with jax.named_scope("turn"):
        loaded(1, cots)
        for m in range(3):

            def turn(i, _):
                rows = pl.ds(pl.multiple_of(i * 256, 256), 256)
                cots_t[0, m, :, rows] = cots[m, rows, :].T
                return _

            lax.fori_loop(0, TOK // 256, turn, 0)

    to_partner(cots_t.at[0], cots_t.at[1], 3).start()
    with jax.named_scope("wait_loads"):
        loaded(2, left.at[0])
        loaded(3, left.at[1])
    multiply(me, first=True)
    for group in ("3_0", "3_1", "3_2", "4_1"):
        multiply(*slots_until(group))
    to_partner(cots_t.at[0], cots_t.at[1], 3).wait_recv()
    last = slots_until("4_2")
    order = (odd_base, odd_base + 1, lacking)
    multiply(*last, matrices=order[:1])
    project(order[0])
    multiply(*last, matrices=order[1:2])
    send_pieces(order[0])
    project(order[1])
    with jax.named_scope("wait_y"):
        along_y(fbuf.at[others, 0, pl.ds(0, HALF)], 0).wait_recv()
    multiply_lacking()
    send_pieces(order[1])
    project(order[2])
    send_pieces(order[2])
    loaded(4, mom)
    for m in order:
        moments(m)

    square = squares[0] + squares[1] + squares[2]
    sums[t] = square[:, :128] + square[:, 128:]

    def to_tp(ref, j):
        return pltpu.make_async_remote_copy(
            src_ref=ref,
            dst_ref=ref,
            send_sem=s_send.at[0],
            recv_sem=s_recv.at[0],
            device_id={"tp": lax.rem(t + j, TP)},
            device_id_type=MESH,
        )

    loop(1, TP, lambda j: to_tp(sums.at[t], j).start())

    def wait_directions(m):
        with jax.named_scope("wait_directions"):
            ref = dirs.at[m, others]
            to_fs(ref, ref, d_send.at[0], d_recv.at[m], 1).wait_recv()

    def update(m):
        full = dirs[m].reshape(RANK, W)
        if m == 2:
            upper, lower = high_low(full.T)
            contract = (((1,), (1,)), ((), ()))
            own = fbuf[me, m]
            product = lax.dot_general(upper, own, contract, preferred_element_type=F32)
            product += lax.dot_general(lower, own, contract, preferred_element_type=F32)
        else:
            upper, lower = high_low(full)
            product = jnp.dot(fbuf[me, m], upper, preferred_element_type=F32)
            product += jnp.dot(fbuf[me, m], lower, preferred_element_type=F32)
        upd[m] = product

    loaded(5, wbuf)
    wait_directions(order[0])
    with jax.named_scope("wait_scalar"):
        to_tp(sums.at[pl.ds(0, TP - 1)], 1).wait_recv()
    fs_sums[me] = jnp.sum(sums[...], axis=0)

    def send_sum(j):
        ref = fs_sums.at[me]
        to_fs(ref, ref, s_send.at[1], s_recv.at[1], j).start()

    loop(1, FS, send_sum)
    wait_directions(order[1])
    update(1)

    @pl.when(odd == 1)
    def _():
        update(0)

    @pl.when(odd == 0)
    def _():
        update(2)

    @pl.when(core == 1)
    def _():
        ring.finish(fbuf.at[others, pl.ds(0, 2)])
        along_y(fbuf.at[others, 0], 0).wait_send()
        to_other_core(fbuf.at[others, pl.ds(0, 2), pl.ds(0, HALF)], 0).wait_send()

    wait_directions(order[2])

    @pl.when(odd == 0)
    def _():
        update(0)

    @pl.when(odd == 1)
    def _():
        update(2)

    with jax.named_scope("wait_fs_scalar"):
        ref = fs_sums.at[others]
        to_fs(ref, ref, s_send.at[1], s_recv.at[1], 1).wait_recv()
    total = jnp.sum(jnp.sum(fs_sums[...], axis=0), keepdims=True)
    norm_scale = lax.rsqrt(total / (3 * RANK * C) + SQUARE_EPS)
    for m in range(3):
        scaled = norm_scale * upd[m]
        upd[m] = scaled
        copies[me, m] = (wbuf[m] - LEARN_RATE * scaled).astype(BF16)

    def copy_part(s, k, half):
        at, size = 128 * k, 128
        if half is not None:
            at, size = at + 64 * half, 64
        return copies.at[s, :, pl.ds(at, size), :]

    gather = RingGather("c", me, copy_part, ring_send.at[0], ring_recv)
    for _ in gather.steps(lambda k, po, qo: None):
        pass

    with jax.named_scope("finish"):
        gather.finish(copies.at[others])
        to_partner(cots_t.at[0], cots_t.at[1], 3).wait_send()
        for m in range(3):
            to_partner(pieces.at[1, m], from_core.at[m], m).wait_send()
            ref = pieces.at[0, m, others]
            to_fs(ref, ref, a_send.at[0], a_recv.at[m], 1).wait_send()
            ref = dirs.at[m, others]
            to_fs(ref, ref, d_send.at[0], d_recv.at[m], 1).wait_send()
        to_tp(sums.at[pl.ds(0, TP - 1)], 1).wait_send()
        ref = fs_sums.at[others]
        to_fs(ref, ref, s_send.at[1], s_recv.at[1], 1).wait_send()


def store_kernel(
    mom,
    upd,
    copies,
    first_out,
    second_out,
    value_update,
    gate_update,
    out_update,
    value_copy,
    gate_copy,
    out_copy,
    sem,
):
    def store(src, dst):
        pltpu.make_async_copy(src, dst, sem.at[0]).start()

    def store_block(s, carry):
        at = pl.ds(pl.multiple_of(s * W, W), W)
        store(copies.at[s, 0], value_copy.at[at, :])
        store(copies.at[s, 1], gate_copy.at[at, :])
        store(copies.at[s, 2], out_copy.at[:, at])
        return carry

    lax.fori_loop(0, FS, store_block, 0)
    store(upd.at[0], value_update)
    store(upd.at[1], gate_update)
    store(upd.at[2], out_update)
    store(mom.at[0], first_out)
    store(mom.at[1], second_out)
    for ref in (copies, upd, mom):
        pltpu.make_async_copy(ref, ref, sem.at[0]).wait()


def shards(*args):
    anywhere = pl.BlockSpec(memory_space=pl.ANY)
    vmem = pl.BlockSpec(memory_space=pltpu.VMEM)
    dma = pltpu.SemaphoreType.DMA
    results = pl.pallas_call(
        kernel,
        out_shape=(
            pltpu.VMEM((2, 3, RS, W), F32),
            pltpu.VMEM((3, W, W), F32),
            pltpu.VMEM((FS, 3, W, W), BF16),
        ),
        in_specs=[anywhere] * 11,
        out_specs=(vmem,) * 3,
        scratch_shapes=[
            pltpu.VMEM((2, TOK, D // 2), BF16),
            pltpu.VMEM((3, TOK, W), BF16),
            pltpu.VMEM((2, 3, W, TOK), BF16),
            pltpu.VMEM((FS, 3, W, RANK), BF16),
            pltpu.VMEM((3, W, W), F32),
            pltpu.VMEM((3, TOK, RANK), F32),
            pltpu.VMEM((2, 3, FS, RS, W), F32),
            pltpu.VMEM((3, FS, RS, W), F32),
            pltpu.VMEM((3, FS, RS, W), F32),
            pltpu.VMEM((3, FS, RS, W), F32),
            pltpu.VMEM((TP, 8, 128), F32),
            pltpu.VMEM((FS, 8, 128), F32),
            dma((6,)),
            dma((1,)),
            dma((len(RECEIVED),)),
            dma((3,)),
            dma((5,)),
            dma((5,)),
            dma((1,)),
            dma((3,)),
            dma((1,)),
            dma((3,)),
            dma((2,)),
            dma((2,)),
        ],
        compiler_params=pltpu.CompilerParams(
            collective_id=0, has_side_effects=True, vmem_limit_bytes=48 * 1024 * 1024
        ),
    )(*[pltpu.with_memory_space_constraint(a, pltpu.HBM) for a in args])
    return pl.pallas_call(
        store_kernel,
        out_shape=(
            jax.ShapeDtypeStruct((3, RS, W), F32),
            jax.ShapeDtypeStruct((3, RS, W), F32),
            jax.ShapeDtypeStruct((W, W), F32),
            jax.ShapeDtypeStruct((W, W), F32),
            jax.ShapeDtypeStruct((W, W), F32),
            jax.ShapeDtypeStruct((D, W), BF16),
            jax.ShapeDtypeStruct((D, W), BF16),
            jax.ShapeDtypeStruct((W, D), BF16),
        ),
        in_specs=[vmem] * 3,
        out_specs=(anywhere,) * 8,
        scratch_shapes=[dma((1,))],
        compiler_params=pltpu.CompilerParams(vmem_limit_bytes=4 * 1024 * 1024),
    )(*[pltpu.with_memory_space_constraint(r, pltpu.VMEM) for r in results])


def solution(mesh):
    placed = (
        P("fs", None),
        P("fs", "tp"),
        P("fs", "tp"),
        P("fs", None),
        P("fs", "tp"),
        P(None, "fs", None),
        P("fs", "tp"),
        P("fs", "tp"),
        P("tp", "fs"),
        P(None, "fs", "tp"),
        P(None, "fs", "tp"),
    )
    return jax.shard_map(
        shards,
        mesh=mesh,
        in_specs=placed,
        out_specs=(
            P(None, "fs", "tp"),
            P(None, "fs", "tp"),
            P("fs", "tp"),
            P("fs", "tp"),
            P("tp", "fs"),
            P(None, "tp"),
            P(None, "tp"),
            P("tp", None),
        ),
        check_vma=False,
    )
```

```python
import functools

import jax
import jax.numpy as jnp
from jax import lax
from jax.experimental import pallas as pl
from jax.experimental.pallas import tpu as pltpu
from jax.sharding import PartitionSpec as P

C = 2048
RANK = 256
FIRST_DECAY = 0.9
SECOND_DECAY = 0.95
DIVISOR_EPS = 1e-08
SQUARE_EPS = 1e-06
LEARN_RATE = 0.01

SIDE = 4
FS = SIDE * SIDE
TP = 8
HALF = 128
W = 256
RS = RANK // FS
TOK = 1024
D = 4096
MESH = pl.DeviceIdType.MESH
F32 = jnp.float32
BF16 = jnp.bfloat16

RECEIVED = []
for _k in (0, 1):
    RECEIVED += [(_k, 1, 0, 1), (_k, 1, 0, -1), (_k, 2, 0, 0)]
    for _po in (0, -1, 1, 2):
        RECEIVED += [(_k, 3, _po, 1), (_k, 3, _po, -1), (_k, 4, _po, 0)]
INDEX = {message: at for at, message in enumerate(RECEIVED)}


class RingGather:
    def __init__(self, name, me, part, send, recv):
        self.name = name
        self.z, self.x = me // SIDE, lax.rem(me, SIDE)
        self.part, self.send, self.recv = part, send, recv

    def slot(self, k, po, qo):
        dx, dz = (po, qo) if k == 0 else (qo, po)
        z = lax.rem(self.z + dz + SIDE, SIDE)
        x = lax.rem(self.x + dx + SIDE, SIDE)
        return z * SIDE + x

    def copy(self, ref, k, stage, po, d, to):
        sem = self.recv.at[INDEX[k, stage, po, 0 if stage in (2, 4) else d]]
        return pltpu.make_async_remote_copy(
            src_ref=ref,
            dst_ref=ref,
            send_sem=self.send,
            recv_sem=sem,
            device_id={"fs": to},
            device_id_type=MESH,
        )

    def start(self, k, stage, po, d):
        first = stage in (1, 2)
        at = {1: (0, 0), 2: (-d, 0), 3: (po, 0), 4: (po, -d)}[stage]
        half = None if stage in (1, 3) else (0 if d > 0 else 1)
        to = self.slot(k, d, 0) if first else self.slot(k, 0, d)
        ref = self.part(self.slot(k, *at), k, half)
        self.copy(ref, k, stage, po, d, to).start()

    def wait(self, k, stage, po, d=0):
        at = {1: (-d, 0), 2: (2, 0), 3: (po, -d), 4: (po, 2)}[stage]
        ref = self.part(self.slot(k, *at), k, None)
        with jax.named_scope(f"w{self.name}_{k}_{stage}_{po}_{d}"):
            self.copy(ref, k, stage, po, d, self.slot(k, 1, 0)).wait_recv()

    def steps(self, arrived):
        for stage in (1, 3):
            for d in (1, -1):
                for k in (0, 1):
                    self.start(k, stage, 0, d)
        yield "start"
        for d in (1, -1):
            for k in (0, 1):
                self.wait(k, 1, 0, d)
                self.start(k, 2, 0, d)
                arrived(k, -d, 0)
        for po in (-1, 1):
            for d in (1, -1):
                for k in (0, 1):
                    self.start(k, 3, po, d)
        yield "1"
        self.second(arrived, 0)
        yield "3_0"
        for k in (0, 1):
            self.wait(k, 2, 0)
            self.start(k, 3, 2, 1)
            self.start(k, 3, 2, -1)
            arrived(k, 2, 0)
        yield "2"
        for po in (-1, 1):
            self.second(arrived, po)
            yield f"3_{po}"
        self.last(arrived, 0)
        yield "4_0"
        self.second(arrived, 2)
        yield "3_2"
        for po in (-1, 1, 2):
            self.last(arrived, po)
            yield f"4_{po}"

    def second(self, arrived, po):
        for d in (1, -1):
            for k in (0, 1):
                self.wait(k, 3, po, d)
                self.start(k, 4, po, d)
                arrived(k, po, -d)

    def last(self, arrived, po):
        for k in (0, 1):
            self.wait(k, 4, po)
            arrived(k, po, 2)

    def finish(self, everything):
        self.copy(everything, 0, 1, 0, 1, self.slot(0, 1, 0)).wait_send()


def high_low(values):
    upper = values.astype(BF16)
    return upper, (values - upper.astype(F32)).astype(BF16)


def kernel(
    inputs,
    value_cot,
    gate_cot,
    out_cot,
    conv_output,
    factors,
    value_weight,
    gate_weight,
    out_weight,
    first_moment,
    second_moment,
    mom,
    upd,
    copies,
    left,
    cots,
    cots_t,
    fbuf,
    wbuf,
    summed,
    pieces,
    from_core,
    arrived,
    dirs,
    sums,
    fs_sums,
    load_sem,
    ring_send,
    ring_recv,
    core_send,
    core_recv,
    batch_recv,
    a_send,
    a_recv,
    d_send,
    d_recv,
    s_send,
    s_recv,
):
    me = lax.axis_index("fs")
    t = lax.axis_index("tp")
    core = lax.rem(t, 2)
    partner = t + 1 - 2 * core

    barrier = pltpu.get_barrier_semaphore()

    def greet_fs(j, _):
        pl.semaphore_signal(
            barrier, inc=1, device_id={"fs": lax.rem(me + j, FS)}, device_id_type=MESH
        )
        return _

    def greet_tp(j, _):
        pl.semaphore_signal(
            barrier, inc=1, device_id={"tp": lax.rem(t + j, TP)}, device_id_type=MESH
        )
        return _

    lax.fori_loop(1, FS, greet_fs, 0)
    lax.fori_loop(1, TP, greet_tp, 0)

    def load(at, *pairs):
        for src, dst in pairs:
            pltpu.make_async_copy(src, dst, load_sem.at[at]).start()

    def loaded(at, ref):
        pltpu.make_async_copy(ref, ref, load_sem.at[at]).wait()

    half = pl.ds(pl.multiple_of(core * HALF, HALF), HALF)
    load(0, (factors, fbuf.at[me]))
    load(1, *((r, cots.at[m]) for m, r in enumerate((value_cot, gate_cot, conv_output))))

    def load_half(s, carry):
        src = pl.ds(pl.multiple_of(s * W + core * HALF, HALF), HALF)
        dst = pl.ds(pl.multiple_of(s * HALF, HALF), HALF)
        load(2, (inputs.at[:, src], left.at[0, :, dst]))
        load(3, (out_cot.at[:, src], left.at[1, :, dst]))
        return carry

    lax.fori_loop(0, FS, load_half, 0)
    load(4, (first_moment, mom.at[0]), (second_moment, mom.at[1]))
    load(5, *((r, wbuf.at[m]) for m, r in enumerate((value_weight, gate_weight, out_weight))))

    with jax.named_scope("barrier"):
        pl.semaphore_wait(barrier, FS - 1 + TP - 1)

    def to_partner(src, dst, at):
        return pltpu.make_async_remote_copy(
            src_ref=src,
            dst_ref=dst,
            send_sem=core_send.at[0],
            recv_sem=core_recv.at[at],
            device_id={"tp": partner},
            device_id_type=MESH,
        )

    def factor_part(s, k, half):
        at, size = HALF * k, HALF
        if half is not None:
            at, size = at + 64 * half, 64
        return fbuf.at[s, pl.ds(odd_base, 2), pl.ds(at, size), :]

    y = t // 2
    odd = lax.rem(y, 2)
    odd_base = 1 - odd
    lacking, handed = 2 * odd, 2 - 2 * odd

    def along_y(ref, k):
        to = lax.rem(2 * y + (2 if k == 0 else TP - 2), TP) + k
        return pltpu.make_async_remote_copy(
            src_ref=ref,
            dst_ref=ref,
            send_sem=core_send.at[1],
            recv_sem=core_recv.at[4],
            device_id={"tp": to},
            device_id_type=MESH,
        )

    ring = RingGather("a", me, factor_part, ring_send.at[0], ring_recv)
    here = []

    def to_other_core(ref, batch):
        return pltpu.make_async_remote_copy(
            src_ref=ref,
            dst_ref=ref,
            send_sem=core_send.at[2],
            recv_sem=batch_recv.at[batch],
            device_id={"tp": partner},
            device_id_type=MESH,
        )

    def factor_arrived(k, po, qo):
        s = ring.slot(k, po, qo)
        if k == 0:
            here.append((po, qo))
            to_other_core(factor_part(s, 0, None), state["batch"]).start()
        along_y(fbuf.at[s, handed, pl.ds(HALF * k, HALF), :], k).start()

    state = {"batch": 0}
    groups = ring.steps(factor_arrived)

    def slots_until(group):
        @pl.when(core == 1)
        def _():
            while next(groups) != group:
                pass

        count = len(here)

        @pl.when(core == 0)
        def _():
            with jax.named_scope("wait_batch"):
                ref = fbuf.at[pl.ds(0, count), pl.ds(0, 2), pl.ds(0, HALF), :]
                to_other_core(ref, state["batch"]).wait_recv()

        slots = []
        for po, qo in here:
            zero, one = ring.slot(0, po, qo), ring.slot(1, po, qo)
            slots.append(zero + core * (one - zero))
        here.clear()
        state["batch"] += 1
        return slots

    def multiply(*slots, first=False, matrices=(odd_base, odd_base + 1)):
        with jax.named_scope("multiply"):
            for m in matrices:
                ours = [
                    left[m // 2, :, pl.ds(pl.multiple_of(s * HALF, HALF), HALF)]
                    for s in slots
                ]
                product = jnp.dot(
                    jnp.concatenate(ours, axis=1),
                    jnp.concatenate([fbuf[s, m, half, :] for s in slots], axis=0),
                    preferred_element_type=F32,
                )
                if first:
                    summed[m] = product
                else:
                    summed[m] += product

    def multiply_lacking():
        with jax.named_scope("multiply_lacking"):
            right = fbuf[:, lacking, half, :].reshape(D // 2, RANK)

            def tile(i, carry):
                rows = pl.ds(pl.multiple_of(i * 512, 512), 512)
                ours = left[lacking // 2, rows, :]
                summed[lacking, rows, :] = jnp.dot(ours, right, preferred_element_type=F32)
                return carry

            lax.fori_loop(0, TOK // 512, tile, 0)

    def loop(start, stop, step):
        def body(j, carry):
            step(j)
            return carry

        lax.fori_loop(start, stop, body, 0)

    def to_fs(src, dst, send, recv, j):
        return pltpu.make_async_remote_copy(
            src_ref=src,
            dst_ref=dst,
            send_sem=send,
            recv_sem=recv,
            device_id={"fs": lax.rem(me + j, FS)},
            device_id_type=MESH,
        )

    others = pl.ds(0, FS - 1)

    def project(m):
        with jax.named_scope("project"):
            split = jnp.concatenate(high_low(summed[m]), axis=1)
            for side in (1, 0):
                product = jnp.dot(cots_t[side, m], split, preferred_element_type=F32)
                product = product[:, :RANK] + product[:, RANK:]
                pieces[side, m] = product.T.reshape(FS, RS, W)
                if side == 1:
                    to_partner(pieces.at[1, m], from_core.at[m], m).start()

    def send_pieces(m):
        with jax.named_scope("wait_core"):
            to_partner(pieces.at[1, m], from_core.at[m], m).wait_recv()
        pieces[0, m] += from_core[m]

        def send_piece(j):
            to_fs(
                pieces.at[0, m, lax.rem(me + j, FS)],
                arrived.at[m, me],
                a_send.at[0],
                a_recv.at[m],
                j,
            ).start()

        loop(1, FS, send_piece)
        arrived[m, me] = pieces[0, m, me]

    def to_tp(ref, j):
        return pltpu.make_async_remote_copy(
            src_ref=ref,
            dst_ref=ref,
            send_sem=s_send.at[0],
            recv_sem=s_recv.at[0],
            device_id={"tp": lax.rem(t + j, TP)},
            device_id_type=MESH,
        )

    squares = []

    def moments(m):
        with jax.named_scope("wait_pieces"):
            ref = arrived.at[m, others]
            to_fs(ref, ref, a_send.at[0], a_recv.at[m], 1).wait_recv()
        projected = jnp.sum(arrived[m], axis=0)
        new_first = FIRST_DECAY * mom[0, m] + (1.0 - FIRST_DECAY) * projected
        new_second = (
            SECOND_DECAY * mom[1, m] + (1.0 - SECOND_DECAY) * projected * projected
        )
        direction = new_first / (jnp.sqrt(new_second) + DIVISOR_EPS)
        mom[0, m] = new_first
        mom[1, m] = new_second
        dirs[m, me] = direction
        squares.append(jnp.sum(direction * direction, axis=0, keepdims=True))
        if len(squares) == 3:
            square = squares[0] + squares[1] + squares[2]
            sums[t] = square[:, :128] + square[:, 128:]
            loop(1, TP, lambda j: to_tp(sums.at[t], j).start())

        def send_direction(j):
            ref = dirs.at[m, me]
            to_fs(ref, ref, d_send.at[0], d_recv.at[m], j).start()

        loop(1, FS, send_direction)

    loaded(0, fbuf.at[me])

    @pl.when(core == 1)
    def _():
        next(groups)

    with jax.named_scope("turn"):
        loaded(1, cots)
        for m in range(3):

            def turn(i, _):
                rows = pl.ds(pl.multiple_of(i * 256, 256), 256)
                cots_t[0, m, :, rows] = cots[m, rows, :].T
                return _

            lax.fori_loop(0, TOK // 256, turn, 0)

    to_partner(cots_t.at[0], cots_t.at[1], 3).start()
    with jax.named_scope("wait_loads"):
        loaded(2, left.at[0])
        loaded(3, left.at[1])
    multiply(me, first=True)
    for group in ("3_0", "3_1", "3_2", "4_1"):
        multiply(*slots_until(group))
    to_partner(cots_t.at[0], cots_t.at[1], 3).wait_recv()
    last = slots_until("4_2")
    order = (odd_base, odd_base + 1, lacking)
    multiply(*last, matrices=order[:1])
    project(order[0])
    multiply(*last, matrices=order[1:2])
    send_pieces(order[0])
    project(order[1])
    send_pieces(order[1])
    with jax.named_scope("wait_y"):
        along_y(fbuf.at[others, 0, pl.ds(0, HALF)], 0).wait_recv()
    multiply_lacking()
    project(order[2])
    send_pieces(order[2])
    loaded(4, mom)
    for m in order:
        moments(m)

    def wait_directions(m):
        with jax.named_scope("wait_directions"):
            ref = dirs.at[m, others]
            to_fs(ref, ref, d_send.at[0], d_recv.at[m], 1).wait_recv()

    def update(m):
        full = dirs[m].reshape(RANK, W)
        if m == 2:
            upper, lower = high_low(full.T)
            contract = (((1,), (1,)), ((), ()))
            own = fbuf[me, m]
            product = lax.dot_general(upper, own, contract, preferred_element_type=F32)
            product += lax.dot_general(lower, own, contract, preferred_element_type=F32)
        else:
            upper, lower = high_low(full)
            product = jnp.dot(fbuf[me, m], upper, preferred_element_type=F32)
            product += jnp.dot(fbuf[me, m], lower, preferred_element_type=F32)
        upd[m] = product

    loaded(5, wbuf)
    wait_directions(order[0])
    with jax.named_scope("wait_scalar"):
        to_tp(sums.at[pl.ds(0, TP - 1)], 1).wait_recv()
    fs_sums[me] = jnp.sum(sums[...], axis=0)

    def send_sum(j):
        ref = fs_sums.at[me]
        to_fs(ref, ref, s_send.at[1], s_recv.at[1], j).start()

    loop(1, FS, send_sum)
    wait_directions(order[1])
    update(1)

    @pl.when(odd == 1)
    def _():
        update(0)

    @pl.when(odd == 0)
    def _():
        update(2)

    @pl.when(core == 1)
    def _():
        ring.finish(fbuf.at[others, pl.ds(0, 2)])
        along_y(fbuf.at[others, 0], 0).wait_send()
        to_other_core(fbuf.at[others, pl.ds(0, 2), pl.ds(0, HALF)], 0).wait_send()

    wait_directions(order[2])

    @pl.when(odd == 0)
    def _():
        update(0)

    @pl.when(odd == 1)
    def _():
        update(2)

    with jax.named_scope("wait_fs_scalar"):
        ref = fs_sums.at[others]
        to_fs(ref, ref, s_send.at[1], s_recv.at[1], 1).wait_recv()
    total = jnp.sum(jnp.sum(fs_sums[...], axis=0), keepdims=True)
    norm_scale = lax.rsqrt(total / (3 * RANK * C) + SQUARE_EPS)
    for m in range(3):
        scaled = norm_scale * upd[m]
        upd[m] = scaled
        copies[me, m] = (wbuf[m] - LEARN_RATE * scaled).astype(BF16)

    def copy_part(s, k, half):
        at, size = 128 * k, 128
        if half is not None:
            at, size = at + 64 * half, 64
        return copies.at[s, :, pl.ds(at, size), :]

    gather = RingGather("c", me, copy_part, ring_send.at[0], ring_recv)
    for _ in gather.steps(lambda k, po, qo: None):
        pass

    with jax.named_scope("finish"):
        gather.finish(copies.at[others])
        to_partner(cots_t.at[0], cots_t.at[1], 3).wait_send()
        for m in range(3):
            to_partner(pieces.at[1, m], from_core.at[m], m).wait_send()
            ref = pieces.at[0, m, others]
            to_fs(ref, ref, a_send.at[0], a_recv.at[m], 1).wait_send()
            ref = dirs.at[m, others]
            to_fs(ref, ref, d_send.at[0], d_recv.at[m], 1).wait_send()
        to_tp(sums.at[pl.ds(0, TP - 1)], 1).wait_send()
        ref = fs_sums.at[others]
        to_fs(ref, ref, s_send.at[1], s_recv.at[1], 1).wait_send()


def store_kernel(
    mom,
    upd,
    copies,
    first_out,
    second_out,
    value_update,
    gate_update,
    out_update,
    value_copy,
    gate_copy,
    out_copy,
    sem,
):
    def store(src, dst):
        pltpu.make_async_copy(src, dst, sem.at[0]).start()

    def store_block(s, carry):
        at = pl.ds(pl.multiple_of(s * W, W), W)
        store(copies.at[s, 0], value_copy.at[at, :])
        store(copies.at[s, 1], gate_copy.at[at, :])
        store(copies.at[s, 2], out_copy.at[:, at])
        return carry

    lax.fori_loop(0, FS, store_block, 0)
    store(upd.at[0], value_update)
    store(upd.at[1], gate_update)
    store(upd.at[2], out_update)
    store(mom.at[0], first_out)
    store(mom.at[1], second_out)
    for ref in (copies, upd, mom):
        pltpu.make_async_copy(ref, ref, sem.at[0]).wait()


def shards(*args):
    anywhere = pl.BlockSpec(memory_space=pl.ANY)
    vmem = pl.BlockSpec(memory_space=pltpu.VMEM)
    dma = pltpu.SemaphoreType.DMA
    results = pl.pallas_call(
        kernel,
        out_shape=(
            pltpu.VMEM((2, 3, RS, W), F32),
            pltpu.VMEM((3, W, W), F32),
            pltpu.VMEM((FS, 3, W, W), BF16),
        ),
        in_specs=[anywhere] * 11,
        out_specs=(vmem,) * 3,
        scratch_shapes=[
            pltpu.VMEM((2, TOK, D // 2), BF16),
            pltpu.VMEM((3, TOK, W), BF16),
            pltpu.VMEM((2, 3, W, TOK), BF16),
            pltpu.VMEM((FS, 3, W, RANK), BF16),
            pltpu.VMEM((3, W, W), F32),
            pltpu.VMEM((3, TOK, RANK), F32),
            pltpu.VMEM((2, 3, FS, RS, W), F32),
            pltpu.VMEM((3, FS, RS, W), F32),
            pltpu.VMEM((3, FS, RS, W), F32),
            pltpu.VMEM((3, FS, RS, W), F32),
            pltpu.VMEM((TP, 1, 128), F32),
            pltpu.VMEM((FS, 1, 128), F32),
            dma((6,)),
            dma((1,)),
            dma((len(RECEIVED),)),
            dma((3,)),
            dma((5,)),
            dma((5,)),
            dma((1,)),
            dma((3,)),
            dma((1,)),
            dma((3,)),
            dma((2,)),
            dma((2,)),
        ],
        compiler_params=pltpu.CompilerParams(
            collective_id=0, has_side_effects=True, vmem_limit_bytes=48 * 1024 * 1024
        ),
    )(*[pltpu.with_memory_space_constraint(a, pltpu.HBM) for a in args])
    return pl.pallas_call(
        store_kernel,
        out_shape=(
            jax.ShapeDtypeStruct((3, RS, W), F32),
            jax.ShapeDtypeStruct((3, RS, W), F32),
            jax.ShapeDtypeStruct((W, W), F32),
            jax.ShapeDtypeStruct((W, W), F32),
            jax.ShapeDtypeStruct((W, W), F32),
            jax.ShapeDtypeStruct((D, W), BF16),
            jax.ShapeDtypeStruct((D, W), BF16),
            jax.ShapeDtypeStruct((W, D), BF16),
        ),
        in_specs=[vmem] * 3,
        out_specs=(anywhere,) * 8,
        scratch_shapes=[dma((1,))],
        compiler_params=pltpu.CompilerParams(vmem_limit_bytes=4 * 1024 * 1024),
    )(*[pltpu.with_memory_space_constraint(r, pltpu.VMEM) for r in results])


def solution(mesh):
    placed = (
        P("fs", None),
        P("fs", "tp"),
        P("fs", "tp"),
        P("fs", None),
        P("fs", "tp"),
        P(None, "fs", None),
        P("fs", "tp"),
        P("fs", "tp"),
        P("tp", "fs"),
        P(None, "fs", "tp"),
        P(None, "fs", "tp"),
    )
    return jax.shard_map(
        shards,
        mesh=mesh,
        in_specs=placed,
        out_specs=(
            P(None, "fs", "tp"),
            P(None, "fs", "tp"),
            P("fs", "tp"),
            P("fs", "tp"),
            P("tp", "fs"),
            P(None, "tp"),
            P(None, "tp"),
            P("tp", None),
        ),
        check_vma=False,
    )
```

```python
import functools

import jax
import jax.numpy as jnp
from jax import lax
from jax.experimental import pallas as pl
from jax.experimental.pallas import tpu as pltpu
from jax.sharding import PartitionSpec as P

C = 2048
RANK = 256
FIRST_DECAY = 0.9
SECOND_DECAY = 0.95
DIVISOR_EPS = 1e-08
SQUARE_EPS = 1e-06
LEARN_RATE = 0.01

SIDE = 4
FS = SIDE * SIDE
TP = 8
HALF = 128
W = 256
RS = RANK // FS
TOK = 1024
D = 4096
MESH = pl.DeviceIdType.MESH
F32 = jnp.float32
BF16 = jnp.bfloat16

RECEIVED = []
for _k in (0, 1):
    RECEIVED += [(_k, 1, 0, 1), (_k, 1, 0, -1), (_k, 2, 0, 0)]
    for _po in (0, -1, 1, 2):
        RECEIVED += [(_k, 3, _po, 1), (_k, 3, _po, -1), (_k, 4, _po, 0)]
INDEX = {message: at for at, message in enumerate(RECEIVED)}


class RingGather:
    def __init__(self, name, me, part, send, recv, near=None):
        self.near = near
        self.name = name
        self.z, self.x = me // SIDE, lax.rem(me, SIDE)
        self.part, self.send, self.recv = part, send, recv

    def slot(self, k, po, qo):
        dx, dz = (po, qo) if k == 0 else (qo, po)
        z = lax.rem(self.z + dz + SIDE, SIDE)
        x = lax.rem(self.x + dx + SIDE, SIDE)
        return z * SIDE + x

    def copy(self, ref, k, stage, po, d, to):
        sem = self.recv.at[INDEX[k, stage, po, 0 if stage in (2, 4) else d]]
        return pltpu.make_async_remote_copy(
            src_ref=ref,
            dst_ref=ref,
            send_sem=self.send,
            recv_sem=sem,
            device_id={"fs": to},
            device_id_type=MESH,
        )

    def ref(self, k, stage, po, s, half):
        if self.near and k == 0 and (stage == 1 or (stage == 3 and po == 0)):
            return self.near(s)
        return self.part(s, k, half)

    def start(self, k, stage, po, d):
        first = stage in (1, 2)
        at = {1: (0, 0), 2: (-d, 0), 3: (po, 0), 4: (po, -d)}[stage]
        half = None if stage in (1, 3) else (0 if d > 0 else 1)
        to = self.slot(k, d, 0) if first else self.slot(k, 0, d)
        ref = self.ref(k, stage, po, self.slot(k, *at), half)
        self.copy(ref, k, stage, po, d, to).start()

    def wait(self, k, stage, po, d=0):
        at = {1: (-d, 0), 2: (2, 0), 3: (po, -d), 4: (po, 2)}[stage]
        ref = self.ref(k, stage, po, self.slot(k, *at), None)
        with jax.named_scope(f"w{self.name}_{k}_{stage}_{po}_{d}"):
            self.copy(ref, k, stage, po, d, self.slot(k, 1, 0)).wait_recv()

    def steps(self, arrived):
        for stage in (1, 3):
            for d in (1, -1):
                for k in (0, 1):
                    self.start(k, stage, 0, d)
        yield "start"
        for d in (1, -1):
            for k in (0, 1):
                self.wait(k, 1, 0, d)
                self.start(k, 2, 0, d)
                arrived(k, -d, 0)
        for po in (-1, 1):
            for d in (1, -1):
                for k in (0, 1):
                    self.start(k, 3, po, d)
        yield "1"
        self.second(arrived, 0)
        yield "3_0"
        for k in (0, 1):
            self.wait(k, 2, 0)
            self.start(k, 3, 2, 1)
            self.start(k, 3, 2, -1)
            arrived(k, 2, 0)
        yield "2"
        for po in (-1, 1):
            self.second(arrived, po)
            yield f"3_{po}"
        self.last(arrived, 0)
        yield "4_0"
        self.second(arrived, 2)
        yield "3_2"
        for po in (-1, 1, 2):
            self.last(arrived, po)
            yield f"4_{po}"

    def second(self, arrived, po):
        for d in (1, -1):
            for k in (0, 1):
                self.wait(k, 3, po, d)
                self.start(k, 4, po, d)
                arrived(k, po, -d)

    def last(self, arrived, po):
        for k in (0, 1):
            self.wait(k, 4, po)
            arrived(k, po, 2)

    def finish(self, everything):
        self.copy(everything, 0, 1, 0, 1, self.slot(0, 1, 0)).wait_send()


def high_low(values):
    upper = values.astype(BF16)
    return upper, (values - upper.astype(F32)).astype(BF16)


def kernel(
    inputs,
    value_cot,
    gate_cot,
    out_cot,
    conv_output,
    factors,
    value_weight,
    gate_weight,
    out_weight,
    first_moment,
    second_moment,
    mom,
    upd,
    copies,
    left,
    cots,
    cots_t,
    fbuf,
    wbuf,
    near_w,
    summed,
    pieces,
    from_core,
    arrived,
    dirs,
    sums,
    fs_sums,
    load_sem,
    ring_send,
    ring_recv,
    core_send,
    core_recv,
    batch_recv,
    a_send,
    a_recv,
    d_send,
    d_recv,
    s_send,
    s_recv,
    w_send,
    w_recv,
):
    me = lax.axis_index("fs")
    t = lax.axis_index("tp")
    core = lax.rem(t, 2)
    partner = t + 1 - 2 * core

    barrier = pltpu.get_barrier_semaphore()

    def greet_fs(j, _):
        pl.semaphore_signal(
            barrier, inc=1, device_id={"fs": lax.rem(me + j, FS)}, device_id_type=MESH
        )
        return _

    def greet_tp(j, _):
        pl.semaphore_signal(
            barrier, inc=1, device_id={"tp": lax.rem(t + j, TP)}, device_id_type=MESH
        )
        return _

    lax.fori_loop(1, FS, greet_fs, 0)
    lax.fori_loop(1, TP, greet_tp, 0)

    def load(at, *pairs):
        for src, dst in pairs:
            pltpu.make_async_copy(src, dst, load_sem.at[at]).start()

    def loaded(at, ref):
        pltpu.make_async_copy(ref, ref, load_sem.at[at]).wait()

    half = pl.ds(pl.multiple_of(core * HALF, HALF), HALF)
    load(0, (factors, fbuf.at[me]))
    load(1, *((r, cots.at[m]) for m, r in enumerate((value_cot, gate_cot, conv_output))))

    def load_half(s, carry):
        src = pl.ds(pl.multiple_of(s * W + core * HALF, HALF), HALF)
        dst = pl.ds(pl.multiple_of(s * HALF, HALF), HALF)
        load(2, (inputs.at[:, src], left.at[0, :, dst]))
        load(3, (out_cot.at[:, src], left.at[1, :, dst]))
        return carry

    lax.fori_loop(0, FS, load_half, 0)
    load(4, (first_moment, mom.at[0]), (second_moment, mom.at[1]))
    load(5, *((r, wbuf.at[m]) for m, r in enumerate((value_weight, gate_weight, out_weight))))

    with jax.named_scope("barrier"):
        pl.semaphore_wait(barrier, FS - 1 + TP - 1)

    def to_partner(src, dst, at):
        return pltpu.make_async_remote_copy(
            src_ref=src,
            dst_ref=dst,
            send_sem=core_send.at[0],
            recv_sem=core_recv.at[at],
            device_id={"tp": partner},
            device_id_type=MESH,
        )

    def factor_part(s, k, half):
        at, size = HALF * k, HALF
        if half is not None:
            at, size = at + 64 * half, 64
        return fbuf.at[s, pl.ds(odd_base, 2), pl.ds(at, size), :]

    y = t // 2
    odd = lax.rem(y, 2)
    odd_base = 1 - odd
    lacking, handed = 2 * odd, 2 - 2 * odd

    def along_y(ref, k):
        to = lax.rem(2 * y + (2 if k == 0 else TP - 2), TP) + k
        return pltpu.make_async_remote_copy(
            src_ref=ref,
            dst_ref=ref,
            send_sem=core_send.at[1],
            recv_sem=core_recv.at[4],
            device_id={"tp": to},
            device_id_type=MESH,
        )

    ring = RingGather("a", me, factor_part, ring_send.at[0], ring_recv)
    here = []

    def to_other_core(ref, batch):
        return pltpu.make_async_remote_copy(
            src_ref=ref,
            dst_ref=ref,
            send_sem=core_send.at[2],
            recv_sem=batch_recv.at[batch],
            device_id={"tp": partner},
            device_id_type=MESH,
        )

    def factor_arrived(k, po, qo):
        s = ring.slot(k, po, qo)
        if k == 0:
            here.append((po, qo))
            to_other_core(factor_part(s, 0, None), state["batch"]).start()
        along_y(fbuf.at[s, handed, pl.ds(HALF * k, HALF), :], k).start()

    state = {"batch": 0}
    groups = ring.steps(factor_arrived)

    def slots_until(group):
        @pl.when(core == 1)
        def _():
            while next(groups) != group:
                pass

        count = len(here)

        @pl.when(core == 0)
        def _():
            with jax.named_scope("wait_batch"):
                ref = fbuf.at[pl.ds(0, count), pl.ds(0, 2), pl.ds(0, HALF), :]
                to_other_core(ref, state["batch"]).wait_recv()

        slots = []
        for po, qo in here:
            zero, one = ring.slot(0, po, qo), ring.slot(1, po, qo)
            slots.append(zero + core * (one - zero))
        here.clear()
        state["batch"] += 1
        return slots

    def multiply(*slots, first=False, matrices=(odd_base, odd_base + 1)):
        with jax.named_scope("multiply"):
            for m in matrices:
                ours = [
                    left[m // 2, :, pl.ds(pl.multiple_of(s * HALF, HALF), HALF)]
                    for s in slots
                ]
                product = jnp.dot(
                    jnp.concatenate(ours, axis=1),
                    jnp.concatenate([fbuf[s, m, half, :] for s in slots], axis=0),
                    preferred_element_type=F32,
                )
                if first:
                    summed[m] = product
                else:
                    summed[m] += product

    def multiply_lacking():
        with jax.named_scope("multiply_lacking"):
            right = fbuf[:, lacking, half, :].reshape(D // 2, RANK)

            def tile(i, carry):
                rows = pl.ds(pl.multiple_of(i * 512, 512), 512)
                ours = left[lacking // 2, rows, :]
                summed[lacking, rows, :] = jnp.dot(ours, right, preferred_element_type=F32)
                return carry

            lax.fori_loop(0, TOK // 512, tile, 0)

    def loop(start, stop, step):
        def body(j, carry):
            step(j)
            return carry

        lax.fori_loop(start, stop, body, 0)

    def to_fs(src, dst, send, recv, j):
        return pltpu.make_async_remote_copy(
            src_ref=src,
            dst_ref=dst,
            send_sem=send,
            recv_sem=recv,
            device_id={"fs": lax.rem(me + j, FS)},
            device_id_type=MESH,
        )

    others = pl.ds(0, FS - 1)

    def project(m):
        with jax.named_scope("project"):
            split = jnp.concatenate(high_low(summed[m]), axis=1)
            for side in (1, 0):
                product = jnp.dot(cots_t[side, m], split, preferred_element_type=F32)
                product = product[:, :RANK] + product[:, RANK:]
                pieces[side, m] = product.T.reshape(FS, RS, W)
                if side == 1:
                    to_partner(pieces.at[1, m], from_core.at[m], m).start()

    def send_pieces(m):
        with jax.named_scope("wait_core"):
            to_partner(pieces.at[1, m], from_core.at[m], m).wait_recv()
        pieces[0, m] += from_core[m]

        def send_piece(j):
            to_fs(
                pieces.at[0, m, lax.rem(me + j, FS)],
                arrived.at[m, me],
                a_send.at[0],
                a_recv.at[m],
                j,
            ).start()

        loop(1, FS, send_piece)
        arrived[m, me] = pieces[0, m, me]

    def to_tp(ref, j):
        return pltpu.make_async_remote_copy(
            src_ref=ref,
            dst_ref=ref,
            send_sem=s_send.at[0],
            recv_sem=s_recv.at[0],
            device_id={"tp": lax.rem(t + j, TP)},
            device_id_type=MESH,
        )

    squares = []

    def moments(m):
        with jax.named_scope("wait_pieces"):
            ref = arrived.at[m, others]
            to_fs(ref, ref, a_send.at[0], a_recv.at[m], 1).wait_recv()
        projected = jnp.sum(arrived[m], axis=0)
        new_first = FIRST_DECAY * mom[0, m] + (1.0 - FIRST_DECAY) * projected
        new_second = (
            SECOND_DECAY * mom[1, m] + (1.0 - SECOND_DECAY) * projected * projected
        )
        direction = new_first / (jnp.sqrt(new_second) + DIVISOR_EPS)
        mom[0, m] = new_first
        mom[1, m] = new_second
        dirs[m, me] = direction
        squares.append(jnp.sum(direction * direction, axis=0, keepdims=True))
        if len(squares) == 3:
            square = squares[0] + squares[1] + squares[2]
            sums[t] = square[:, :128] + square[:, 128:]
            loop(1, TP, lambda j: to_tp(sums.at[t], j).start())

        def send_direction(j):
            ref = dirs.at[m, me]
            to_fs(ref, ref, d_send.at[0], d_recv.at[m], j).start()

        loop(1, FS, send_direction)

    loaded(0, fbuf.at[me])

    @pl.when(core == 1)
    def _():
        next(groups)

    with jax.named_scope("turn"):
        loaded(1, cots)
        for m in range(3):

            def turn(i, _):
                rows = pl.ds(pl.multiple_of(i * 256, 256), 256)
                cots_t[0, m, :, rows] = cots[m, rows, :].T
                return _

            lax.fori_loop(0, TOK // 256, turn, 0)

    to_partner(cots_t.at[0], cots_t.at[1], 3).start()
    with jax.named_scope("wait_loads"):
        loaded(2, left.at[0])
        loaded(3, left.at[1])
    multiply(me, first=True)
    near_slots = [ring.slot(0, *at) for at in ((-1, 0), (1, 0), (0, -1), (0, 1))]

    def weights_to(i):
        at = ((1, 0), (-1, 0), (0, 1), (0, -1))[i]
        return pltpu.make_async_remote_copy(
            src_ref=wbuf.at[pl.ds(0, 2), half, :],
            dst_ref=near_w.at[i],
            send_sem=w_send.at[0],
            recv_sem=w_recv.at[0],
            device_id={"fs": ring.slot(0, *at)},
            device_id_type=MESH,
        )

    def all_weights():
        return pltpu.make_async_remote_copy(
            src_ref=near_w,
            dst_ref=near_w,
            send_sem=w_send.at[0],
            recv_sem=w_recv.at[0],
            device_id={"fs": near_slots[0]},
            device_id_type=MESH,
        )

    for group in ("3_0", "3_1", "3_2", "4_1"):
        slots = slots_until(group)
        if group == "3_2":
            loaded(5, wbuf)
            for i in range(4):
                weights_to(i).start()
        multiply(*slots)
    to_partner(cots_t.at[0], cots_t.at[1], 3).wait_recv()
    last = slots_until("4_2")
    order = (odd_base, odd_base + 1, lacking)
    multiply(*last, matrices=order[:1])
    project(order[0])
    multiply(*last, matrices=order[1:2])
    send_pieces(order[0])
    project(order[1])
    send_pieces(order[1])
    with jax.named_scope("wait_y"):
        along_y(fbuf.at[others, 0, pl.ds(0, HALF)], 0).wait_recv()
    multiply_lacking()
    project(order[2])
    send_pieces(order[2])
    loaded(4, mom)
    for m in order:
        moments(m)

    def wait_directions(m):
        with jax.named_scope("wait_directions"):
            ref = dirs.at[m, others]
            to_fs(ref, ref, d_send.at[0], d_recv.at[m], 1).wait_recv()

    def update(m):
        full = dirs[m].reshape(RANK, W)
        if m == 2:
            upper, lower = high_low(full.T)
            contract = (((1,), (1,)), ((), ()))
            own = fbuf[me, m]
            product = lax.dot_general(upper, own, contract, preferred_element_type=F32)
            product += lax.dot_general(lower, own, contract, preferred_element_type=F32)
        else:
            upper, lower = high_low(full)
            product = jnp.dot(fbuf[me, m], upper, preferred_element_type=F32)
            product += jnp.dot(fbuf[me, m], lower, preferred_element_type=F32)
        upd[m] = product

    wait_directions(order[0])
    with jax.named_scope("wait_scalar"):
        to_tp(sums.at[pl.ds(0, TP - 1)], 1).wait_recv()
    fs_sums[me] = jnp.sum(sums[...], axis=0)

    def send_sum(j):
        ref = fs_sums.at[me]
        to_fs(ref, ref, s_send.at[1], s_recv.at[1], j).start()

    loop(1, FS, send_sum)
    wait_directions(order[1])
    update(1)

    @pl.when(odd == 1)
    def _():
        update(0)

    @pl.when(odd == 0)
    def _():
        update(2)

    @pl.when(core == 1)
    def _():
        ring.finish(fbuf.at[others, pl.ds(0, 2)])
        along_y(fbuf.at[others, 0], 0).wait_send()
        to_other_core(fbuf.at[others, pl.ds(0, 2), pl.ds(0, HALF)], 0).wait_send()

    wait_directions(order[2])

    @pl.when(odd == 0)
    def _():
        update(0)

    @pl.when(odd == 1)
    def _():
        update(2)

    with jax.named_scope("wait_fs_scalar"):
        ref = fs_sums.at[others]
        to_fs(ref, ref, s_send.at[1], s_recv.at[1], 1).wait_recv()
    total = jnp.sum(jnp.sum(fs_sums[...], axis=0), keepdims=True)
    norm_scale = lax.rsqrt(total / (3 * RANK * C) + SQUARE_EPS)
    for m in range(3):
        scaled = norm_scale * upd[m]
        upd[m] = scaled
        copies[me, m] = (wbuf[m] - LEARN_RATE * scaled).astype(BF16)

    def copy_part(s, k, part_half):
        at, size = HALF * (k + core - 2 * k * core), HALF
        if part_half is not None:
            at, size = at + 64 * part_half, 64
        return copies.at[s, :, pl.ds(pl.multiple_of(at, 64), size), :]

    def copy_near(s):
        return copies.at[s, pl.ds(2, 1), half, :]

    def near_copies():
        with jax.named_scope("wait_near"):
            all_weights().wait_recv()
        with jax.named_scope("near"):
            for m in range(2):
                upper, lower = high_low(dirs[m].reshape(RANK, W))
                rows = jnp.concatenate([fbuf[s, m, half, :] for s in near_slots], axis=0)
                product = jnp.dot(rows, upper, preferred_element_type=F32)
                product += jnp.dot(rows, lower, preferred_element_type=F32)
                scaled = norm_scale * product
                for i, s in enumerate(near_slots):
                    update = scaled[HALF * i : HALF * (i + 1)]
                    copies[s, m, half, :] = (near_w[i, m] - LEARN_RATE * update).astype(BF16)

    gather = RingGather("c", me, copy_part, ring_send.at[0], ring_recv, copy_near)
    for group in gather.steps(lambda k, po, qo: None):
        if group == "start":
            near_copies()

    with jax.named_scope("finish"):
        gather.finish(copies.at[pl.ds(0, 13)])
        gather.finish(copies.at[pl.ds(0, 4), 0, pl.ds(0, HALF)])
        all_weights().wait_send()
        to_partner(cots_t.at[0], cots_t.at[1], 3).wait_send()
        for m in range(3):
            to_partner(pieces.at[1, m], from_core.at[m], m).wait_send()
            ref = pieces.at[0, m, others]
            to_fs(ref, ref, a_send.at[0], a_recv.at[m], 1).wait_send()
            ref = dirs.at[m, others]
            to_fs(ref, ref, d_send.at[0], d_recv.at[m], 1).wait_send()
        to_tp(sums.at[pl.ds(0, TP - 1)], 1).wait_send()
        ref = fs_sums.at[others]
        to_fs(ref, ref, s_send.at[1], s_recv.at[1], 1).wait_send()


def store_kernel(
    mom,
    upd,
    copies,
    first_out,
    second_out,
    value_update,
    gate_update,
    out_update,
    value_copy,
    gate_copy,
    out_copy,
    sem,
):
    def store(src, dst):
        pltpu.make_async_copy(src, dst, sem.at[0]).start()

    def store_block(s, carry):
        at = pl.ds(pl.multiple_of(s * W, W), W)
        store(copies.at[s, 0], value_copy.at[at, :])
        store(copies.at[s, 1], gate_copy.at[at, :])
        store(copies.at[s, 2], out_copy.at[:, at])
        return carry

    lax.fori_loop(0, FS, store_block, 0)
    store(upd.at[0], value_update)
    store(upd.at[1], gate_update)
    store(upd.at[2], out_update)
    store(mom.at[0], first_out)
    store(mom.at[1], second_out)
    for ref in (copies, upd, mom):
        pltpu.make_async_copy(ref, ref, sem.at[0]).wait()


def shards(*args):
    anywhere = pl.BlockSpec(memory_space=pl.ANY)
    vmem = pl.BlockSpec(memory_space=pltpu.VMEM)
    dma = pltpu.SemaphoreType.DMA
    results = pl.pallas_call(
        kernel,
        out_shape=(
            pltpu.VMEM((2, 3, RS, W), F32),
            pltpu.VMEM((3, W, W), F32),
            pltpu.VMEM((FS, 3, W, W), BF16),
        ),
        in_specs=[anywhere] * 11,
        out_specs=(vmem,) * 3,
        scratch_shapes=[
            pltpu.VMEM((2, TOK, D // 2), BF16),
            pltpu.VMEM((3, TOK, W), BF16),
            pltpu.VMEM((2, 3, W, TOK), BF16),
            pltpu.VMEM((FS, 3, W, RANK), BF16),
            pltpu.VMEM((3, W, W), F32),
            pltpu.VMEM((4, 2, HALF, W), F32),
            pltpu.VMEM((3, TOK, RANK), F32),
            pltpu.VMEM((2, 3, FS, RS, W), F32),
            pltpu.VMEM((3, FS, RS, W), F32),
            pltpu.VMEM((3, FS, RS, W), F32),
            pltpu.VMEM((3, FS, RS, W), F32),
            pltpu.VMEM((TP, 1, 128), F32),
            pltpu.VMEM((FS, 1, 128), F32),
            dma((6,)),
            dma((1,)),
            dma((len(RECEIVED),)),
            dma((3,)),
            dma((5,)),
            dma((5,)),
            dma((1,)),
            dma((3,)),
            dma((1,)),
            dma((3,)),
            dma((2,)),
            dma((2,)),
            dma((1,)),
            dma((1,)),
        ],
        compiler_params=pltpu.CompilerParams(
            collective_id=0, has_side_effects=True, vmem_limit_bytes=48 * 1024 * 1024
        ),
    )(*[pltpu.with_memory_space_constraint(a, pltpu.HBM) for a in args])
    return pl.pallas_call(
        store_kernel,
        out_shape=(
            jax.ShapeDtypeStruct((3, RS, W), F32),
            jax.ShapeDtypeStruct((3, RS, W), F32),
            jax.ShapeDtypeStruct((W, W), F32),
            jax.ShapeDtypeStruct((W, W), F32),
            jax.ShapeDtypeStruct((W, W), F32),
            jax.ShapeDtypeStruct((D, W), BF16),
            jax.ShapeDtypeStruct((D, W), BF16),
            jax.ShapeDtypeStruct((W, D), BF16),
        ),
        in_specs=[vmem] * 3,
        out_specs=(anywhere,) * 8,
        scratch_shapes=[dma((1,))],
        compiler_params=pltpu.CompilerParams(vmem_limit_bytes=4 * 1024 * 1024),
    )(*[pltpu.with_memory_space_constraint(r, pltpu.VMEM) for r in results])


def solution(mesh):
    placed = (
        P("fs", None),
        P("fs", "tp"),
        P("fs", "tp"),
        P("fs", None),
        P("fs", "tp"),
        P(None, "fs", None),
        P("fs", "tp"),
        P("fs", "tp"),
        P("tp", "fs"),
        P(None, "fs", "tp"),
        P(None, "fs", "tp"),
    )
    return jax.shard_map(
        shards,
        mesh=mesh,
        in_specs=placed,
        out_specs=(
            P(None, "fs", "tp"),
            P(None, "fs", "tp"),
            P("fs", "tp"),
            P("fs", "tp"),
            P("tp", "fs"),
            P(None, "tp"),
            P(None, "tp"),
            P("tp", None),
        ),
        check_vma=False,
    )
```

```python
import functools

import jax
import jax.numpy as jnp
from jax import lax
from jax.experimental import pallas as pl
from jax.experimental.pallas import tpu as pltpu
from jax.sharding import PartitionSpec as P

C = 2048
RANK = 256
FIRST_DECAY = 0.9
SECOND_DECAY = 0.95
DIVISOR_EPS = 1e-08
SQUARE_EPS = 1e-06
LEARN_RATE = 0.01

SIDE = 4
FS = SIDE * SIDE
TP = 8
HALF = 128
W = 256
RS = RANK // FS
TOK = 1024
D = 4096
MESH = pl.DeviceIdType.MESH
F32 = jnp.float32
BF16 = jnp.bfloat16

RECEIVED = []
for _k in (0, 1):
    RECEIVED += [(_k, 1, 0, 1), (_k, 1, 0, -1), (_k, 2, 0, 0)]
    for _po in (0, -1, 1, 2):
        RECEIVED += [(_k, 3, _po, 1), (_k, 3, _po, -1), (_k, 4, _po, 0)]
INDEX = {message: at for at, message in enumerate(RECEIVED)}


class RingGather:
    def __init__(self, name, me, part, send, recv, near=False):
        self.near = near
        self.name = name
        self.z, self.x = me // SIDE, lax.rem(me, SIDE)
        self.part, self.send, self.recv = part, send, recv

    def slot(self, k, po, qo):
        dx, dz = (po, qo) if k == 0 else (qo, po)
        z = lax.rem(self.z + dz + SIDE, SIDE)
        x = lax.rem(self.x + dx + SIDE, SIDE)
        return z * SIDE + x

    def copy(self, ref, k, stage, po, d, to):
        sem = self.recv.at[INDEX[k, stage, po, 0 if stage in (2, 4) else d]]
        return pltpu.make_async_remote_copy(
            src_ref=ref,
            dst_ref=ref,
            send_sem=self.send,
            recv_sem=sem,
            device_id={"fs": to},
            device_id_type=MESH,
        )

    def skipped(self, k, stage, po):
        return self.near and k == 0 and (stage == 1 or (stage == 3 and po == 0))

    def start(self, k, stage, po, d):
        first = stage in (1, 2)
        at = {1: (0, 0), 2: (-d, 0), 3: (po, 0), 4: (po, -d)}[stage]
        half = None if stage in (1, 3) else (0 if d > 0 else 1)
        to = self.slot(k, d, 0) if first else self.slot(k, 0, d)
        if self.skipped(k, stage, po):
            return
        ref = self.part(self.slot(k, *at), k, half)
        self.copy(ref, k, stage, po, d, to).start()

    def wait(self, k, stage, po, d=0):
        at = {1: (-d, 0), 2: (2, 0), 3: (po, -d), 4: (po, 2)}[stage]
        ref = self.part(self.slot(k, *at), k, None)
        with jax.named_scope(f"w{self.name}_{k}_{stage}_{po}_{d}"):
            self.copy(ref, k, stage, po, d, self.slot(k, 1, 0)).wait_recv()

    def steps(self, arrived):
        for stage in (1, 3):
            for d in (1, -1):
                for k in (0, 1):
                    self.start(k, stage, 0, d)
        yield "start"
        if self.near:
            for d in (1, -1):
                self.start(0, 2, 0, d)
                self.start(0, 4, 0, d)
        for d in (1, -1):
            for k in (1,) if self.near else (0, 1):
                self.wait(k, 1, 0, d)
                self.start(k, 2, 0, d)
                arrived(k, -d, 0)
        for po in (-1, 1):
            for d in (1, -1):
                for k in (0, 1):
                    self.start(k, 3, po, d)
        yield "1"
        self.second(arrived, 0)
        yield "3_0"
        for k in (0, 1):
            self.wait(k, 2, 0)
            self.start(k, 3, 2, 1)
            self.start(k, 3, 2, -1)
            arrived(k, 2, 0)
        yield "2"
        for po in (-1, 1):
            self.second(arrived, po)
            yield f"3_{po}"
        self.last(arrived, 0)
        yield "4_0"
        self.second(arrived, 2)
        yield "3_2"
        for po in (-1, 1, 2):
            self.last(arrived, po)
            yield f"4_{po}"

    def second(self, arrived, po):
        for d in (1, -1):
            for k in (0, 1):
                if not self.skipped(k, 3, po):
                    self.wait(k, 3, po, d)
                    self.start(k, 4, po, d)
                arrived(k, po, -d)

    def last(self, arrived, po):
        for k in (0, 1):
            self.wait(k, 4, po)
            arrived(k, po, 2)

    def finish(self, everything):
        self.copy(everything, 0, 1, 0, 1, self.slot(0, 1, 0)).wait_send()


def high_low(values):
    upper = values.astype(BF16)
    return upper, (values - upper.astype(F32)).astype(BF16)


def kernel(
    inputs,
    value_cot,
    gate_cot,
    out_cot,
    conv_output,
    factors,
    value_weight,
    gate_weight,
    out_weight,
    first_moment,
    second_moment,
    mom,
    upd,
    copies,
    left,
    cots,
    cots_t,
    fbuf,
    wbuf,
    near_w,
    near_out,
    near_f,
    turned,
    summed,
    pieces,
    from_core,
    arrived,
    dirs,
    sums,
    fs_sums,
    load_sem,
    ring_send,
    ring_recv,
    core_send,
    core_recv,
    batch_recv,
    a_send,
    a_recv,
    d_send,
    d_recv,
    s_send,
    s_recv,
    w_send,
    w_recv,
):
    me = lax.axis_index("fs")
    t = lax.axis_index("tp")
    core = lax.rem(t, 2)
    partner = t + 1 - 2 * core

    barrier = pltpu.get_barrier_semaphore()

    def greet_fs(j, _):
        pl.semaphore_signal(
            barrier, inc=1, device_id={"fs": lax.rem(me + j, FS)}, device_id_type=MESH
        )
        return _

    def greet_tp(j, _):
        pl.semaphore_signal(
            barrier, inc=1, device_id={"tp": lax.rem(t + j, TP)}, device_id_type=MESH
        )
        return _

    lax.fori_loop(1, FS, greet_fs, 0)
    lax.fori_loop(1, TP, greet_tp, 0)

    def load(at, *pairs):
        for src, dst in pairs:
            pltpu.make_async_copy(src, dst, load_sem.at[at]).start()

    def loaded(at, ref):
        pltpu.make_async_copy(ref, ref, load_sem.at[at]).wait()

    half = pl.ds(pl.multiple_of(core * HALF, HALF), HALF)
    load(0, (factors, fbuf.at[me]))
    load(1, *((r, cots.at[m]) for m, r in enumerate((value_cot, gate_cot, conv_output))))

    def load_half(s, carry):
        src = pl.ds(pl.multiple_of(s * W + core * HALF, HALF), HALF)
        dst = pl.ds(pl.multiple_of(s * HALF, HALF), HALF)
        load(2, (inputs.at[:, src], left.at[0, :, dst]))
        load(3, (out_cot.at[:, src], left.at[1, :, dst]))
        return carry

    lax.fori_loop(0, FS, load_half, 0)
    load(4, (first_moment, mom.at[0]), (second_moment, mom.at[1]))
    load(5, *((r, wbuf.at[m]) for m, r in enumerate((value_weight, gate_weight, out_weight))))

    with jax.named_scope("barrier"):
        pl.semaphore_wait(barrier, FS - 1 + TP - 1)

    def to_partner(src, dst, at):
        return pltpu.make_async_remote_copy(
            src_ref=src,
            dst_ref=dst,
            send_sem=core_send.at[0],
            recv_sem=core_recv.at[at],
            device_id={"tp": partner},
            device_id_type=MESH,
        )

    def factor_part(s, k, half):
        at, size = HALF * k, HALF
        if half is not None:
            at, size = at + 64 * half, 64
        return fbuf.at[s, pl.ds(odd_base, 2), pl.ds(at, size), :]

    y = t // 2
    odd = lax.rem(y, 2)
    odd_base = 1 - odd
    lacking, handed = 2 * odd, 2 - 2 * odd

    def along_y(ref, k):
        to = lax.rem(2 * y + (2 if k == 0 else TP - 2), TP) + k
        return pltpu.make_async_remote_copy(
            src_ref=ref,
            dst_ref=ref,
            send_sem=core_send.at[1],
            recv_sem=core_recv.at[4],
            device_id={"tp": to},
            device_id_type=MESH,
        )

    ring = RingGather("a", me, factor_part, ring_send.at[0], ring_recv)
    here = []

    def to_other_core(ref, batch):
        return pltpu.make_async_remote_copy(
            src_ref=ref,
            dst_ref=ref,
            send_sem=core_send.at[2],
            recv_sem=batch_recv.at[batch],
            device_id={"tp": partner},
            device_id_type=MESH,
        )

    def factor_arrived(k, po, qo):
        s = ring.slot(k, po, qo)
        if k == 0:
            here.append((po, qo))
            to_other_core(factor_part(s, 0, None), state["batch"]).start()
        along_y(fbuf.at[s, handed, pl.ds(HALF * k, HALF), :], k).start()

    state = {"batch": 0}
    groups = ring.steps(factor_arrived)

    def slots_until(group):
        @pl.when(core == 1)
        def _():
            while next(groups) != group:
                pass

        count = len(here)

        @pl.when(core == 0)
        def _():
            with jax.named_scope("wait_batch"):
                ref = fbuf.at[pl.ds(0, count), pl.ds(0, 2), pl.ds(0, HALF), :]
                to_other_core(ref, state["batch"]).wait_recv()

        slots = []
        for po, qo in here:
            zero, one = ring.slot(0, po, qo), ring.slot(1, po, qo)
            slots.append(zero + core * (one - zero))
        here.clear()
        state["batch"] += 1
        return slots

    def multiply(*slots, first=False, matrices=(odd_base, odd_base + 1)):
        with jax.named_scope("multiply"):
            for m in matrices:
                ours = [
                    left[m // 2, :, pl.ds(pl.multiple_of(s * HALF, HALF), HALF)]
                    for s in slots
                ]
                product = jnp.dot(
                    jnp.concatenate(ours, axis=1),
                    jnp.concatenate([fbuf[s, m, half, :] for s in slots], axis=0),
                    preferred_element_type=F32,
                )
                if first:
                    summed[m] = product
                else:
                    summed[m] += product

    def multiply_lacking():
        with jax.named_scope("multiply_lacking"):
            right = fbuf[:, lacking, half, :].reshape(D // 2, RANK)

            def tile(i, carry):
                rows = pl.ds(pl.multiple_of(i * 512, 512), 512)
                ours = left[lacking // 2, rows, :]
                summed[lacking, rows, :] = jnp.dot(ours, right, preferred_element_type=F32)
                return carry

            lax.fori_loop(0, TOK // 512, tile, 0)

    def loop(start, stop, step):
        def body(j, carry):
            step(j)
            return carry

        lax.fori_loop(start, stop, body, 0)

    def to_fs(src, dst, send, recv, j):
        return pltpu.make_async_remote_copy(
            src_ref=src,
            dst_ref=dst,
            send_sem=send,
            recv_sem=recv,
            device_id={"fs": lax.rem(me + j, FS)},
            device_id_type=MESH,
        )

    others = pl.ds(0, FS - 1)

    def project(m):
        with jax.named_scope("project"):
            split = jnp.concatenate(high_low(summed[m]), axis=1)
            for side in (1, 0):
                product = jnp.dot(cots_t[side, m], split, preferred_element_type=F32)
                product = product[:, :RANK] + product[:, RANK:]
                pieces[side, m] = product.T.reshape(FS, RS, W)
                if side == 1:
                    to_partner(pieces.at[1, m], from_core.at[m], m).start()

    def send_pieces(m):
        with jax.named_scope("wait_core"):
            to_partner(pieces.at[1, m], from_core.at[m], m).wait_recv()
        pieces[0, m] += from_core[m]

        def send_piece(j):
            to_fs(
                pieces.at[0, m, lax.rem(me + j, FS)],
                arrived.at[m, me],
                a_send.at[0],
                a_recv.at[m],
                j,
            ).start()

        loop(1, FS, send_piece)
        arrived[m, me] = pieces[0, m, me]

    def to_tp(ref, j):
        return pltpu.make_async_remote_copy(
            src_ref=ref,
            dst_ref=ref,
            send_sem=s_send.at[0],
            recv_sem=s_recv.at[0],
            device_id={"tp": lax.rem(t + j, TP)},
            device_id_type=MESH,
        )

    squares = []

    def moments(m):
        with jax.named_scope("wait_pieces"):
            ref = arrived.at[m, others]
            to_fs(ref, ref, a_send.at[0], a_recv.at[m], 1).wait_recv()
        projected = jnp.sum(arrived[m], axis=0)
        new_first = FIRST_DECAY * mom[0, m] + (1.0 - FIRST_DECAY) * projected
        new_second = (
            SECOND_DECAY * mom[1, m] + (1.0 - SECOND_DECAY) * projected * projected
        )
        direction = new_first / (jnp.sqrt(new_second) + DIVISOR_EPS)
        mom[0, m] = new_first
        mom[1, m] = new_second
        dirs[m, me] = direction
        squares.append(jnp.sum(direction * direction, axis=0, keepdims=True))
        if len(squares) == 3:
            square = squares[0] + squares[1] + squares[2]
            sums[t] = square[:, :128] + square[:, 128:]
            loop(1, TP, lambda j: to_tp(sums.at[t], j).start())

        def send_direction(j):
            ref = dirs.at[m, me]
            to_fs(ref, ref, d_send.at[0], d_recv.at[m], j).start()

        loop(1, FS, send_direction)

    loaded(0, fbuf.at[me])

    @pl.when(core == 1)
    def _():
        next(groups)

    with jax.named_scope("turn"):
        loaded(1, cots)
        for m in range(3):

            def turn(i, _):
                rows = pl.ds(pl.multiple_of(i * 256, 256), 256)
                cots_t[0, m, :, rows] = cots[m, rows, :].T
                return _

            lax.fori_loop(0, TOK // 256, turn, 0)

    to_partner(cots_t.at[0], cots_t.at[1], 3).start()
    with jax.named_scope("wait_loads"):
        loaded(2, left.at[0])
        loaded(3, left.at[1])
    multiply(me, first=True)
    near_slots = [ring.slot(0, *at) for at in ((-1, 0), (1, 0), (0, -1), (0, 1))]

    def weights_to(i, src, dst, at):
        to = ((1, 0), (-1, 0), (0, 1), (0, -1))[i]
        return pltpu.make_async_remote_copy(
            src_ref=src,
            dst_ref=dst,
            send_sem=w_send.at[at],
            recv_sem=w_recv.at[at],
            device_id={"fs": ring.slot(0, *to)},
            device_id_type=MESH,
        )

    for group in ("3_0", "3_1", "3_2", "4_1"):
        slots = slots_until(group)
        if group == "3_2":
            loaded(5, wbuf)
            for i in range(4):
                weights_to(i, wbuf.at[pl.ds(0, 2), half, :], near_w.at[i], 0).start()
        multiply(*slots)
    to_partner(cots_t.at[0], cots_t.at[1], 3).wait_recv()
    last = slots_until("4_2")
    order = (odd_base, odd_base + 1, lacking)
    multiply(*last, matrices=order[:1])
    project(order[0])
    multiply(*last, matrices=order[1:2])
    send_pieces(order[0])
    project(order[1])
    send_pieces(order[1])
    with jax.named_scope("wait_y"):
        along_y(fbuf.at[others, 0, pl.ds(0, HALF)], 0).wait_recv()

    def near_factor(i):
        return pltpu.make_async_remote_copy(
            src_ref=fbuf.at[near_slots[i], 2, half, :],
            dst_ref=near_f.at[i],
            send_sem=w_send.at[1],
            recv_sem=w_recv.at[1],
            device_id={"tp": partner},
            device_id_type=MESH,
        )

    def near_factors():
        return pltpu.make_async_remote_copy(
            src_ref=near_f,
            dst_ref=near_f,
            send_sem=w_send.at[1],
            recv_sem=w_recv.at[1],
            device_id={"tp": partner},
            device_id_type=MESH,
        )

    for i in range(4):
        near_factor(i).start()
    multiply_lacking()
    project(order[2])
    send_pieces(order[2])
    loaded(4, mom)
    for m in order:
        moments(m)

    def wait_directions(m):
        with jax.named_scope("wait_directions"):
            ref = dirs.at[m, others]
            to_fs(ref, ref, d_send.at[0], d_recv.at[m], 1).wait_recv()

    def update(m):
        full = dirs[m].reshape(RANK, W)
        if m == 2:
            upper, lower = high_low(full.T)
            contract = (((1,), (1,)), ((), ()))
            own = fbuf[me, m]
            product = lax.dot_general(upper, own, contract, preferred_element_type=F32)
            product += lax.dot_general(lower, own, contract, preferred_element_type=F32)
        else:
            upper, lower = high_low(full)
            product = jnp.dot(fbuf[me, m], upper, preferred_element_type=F32)
            product += jnp.dot(fbuf[me, m], lower, preferred_element_type=F32)
        upd[m] = product

    wait_directions(order[0])
    with jax.named_scope("wait_scalar"):
        to_tp(sums.at[pl.ds(0, TP - 1)], 1).wait_recv()
    fs_sums[me] = jnp.sum(sums[...], axis=0)

    def send_sum(j):
        ref = fs_sums.at[me]
        to_fs(ref, ref, s_send.at[1], s_recv.at[1], j).start()

    loop(1, FS, send_sum)
    for i in range(4):
        weights_to(i, wbuf.at[2, half, :], near_out.at[i], 2).start()
    wait_directions(order[1])
    update(1)

    @pl.when(odd == 1)
    def _():
        update(0)

    @pl.when(odd == 0)
    def _():
        update(2)

    @pl.when(core == 1)
    def _():
        ring.finish(fbuf.at[others, pl.ds(0, 2)])
        along_y(fbuf.at[others, 0], 0).wait_send()
        to_other_core(fbuf.at[others, pl.ds(0, 2), pl.ds(0, HALF)], 0).wait_send()

    wait_directions(order[2])

    @pl.when(odd == 0)
    def _():
        update(0)

    @pl.when(odd == 1)
    def _():
        update(2)

    with jax.named_scope("wait_fs_scalar"):
        ref = fs_sums.at[others]
        to_fs(ref, ref, s_send.at[1], s_recv.at[1], 1).wait_recv()
    total = jnp.sum(jnp.sum(fs_sums[...], axis=0), keepdims=True)
    norm_scale = lax.rsqrt(total / (3 * RANK * C) + SQUARE_EPS)
    for m in range(3):
        scaled = norm_scale * upd[m]
        upd[m] = scaled
        copies[me, m] = (wbuf[m] - LEARN_RATE * scaled).astype(BF16)

    def copy_part(s, k, part_half):
        at, size = HALF * (k + core - 2 * k * core), HALF
        if part_half is not None:
            at, size = at + 64 * part_half, 64
        return copies.at[s, :, pl.ds(pl.multiple_of(at, 64), size), :]

    def near_copies():
        with jax.named_scope("wait_near"):
            weights_to(0, near_w, near_w, 0).wait_recv()
            near_factors().wait_recv()
        with jax.named_scope("near"):
            for m in range(2):
                upper, lower = high_low(dirs[m].reshape(RANK, W))
                rows = jnp.concatenate([fbuf[s, m, half, :] for s in near_slots], axis=0)
                product = jnp.dot(rows, upper, preferred_element_type=F32)
                product += jnp.dot(rows, lower, preferred_element_type=F32)
                scaled = norm_scale * product
                for i, s in enumerate(near_slots):
                    update = scaled[HALF * i : HALF * (i + 1)]
                    copies[s, m, half, :] = (near_w[i, m] - LEARN_RATE * update).astype(BF16)
        with jax.named_scope("wait_near_out"):
            weights_to(0, near_out, near_out, 2).wait_recv()
        with jax.named_scope("near_out"):
            turned[...] = dirs[2].reshape(RANK, W).T
            upper, lower = high_low(turned[half, :])
            contract = (((1,), (1,)), ((), ()))
            other_half = pl.ds(pl.multiple_of((1 - core) * HALF, HALF), HALF)
            for cols, rows in (
                (half, [fbuf[s, 2, half, :] for s in near_slots]),
                (other_half, [near_f[i] for i in range(4)]),
            ):
                rows = jnp.concatenate(rows, axis=0)
                product = lax.dot_general(upper, rows, contract, preferred_element_type=F32)
                product += lax.dot_general(lower, rows, contract, preferred_element_type=F32)
                scaled = norm_scale * product
                for i, s in enumerate(near_slots):
                    update = scaled[:, HALF * i : HALF * (i + 1)]
                    copies[s, 2, half, cols] = (
                        near_out[i, :, cols] - LEARN_RATE * update
                    ).astype(BF16)

    gather = RingGather("c", me, copy_part, ring_send.at[0], ring_recv, True)
    for group in gather.steps(lambda k, po, qo: None):
        if group == "start":
            near_copies()

    with jax.named_scope("finish"):
        gather.finish(copies.at[pl.ds(0, 13)])
        weights_to(0, near_w, near_w, 0).wait_send()
        near_factors().wait_send()
        weights_to(0, near_out, near_out, 2).wait_send()
        to_partner(cots_t.at[0], cots_t.at[1], 3).wait_send()
        for m in range(3):
            to_partner(pieces.at[1, m], from_core.at[m], m).wait_send()
            ref = pieces.at[0, m, others]
            to_fs(ref, ref, a_send.at[0], a_recv.at[m], 1).wait_send()
            ref = dirs.at[m, others]
            to_fs(ref, ref, d_send.at[0], d_recv.at[m], 1).wait_send()
        to_tp(sums.at[pl.ds(0, TP - 1)], 1).wait_send()
        ref = fs_sums.at[others]
        to_fs(ref, ref, s_send.at[1], s_recv.at[1], 1).wait_send()


def store_kernel(
    mom,
    upd,
    copies,
    first_out,
    second_out,
    value_update,
    gate_update,
    out_update,
    value_copy,
    gate_copy,
    out_copy,
    sem,
):
    def store(src, dst):
        pltpu.make_async_copy(src, dst, sem.at[0]).start()

    def store_block(s, carry):
        at = pl.ds(pl.multiple_of(s * W, W), W)
        store(copies.at[s, 0], value_copy.at[at, :])
        store(copies.at[s, 1], gate_copy.at[at, :])
        store(copies.at[s, 2], out_copy.at[:, at])
        return carry

    lax.fori_loop(0, FS, store_block, 0)
    store(upd.at[0], value_update)
    store(upd.at[1], gate_update)
    store(upd.at[2], out_update)
    store(mom.at[0], first_out)
    store(mom.at[1], second_out)
    for ref in (copies, upd, mom):
        pltpu.make_async_copy(ref, ref, sem.at[0]).wait()


def shards(*args):
    anywhere = pl.BlockSpec(memory_space=pl.ANY)
    vmem = pl.BlockSpec(memory_space=pltpu.VMEM)
    dma = pltpu.SemaphoreType.DMA
    results = pl.pallas_call(
        kernel,
        out_shape=(
            pltpu.VMEM((2, 3, RS, W), F32),
            pltpu.VMEM((3, W, W), F32),
            pltpu.VMEM((FS, 3, W, W), BF16),
        ),
        in_specs=[anywhere] * 11,
        out_specs=(vmem,) * 3,
        scratch_shapes=[
            pltpu.VMEM((2, TOK, D // 2), BF16),
            pltpu.VMEM((3, TOK, W), BF16),
            pltpu.VMEM((2, 3, W, TOK), BF16),
            pltpu.VMEM((FS, 3, W, RANK), BF16),
            pltpu.VMEM((3, W, W), F32),
            pltpu.VMEM((4, 2, HALF, W), F32),
            pltpu.VMEM((4, HALF, W), F32),
            pltpu.VMEM((4, HALF, RANK), BF16),
            pltpu.VMEM((W, RANK), F32),
            pltpu.VMEM((3, TOK, RANK), F32),
            pltpu.VMEM((2, 3, FS, RS, W), F32),
            pltpu.VMEM((3, FS, RS, W), F32),
            pltpu.VMEM((3, FS, RS, W), F32),
            pltpu.VMEM((3, FS, RS, W), F32),
            pltpu.VMEM((TP, 1, 128), F32),
            pltpu.VMEM((FS, 1, 128), F32),
            dma((6,)),
            dma((1,)),
            dma((len(RECEIVED),)),
            dma((3,)),
            dma((5,)),
            dma((5,)),
            dma((1,)),
            dma((3,)),
            dma((1,)),
            dma((3,)),
            dma((2,)),
            dma((2,)),
            dma((3,)),
            dma((3,)),
        ],
        compiler_params=pltpu.CompilerParams(
            collective_id=0, has_side_effects=True, vmem_limit_bytes=48 * 1024 * 1024
        ),
    )(*[pltpu.with_memory_space_constraint(a, pltpu.HBM) for a in args])
    return pl.pallas_call(
        store_kernel,
        out_shape=(
            jax.ShapeDtypeStruct((3, RS, W), F32),
            jax.ShapeDtypeStruct((3, RS, W), F32),
            jax.ShapeDtypeStruct((W, W), F32),
            jax.ShapeDtypeStruct((W, W), F32),
            jax.ShapeDtypeStruct((W, W), F32),
            jax.ShapeDtypeStruct((D, W), BF16),
            jax.ShapeDtypeStruct((D, W), BF16),
            jax.ShapeDtypeStruct((W, D), BF16),
        ),
        in_specs=[vmem] * 3,
        out_specs=(anywhere,) * 8,
        scratch_shapes=[dma((1,))],
        compiler_params=pltpu.CompilerParams(vmem_limit_bytes=4 * 1024 * 1024),
    )(*[pltpu.with_memory_space_constraint(r, pltpu.VMEM) for r in results])


def solution(mesh):
    placed = (
        P("fs", None),
        P("fs", "tp"),
        P("fs", "tp"),
        P("fs", None),
        P("fs", "tp"),
        P(None, "fs", None),
        P("fs", "tp"),
        P("fs", "tp"),
        P("tp", "fs"),
        P(None, "fs", "tp"),
        P(None, "fs", "tp"),
    )
    return jax.shard_map(
        shards,
        mesh=mesh,
        in_specs=placed,
        out_specs=(
            P(None, "fs", "tp"),
            P(None, "fs", "tp"),
            P("fs", "tp"),
            P("fs", "tp"),
            P("tp", "fs"),
            P(None, "tp"),
            P(None, "tp"),
            P("tp", None),
        ),
        check_vma=False,
    )
```

```python
import functools

import jax
import jax.numpy as jnp
from jax import lax
from jax.experimental import pallas as pl
from jax.experimental.pallas import tpu as pltpu
from jax.sharding import PartitionSpec as P

C = 2048
RANK = 256
FIRST_DECAY = 0.9
SECOND_DECAY = 0.95
DIVISOR_EPS = 1e-08
SQUARE_EPS = 1e-06
LEARN_RATE = 0.01

SIDE = 4
FS = SIDE * SIDE
TP = 8
HALF = 128
W = 256
RS = RANK // FS
TOK = 1024
D = 4096
MESH = pl.DeviceIdType.MESH
F32 = jnp.float32
BF16 = jnp.bfloat16

RECEIVED = []
for _k in (0, 1):
    RECEIVED += [(_k, 1, 0, 1), (_k, 1, 0, -1), (_k, 2, 0, 0)]
    for _po in (0, -1, 1, 2):
        RECEIVED += [(_k, 3, _po, 1), (_k, 3, _po, -1), (_k, 4, _po, 0)]
INDEX = {message: at for at, message in enumerate(RECEIVED)}


class RingGather:
    def __init__(self, name, me, part, send, recv, near=False):
        self.near = near
        self.name = name
        self.z, self.x = me // SIDE, lax.rem(me, SIDE)
        self.part, self.send, self.recv = part, send, recv

    def slot(self, k, po, qo):
        dx, dz = (po, qo) if k == 0 else (qo, po)
        z = lax.rem(self.z + dz + SIDE, SIDE)
        x = lax.rem(self.x + dx + SIDE, SIDE)
        return z * SIDE + x

    def copy(self, ref, k, stage, po, d, to):
        sem = self.recv.at[INDEX[k, stage, po, 0 if stage in (2, 4) else d]]
        return pltpu.make_async_remote_copy(
            src_ref=ref,
            dst_ref=ref,
            send_sem=self.send,
            recv_sem=sem,
            device_id={"fs": to},
            device_id_type=MESH,
        )

    def skipped(self, k, stage, po):
        return self.near and k == 0 and (stage == 1 or (stage == 3 and po == 0))

    def start(self, k, stage, po, d):
        first = stage in (1, 2)
        at = {1: (0, 0), 2: (-d, 0), 3: (po, 0), 4: (po, -d)}[stage]
        half = None if stage in (1, 3) else (0 if d > 0 else 1)
        to = self.slot(k, d, 0) if first else self.slot(k, 0, d)
        if self.skipped(k, stage, po):
            return
        ref = self.part(self.slot(k, *at), k, half)
        self.copy(ref, k, stage, po, d, to).start()

    def wait(self, k, stage, po, d=0):
        at = {1: (-d, 0), 2: (2, 0), 3: (po, -d), 4: (po, 2)}[stage]
        ref = self.part(self.slot(k, *at), k, None)
        with jax.named_scope(f"w{self.name}_{k}_{stage}_{po}_{d}"):
            self.copy(ref, k, stage, po, d, self.slot(k, 1, 0)).wait_recv()

    def steps(self, arrived):
        for stage in (1, 3):
            for d in (1, -1):
                for k in (0, 1):
                    self.start(k, stage, 0, d)
        yield "start"
        if self.near:
            for d in (1, -1):
                self.start(0, 2, 0, d)
                self.start(0, 4, 0, d)
        for d in (1, -1):
            for k in (1,) if self.near else (0, 1):
                self.wait(k, 1, 0, d)
                self.start(k, 2, 0, d)
                arrived(k, -d, 0)
        for po in (-1, 1):
            for d in (1, -1):
                for k in (0, 1):
                    self.start(k, 3, po, d)
        yield "1"
        self.second(arrived, 0)
        yield "3_0"
        for k in (0, 1):
            self.wait(k, 2, 0)
            self.start(k, 3, 2, 1)
            self.start(k, 3, 2, -1)
            arrived(k, 2, 0)
        yield "2"
        if self.near:
            self.second(arrived, -1)
            self.second(arrived, 1, later=True)
            self.second(arrived, 2)
            for k in (0, 1):
                for d in (1, -1):
                    self.start(k, 4, 1, d)
            self.last(arrived, 0)
        else:
            for po in (-1, 1):
                self.second(arrived, po)
                yield f"3_{po}"
            self.last(arrived, 0)
            yield "4_0"
            self.second(arrived, 2)
            yield "3_2"
        for po in (-1, 1, 2):
            self.last(arrived, po)
            yield f"4_{po}"

    def second(self, arrived, po, later=False):
        for d in (1, -1):
            for k in (0, 1):
                if not self.skipped(k, 3, po):
                    self.wait(k, 3, po, d)
                    if not later:
                        self.start(k, 4, po, d)
                arrived(k, po, -d)

    def last(self, arrived, po):
        for k in (0, 1):
            self.wait(k, 4, po)
            arrived(k, po, 2)

    def finish(self, everything):
        self.copy(everything, 0, 1, 0, 1, self.slot(0, 1, 0)).wait_send()


def high_low(values):
    upper = values.astype(BF16)
    return upper, (values - upper.astype(F32)).astype(BF16)


def kernel(
    inputs,
    value_cot,
    gate_cot,
    out_cot,
    conv_output,
    factors,
    value_weight,
    gate_weight,
    out_weight,
    first_moment,
    second_moment,
    mom,
    upd,
    copies,
    left,
    cots,
    cots_t,
    fbuf,
    wbuf,
    near_w,
    near_out,
    near_f,
    turned,
    summed,
    pieces,
    from_core,
    arrived,
    dirs,
    sums,
    fs_sums,
    load_sem,
    ring_send,
    ring_recv,
    core_send,
    core_recv,
    batch_recv,
    a_send,
    a_recv,
    d_send,
    d_recv,
    s_send,
    s_recv,
    w_send,
    w_recv,
):
    me = lax.axis_index("fs")
    t = lax.axis_index("tp")
    core = lax.rem(t, 2)
    partner = t + 1 - 2 * core

    barrier = pltpu.get_barrier_semaphore()

    def greet_fs(j, _):
        pl.semaphore_signal(
            barrier, inc=1, device_id={"fs": lax.rem(me + j, FS)}, device_id_type=MESH
        )
        return _

    def greet_tp(j, _):
        pl.semaphore_signal(
            barrier, inc=1, device_id={"tp": lax.rem(t + j, TP)}, device_id_type=MESH
        )
        return _

    lax.fori_loop(1, FS, greet_fs, 0)
    lax.fori_loop(1, TP, greet_tp, 0)

    def load(at, *pairs):
        for src, dst in pairs:
            pltpu.make_async_copy(src, dst, load_sem.at[at]).start()

    def loaded(at, ref):
        pltpu.make_async_copy(ref, ref, load_sem.at[at]).wait()

    half = pl.ds(pl.multiple_of(core * HALF, HALF), HALF)
    load(0, (factors, fbuf.at[me]))
    load(1, *((r, cots.at[m]) for m, r in enumerate((value_cot, gate_cot, conv_output))))

    def load_half(s, carry):
        src = pl.ds(pl.multiple_of(s * W + core * HALF, HALF), HALF)
        dst = pl.ds(pl.multiple_of(s * HALF, HALF), HALF)
        load(2, (inputs.at[:, src], left.at[0, :, dst]))
        load(3, (out_cot.at[:, src], left.at[1, :, dst]))
        return carry

    lax.fori_loop(0, FS, load_half, 0)
    load(4, (first_moment, mom.at[0]), (second_moment, mom.at[1]))
    load(5, *((r, wbuf.at[m]) for m, r in enumerate((value_weight, gate_weight, out_weight))))

    with jax.named_scope("barrier"):
        pl.semaphore_wait(barrier, FS - 1 + TP - 1)

    def to_partner(src, dst, at):
        return pltpu.make_async_remote_copy(
            src_ref=src,
            dst_ref=dst,
            send_sem=core_send.at[0],
            recv_sem=core_recv.at[at],
            device_id={"tp": partner},
            device_id_type=MESH,
        )

    def factor_part(s, k, half):
        at, size = HALF * k, HALF
        if half is not None:
            at, size = at + 64 * half, 64
        return fbuf.at[s, pl.ds(odd_base, 2), pl.ds(at, size), :]

    y = t // 2
    odd = lax.rem(y, 2)
    odd_base = 1 - odd
    lacking, handed = 2 * odd, 2 - 2 * odd

    def along_y(ref, k):
        to = lax.rem(2 * y + (2 if k == 0 else TP - 2), TP) + k
        return pltpu.make_async_remote_copy(
            src_ref=ref,
            dst_ref=ref,
            send_sem=core_send.at[1],
            recv_sem=core_recv.at[4],
            device_id={"tp": to},
            device_id_type=MESH,
        )

    ring = RingGather("a", me, factor_part, ring_send.at[0], ring_recv)
    here = []

    def to_other_core(ref, batch):
        return pltpu.make_async_remote_copy(
            src_ref=ref,
            dst_ref=ref,
            send_sem=core_send.at[2],
            recv_sem=batch_recv.at[batch],
            device_id={"tp": partner},
            device_id_type=MESH,
        )

    def factor_arrived(k, po, qo):
        s = ring.slot(k, po, qo)
        if k == 0:
            here.append((po, qo))
            to_other_core(factor_part(s, 0, None), state["batch"]).start()
        along_y(fbuf.at[s, handed, pl.ds(HALF * k, HALF), :], k).start()

    state = {"batch": 0}
    groups = ring.steps(factor_arrived)

    def slots_until(group):
        @pl.when(core == 1)
        def _():
            while next(groups) != group:
                pass

        count = len(here)

        @pl.when(core == 0)
        def _():
            with jax.named_scope("wait_batch"):
                ref = fbuf.at[pl.ds(0, count), pl.ds(0, 2), pl.ds(0, HALF), :]
                to_other_core(ref, state["batch"]).wait_recv()

        slots = []
        for po, qo in here:
            zero, one = ring.slot(0, po, qo), ring.slot(1, po, qo)
            slots.append(zero + core * (one - zero))
        here.clear()
        state["batch"] += 1
        return slots

    def multiply(*slots, first=False, matrices=(odd_base, odd_base + 1)):
        with jax.named_scope("multiply"):
            for m in matrices:
                ours = [
                    left[m // 2, :, pl.ds(pl.multiple_of(s * HALF, HALF), HALF)]
                    for s in slots
                ]
                product = jnp.dot(
                    jnp.concatenate(ours, axis=1),
                    jnp.concatenate([fbuf[s, m, half, :] for s in slots], axis=0),
                    preferred_element_type=F32,
                )
                if first:
                    summed[m] = product
                else:
                    summed[m] += product

    def multiply_lacking():
        with jax.named_scope("multiply_lacking"):
            right = fbuf[:, lacking, half, :].reshape(D // 2, RANK)

            def tile(i, carry):
                rows = pl.ds(pl.multiple_of(i * 512, 512), 512)
                ours = left[lacking // 2, rows, :]
                summed[lacking, rows, :] = jnp.dot(ours, right, preferred_element_type=F32)
                return carry

            lax.fori_loop(0, TOK // 512, tile, 0)

    def loop(start, stop, step):
        def body(j, carry):
            step(j)
            return carry

        lax.fori_loop(start, stop, body, 0)

    def to_fs(src, dst, send, recv, j):
        return pltpu.make_async_remote_copy(
            src_ref=src,
            dst_ref=dst,
            send_sem=send,
            recv_sem=recv,
            device_id={"fs": lax.rem(me + j, FS)},
            device_id_type=MESH,
        )

    others = pl.ds(0, FS - 1)

    def project(m):
        with jax.named_scope("project"):
            split = jnp.concatenate(high_low(summed[m]), axis=1)
            for side in (1, 0):
                product = jnp.dot(cots_t[side, m], split, preferred_element_type=F32)
                product = product[:, :RANK] + product[:, RANK:]
                pieces[side, m] = product.T.reshape(FS, RS, W)
                if side == 1:
                    to_partner(pieces.at[1, m], from_core.at[m], m).start()

    def send_pieces(m):
        with jax.named_scope("wait_core"):
            to_partner(pieces.at[1, m], from_core.at[m], m).wait_recv()
        pieces[0, m] += from_core[m]

        def send_piece(j):
            to_fs(
                pieces.at[0, m, lax.rem(me + j, FS)],
                arrived.at[m, me],
                a_send.at[0],
                a_recv.at[m],
                j,
            ).start()

        loop(1, FS, send_piece)
        arrived[m, me] = pieces[0, m, me]

    def to_tp(ref, j):
        return pltpu.make_async_remote_copy(
            src_ref=ref,
            dst_ref=ref,
            send_sem=s_send.at[0],
            recv_sem=s_recv.at[0],
            device_id={"tp": lax.rem(t + j, TP)},
            device_id_type=MESH,
        )

    squares = []

    def moments(m):
        with jax.named_scope("wait_pieces"):
            ref = arrived.at[m, others]
            to_fs(ref, ref, a_send.at[0], a_recv.at[m], 1).wait_recv()
        projected = jnp.sum(arrived[m], axis=0)
        new_first = FIRST_DECAY * mom[0, m] + (1.0 - FIRST_DECAY) * projected
        new_second = (
            SECOND_DECAY * mom[1, m] + (1.0 - SECOND_DECAY) * projected * projected
        )
        direction = new_first / (jnp.sqrt(new_second) + DIVISOR_EPS)
        mom[0, m] = new_first
        mom[1, m] = new_second
        dirs[m, me] = direction
        squares.append(jnp.sum(direction * direction, axis=0, keepdims=True))
        if len(squares) == 3:
            square = squares[0] + squares[1] + squares[2]
            sums[t] = square[:, :128] + square[:, 128:]
            loop(1, TP, lambda j: to_tp(sums.at[t], j).start())

        def send_direction(j):
            ref = dirs.at[m, me]
            to_fs(ref, ref, d_send.at[0], d_recv.at[m], j).start()

        loop(1, FS, send_direction)

    loaded(0, fbuf.at[me])

    @pl.when(core == 1)
    def _():
        next(groups)

    with jax.named_scope("turn"):
        loaded(1, cots)
        for m in range(3):

            def turn(i, _):
                rows = pl.ds(pl.multiple_of(i * 256, 256), 256)
                cots_t[0, m, :, rows] = cots[m, rows, :].T
                return _

            lax.fori_loop(0, TOK // 256, turn, 0)

    to_partner(cots_t.at[0], cots_t.at[1], 3).start()
    with jax.named_scope("wait_loads"):
        loaded(2, left.at[0])
        loaded(3, left.at[1])
    multiply(me, first=True)
    near_slots = [ring.slot(0, *at) for at in ((-1, 0), (1, 0), (0, -1), (0, 1))]

    def weights_to(i, src, dst, at):
        to = ((1, 0), (-1, 0), (0, 1), (0, -1))[i]
        return pltpu.make_async_remote_copy(
            src_ref=src,
            dst_ref=dst,
            send_sem=w_send.at[at],
            recv_sem=w_recv.at[at],
            device_id={"fs": ring.slot(0, *to)},
            device_id_type=MESH,
        )

    for group in ("3_0", "3_1", "3_2", "4_1"):
        slots = slots_until(group)
        if group == "3_2":
            loaded(5, wbuf)
            for i in range(4):
                weights_to(i, wbuf.at[pl.ds(0, 2), half, :], near_w.at[i], 0).start()
        multiply(*slots)
    to_partner(cots_t.at[0], cots_t.at[1], 3).wait_recv()
    last = slots_until("4_2")
    order = (odd_base, odd_base + 1, lacking)
    multiply(*last, matrices=order[:1])
    project(order[0])
    multiply(*last, matrices=order[1:2])
    send_pieces(order[0])
    project(order[1])
    send_pieces(order[1])
    with jax.named_scope("wait_y"):
        along_y(fbuf.at[others, 0, pl.ds(0, HALF)], 0).wait_recv()

    def near_factor(i):
        return pltpu.make_async_remote_copy(
            src_ref=fbuf.at[near_slots[i], 2, half, :],
            dst_ref=near_f.at[i],
            send_sem=w_send.at[1],
            recv_sem=w_recv.at[1],
            device_id={"tp": partner},
            device_id_type=MESH,
        )

    def near_factors():
        return pltpu.make_async_remote_copy(
            src_ref=near_f,
            dst_ref=near_f,
            send_sem=w_send.at[1],
            recv_sem=w_recv.at[1],
            device_id={"tp": partner},
            device_id_type=MESH,
        )

    for i in range(4):
        near_factor(i).start()
    multiply_lacking()
    project(order[2])
    send_pieces(order[2])
    loaded(4, mom)
    for m in order:
        moments(m)

    def wait_directions(m):
        with jax.named_scope("wait_directions"):
            ref = dirs.at[m, others]
            to_fs(ref, ref, d_send.at[0], d_recv.at[m], 1).wait_recv()

    def update(m):
        full = dirs[m].reshape(RANK, W)
        if m == 2:
            upper, lower = high_low(full.T)
            contract = (((1,), (1,)), ((), ()))
            own = fbuf[me, m]
            product = lax.dot_general(upper, own, contract, preferred_element_type=F32)
            product += lax.dot_general(lower, own, contract, preferred_element_type=F32)
        else:
            upper, lower = high_low(full)
            product = jnp.dot(fbuf[me, m], upper, preferred_element_type=F32)
            product += jnp.dot(fbuf[me, m], lower, preferred_element_type=F32)
        upd[m] = product

    wait_directions(order[0])
    with jax.named_scope("wait_scalar"):
        to_tp(sums.at[pl.ds(0, TP - 1)], 1).wait_recv()
    fs_sums[me] = jnp.sum(sums[...], axis=0)

    def send_sum(j):
        ref = fs_sums.at[me]
        to_fs(ref, ref, s_send.at[1], s_recv.at[1], j).start()

    loop(1, FS, send_sum)
    for i in range(4):
        weights_to(i, wbuf.at[2, half, :], near_out.at[i], 2).start()
    wait_directions(order[1])
    update(1)

    @pl.when(odd == 1)
    def _():
        update(0)

    @pl.when(odd == 0)
    def _():
        update(2)

    @pl.when(core == 1)
    def _():
        ring.finish(fbuf.at[others, pl.ds(0, 2)])
        along_y(fbuf.at[others, 0], 0).wait_send()
        to_other_core(fbuf.at[others, pl.ds(0, 2), pl.ds(0, HALF)], 0).wait_send()

    wait_directions(order[2])

    @pl.when(odd == 0)
    def _():
        update(0)

    @pl.when(odd == 1)
    def _():
        update(2)

    with jax.named_scope("wait_fs_scalar"):
        ref = fs_sums.at[others]
        to_fs(ref, ref, s_send.at[1], s_recv.at[1], 1).wait_recv()
    total = jnp.sum(jnp.sum(fs_sums[...], axis=0), keepdims=True)
    norm_scale = lax.rsqrt(total / (3 * RANK * C) + SQUARE_EPS)
    for m in range(3):
        scaled = norm_scale * upd[m]
        upd[m] = scaled
        copies[me, m] = (wbuf[m] - LEARN_RATE * scaled).astype(BF16)

    def copy_part(s, k, part_half):
        at, size = HALF * (k + core - 2 * k * core), HALF
        if part_half is not None:
            at, size = at + 64 * part_half, 64
        return copies.at[s, :, pl.ds(pl.multiple_of(at, 64), size), :]

    def near_copies():
        with jax.named_scope("wait_near"):
            weights_to(0, near_w, near_w, 0).wait_recv()
            near_factors().wait_recv()
        with jax.named_scope("near"):
            for m in range(2):
                upper, lower = high_low(dirs[m].reshape(RANK, W))
                rows = jnp.concatenate([fbuf[s, m, half, :] for s in near_slots], axis=0)
                product = jnp.dot(rows, upper, preferred_element_type=F32)
                product += jnp.dot(rows, lower, preferred_element_type=F32)
                scaled = norm_scale * product
                for i, s in enumerate(near_slots):
                    update = scaled[HALF * i : HALF * (i + 1)]
                    copies[s, m, half, :] = (near_w[i, m] - LEARN_RATE * update).astype(BF16)
        with jax.named_scope("wait_near_out"):
            weights_to(0, near_out, near_out, 2).wait_recv()
        with jax.named_scope("near_out"):
            turned[...] = dirs[2].reshape(RANK, W).T
            upper, lower = high_low(turned[half, :])
            contract = (((1,), (1,)), ((), ()))
            other_half = pl.ds(pl.multiple_of((1 - core) * HALF, HALF), HALF)
            for cols, rows in (
                (half, [fbuf[s, 2, half, :] for s in near_slots]),
                (other_half, [near_f[i] for i in range(4)]),
            ):
                rows = jnp.concatenate(rows, axis=0)
                product = lax.dot_general(upper, rows, contract, preferred_element_type=F32)
                product += lax.dot_general(lower, rows, contract, preferred_element_type=F32)
                scaled = norm_scale * product
                for i, s in enumerate(near_slots):
                    update = scaled[:, HALF * i : HALF * (i + 1)]
                    copies[s, 2, half, cols] = (
                        near_out[i, :, cols] - LEARN_RATE * update
                    ).astype(BF16)

    gather = RingGather("c", me, copy_part, ring_send.at[0], ring_recv, True)
    for group in gather.steps(lambda k, po, qo: None):
        if group == "start":
            near_copies()

    with jax.named_scope("finish"):
        gather.finish(copies.at[pl.ds(0, 13)])
        weights_to(0, near_w, near_w, 0).wait_send()
        near_factors().wait_send()
        weights_to(0, near_out, near_out, 2).wait_send()
        to_partner(cots_t.at[0], cots_t.at[1], 3).wait_send()
        for m in range(3):
            to_partner(pieces.at[1, m], from_core.at[m], m).wait_send()
            ref = pieces.at[0, m, others]
            to_fs(ref, ref, a_send.at[0], a_recv.at[m], 1).wait_send()
            ref = dirs.at[m, others]
            to_fs(ref, ref, d_send.at[0], d_recv.at[m], 1).wait_send()
        to_tp(sums.at[pl.ds(0, TP - 1)], 1).wait_send()
        ref = fs_sums.at[others]
        to_fs(ref, ref, s_send.at[1], s_recv.at[1], 1).wait_send()


def store_kernel(
    mom,
    upd,
    copies,
    first_out,
    second_out,
    value_update,
    gate_update,
    out_update,
    value_copy,
    gate_copy,
    out_copy,
    sem,
):
    def store(src, dst):
        pltpu.make_async_copy(src, dst, sem.at[0]).start()

    def store_block(s, carry):
        at = pl.ds(pl.multiple_of(s * W, W), W)
        store(copies.at[s, 0], value_copy.at[at, :])
        store(copies.at[s, 1], gate_copy.at[at, :])
        store(copies.at[s, 2], out_copy.at[:, at])
        return carry

    lax.fori_loop(0, FS, store_block, 0)
    store(upd.at[0], value_update)
    store(upd.at[1], gate_update)
    store(upd.at[2], out_update)
    store(mom.at[0], first_out)
    store(mom.at[1], second_out)
    for ref in (copies, upd, mom):
        pltpu.make_async_copy(ref, ref, sem.at[0]).wait()


def shards(*args):
    anywhere = pl.BlockSpec(memory_space=pl.ANY)
    vmem = pl.BlockSpec(memory_space=pltpu.VMEM)
    dma = pltpu.SemaphoreType.DMA
    results = pl.pallas_call(
        kernel,
        out_shape=(
            pltpu.VMEM((2, 3, RS, W), F32),
            pltpu.VMEM((3, W, W), F32),
            pltpu.VMEM((FS, 3, W, W), BF16),
        ),
        in_specs=[anywhere] * 11,
        out_specs=(vmem,) * 3,
        scratch_shapes=[
            pltpu.VMEM((2, TOK, D // 2), BF16),
            pltpu.VMEM((3, TOK, W), BF16),
            pltpu.VMEM((2, 3, W, TOK), BF16),
            pltpu.VMEM((FS, 3, W, RANK), BF16),
            pltpu.VMEM((3, W, W), F32),
            pltpu.VMEM((4, 2, HALF, W), F32),
            pltpu.VMEM((4, HALF, W), F32),
            pltpu.VMEM((4, HALF, RANK), BF16),
            pltpu.VMEM((W, RANK), F32),
            pltpu.VMEM((3, TOK, RANK), F32),
            pltpu.VMEM((2, 3, FS, RS, W), F32),
            pltpu.VMEM((3, FS, RS, W), F32),
            pltpu.VMEM((3, FS, RS, W), F32),
            pltpu.VMEM((3, FS, RS, W), F32),
            pltpu.VMEM((TP, 1, 128), F32),
            pltpu.VMEM((FS, 1, 128), F32),
            dma((6,)),
            dma((1,)),
            dma((len(RECEIVED),)),
            dma((3,)),
            dma((5,)),
            dma((5,)),
            dma((1,)),
            dma((3,)),
            dma((1,)),
            dma((3,)),
            dma((2,)),
            dma((2,)),
            dma((3,)),
            dma((3,)),
        ],
        compiler_params=pltpu.CompilerParams(
            collective_id=0, has_side_effects=True, vmem_limit_bytes=48 * 1024 * 1024
        ),
    )(*[pltpu.with_memory_space_constraint(a, pltpu.HBM) for a in args])
    return pl.pallas_call(
        store_kernel,
        out_shape=(
            jax.ShapeDtypeStruct((3, RS, W), F32),
            jax.ShapeDtypeStruct((3, RS, W), F32),
            jax.ShapeDtypeStruct((W, W), F32),
            jax.ShapeDtypeStruct((W, W), F32),
            jax.ShapeDtypeStruct((W, W), F32),
            jax.ShapeDtypeStruct((D, W), BF16),
            jax.ShapeDtypeStruct((D, W), BF16),
            jax.ShapeDtypeStruct((W, D), BF16),
        ),
        in_specs=[vmem] * 3,
        out_specs=(anywhere,) * 8,
        scratch_shapes=[dma((1,))],
        compiler_params=pltpu.CompilerParams(vmem_limit_bytes=4 * 1024 * 1024),
    )(*[pltpu.with_memory_space_constraint(r, pltpu.VMEM) for r in results])


def solution(mesh):
    placed = (
        P("fs", None),
        P("fs", "tp"),
        P("fs", "tp"),
        P("fs", None),
        P("fs", "tp"),
        P(None, "fs", None),
        P("fs", "tp"),
        P("fs", "tp"),
        P("tp", "fs"),
        P(None, "fs", "tp"),
        P(None, "fs", "tp"),
    )
    return jax.shard_map(
        shards,
        mesh=mesh,
        in_specs=placed,
        out_specs=(
            P(None, "fs", "tp"),
            P(None, "fs", "tp"),
            P("fs", "tp"),
            P("fs", "tp"),
            P("tp", "fs"),
            P(None, "tp"),
            P(None, "tp"),
            P("tp", None),
        ),
        check_vma=False,
    )
```
